256 devices in a mesh: dp: 4 (over y), kv: 32 (over z, x), tp: 2 (over core).
Axes of the slice: x: 4, y: 4, z: 8, core: 2. Of those that a mesh axis runs over, the one named last changes fastest.
Arguments:
- tokens: bfloat16 [256, 4, 2048], P('dp', None, 'kv'), may hold values from -420 to 420
- input_norm_gain: bfloat16 [2048], replicated, may hold values from 0.099609375 to 1.8984375
- head_input_weight: bfloat16 [2048, 3072], P('kv', 'tp'), may hold values from -0.125 to 0.125
- output_gate_weight: bfloat16 [2048, 3072], P('kv', 'tp'), may hold values from -0.125 to 0.125
- state_maps_weight: bfloat16 [2048, 2, 1024], P('kv', None, 'tp'), may hold values from -0.125 to 0.125
- step_size_weight: bfloat16 [2048, 48], replicated, may hold values from -0.125 to 0.125
- step_size_bias: float32 [48], replicated, may hold values from -4 to -1
- head_decay_speed: float32 [48], replicated, may hold values from 0.3 to 8
- proposal_decay_total: float32 [256, 4, 48], P(('dp', 'kv'), None, 'tp'), may hold values from -0.7 to 0
- head_input_kernel: bfloat16 [4, 3072], replicated, may hold values from -3 to 3
- state_maps_kernel: bfloat16 [4, 2, 1024], replicated, may hold values from -3 to 3
- head_direct_gain: float32 [48], replicated, may hold values from 0.5 to 1.5
- grouped_norm_gain: bfloat16 [3072], replicated, may hold values from 0.099609375 to 1.8984375
- output_weight: bfloat16 [3072, 2048], P('tp', 'kv'), may hold values from -0.109375 to 0.109375
- prior_state_value: float32 [256, 48, 64, 128], P(('dp', 'kv'), 'tp'), may hold values from -2.4 to 2.4
- previous_head_input: bfloat16 [256, 4, 3072], P(('dp', 'kv'), None, 'tp'), may hold values from -2.390625 to 2.390625
- previous_input_maps: bfloat16 [256, 4, 1024], P(('dp', 'kv'), None, 'tp'), may hold values from -5 to 5
- previous_log_decays: float32 [256, 4, 48], P(('dp', 'kv'), None, 'tp'), may hold values from -1.5 to -0.05
- prior_heads_window: bfloat16 [256, 7, 3072], P(('dp', 'kv'), None, 'tp'), may hold values from -6 to 6
- prior_maps_window: bfloat16 [256, 7, 2, 1024], P(('dp', 'kv'), None, None, 'tp'), may hold values from -6 to 6
- accepted: int32 [256], P(('dp', 'kv')), may hold values from 1 to 4
Outputs:
- mixed: bfloat16 [256, 4, 2048], P('dp', None, 'kv')
- accepted_state: float32 [256, 48, 64, 128], P(('dp', 'kv'), 'tp')
- current_head_input: bfloat16 [256, 4, 3072], P(('dp', 'kv'), None, 'tp')
- current_input_maps: bfloat16 [256, 4, 1024], P(('dp', 'kv'), None, 'tp')
- current_log_decays: float32 [256, 4, 48], P(('dp', 'kv'), None, 'tp')
- current_heads_window: bfloat16 [256, 7, 3072], P(('dp', 'kv'), None, 'tp')
- current_maps_window: bfloat16 [256, 7, 2, 1024], P(('dp', 'kv'), None, None, 'tp')
The draws below stay inside these ranges and needn't reach their ends.
All inputs are finite; a program needn't handle non-finite values.
Results may differ from the reference program's by a relative error of at most 0.029.
Values may be sent and summed in bfloat16 or wider, within the bound.
A program may use at most 64 MiB of HBM per device.

```python
import math
import jax
import jax.numpy as jnp
from jax import lax

D = 2048
HEADS = 48
HEAD_DIM = 64
STATE = 128
CONV = 4
PROPOSALS = 4
BATCH = 256
INNER = 3072
BC_WIDTH = 1024
N_KV = 32
N_TP = 2


def draw_tokens(key, part):
    key_base, key_rows = jax.random.split(key, 2)
    columns = jnp.arange(D, dtype=jnp.float32) / D
    base = jnp.clip(jax.random.normal(key_base, (BATCH, PROPOSALS, D), jnp.float32), -4.0, 4.0)
    col_scale = 10.0 ** columns
    row_scale = jnp.exp(jax.random.uniform(key_rows, (BATCH, PROPOSALS, 1), jnp.float32, 0.0, math.log(10.0)))
    return (base * col_scale * row_scale).astype(jnp.bfloat16)


def draw_proposal_decay_total(key, part):
    key_pick, key_size = jax.random.split(key)
    pick = jax.random.randint(key_pick, (BATCH, PROPOSALS, HEADS), 0, 6)
    amounts = jnp.log(jax.random.uniform(key_size, (BATCH, PROPOSALS, HEADS), jnp.float32, 0.5, 0.8))
    return jnp.where(pick == 0, amounts, 0.0).astype(jnp.float32)


def touch_ends(result, own_key, low, largest):
    shape = result.shape
    spot = [jax.random.randint(jax.random.fold_in(own_key, axis), (), 0, shape[axis]) for axis in range(len(shape))]
    result = result.at[tuple(spot)].set(low)
    longest = shape.index(max(shape))
    spot[longest] = (spot[longest] + 1) % shape[longest]
    return result.at[tuple(spot)].set(largest)


def shard_levels(key, extent, shards, least, high):
    gain = 1.0
    for dim, blocks in shards:
        steps = jax.random.uniform(jax.random.fold_in(jax.random.fold_in(key, 6), dim), (blocks,), jnp.float32, least / len(shards), high / len(shards))
        gain = gain * jnp.repeat(jnp.exp(steps), extent[dim] // blocks).reshape((-1,) + (1,) * (len(extent) - 1 - dim))
    return gain


def noise(key, extent, deviation, limit, shards=(), kind=jnp.bfloat16):
    values = jax.random.normal(key, extent, jnp.float32) * deviation
    if len(shards) > 0:
        values = shard_levels(key, extent, shards, -0.22, 0.18) * values
    return jnp.clip(values, min=-limit, max=limit).astype(kind)


def setup_inputs(seed: int = 0) -> dict:
    arg_keys = jax.random.split(jax.random.key(seed), 22)
    tokens = draw_tokens(jax.random.fold_in(arg_keys[21], 71), 0)
    input_norm_gain = jnp.clip(1.0 + 0.18 * jax.random.normal(arg_keys[1], (D,), jnp.float32), 0.099609375, 1.8984375).astype(jnp.bfloat16)
    head_input_weight = noise(arg_keys[2], (D, INNER), D ** -0.5, 0.125, ((0, 32), (1, 2)))
    output_gate_weight = noise(arg_keys[3], (D, INNER), D ** -0.5, 0.125, ((0, 32), (1, 2)))
    state_maps_weight = noise(arg_keys[4], (D, 2, BC_WIDTH), D ** -0.5, 0.125, ((0, 32), (2, 2)))
    step_size_weight = noise(arg_keys[5], (D, HEADS), D ** -0.5, 0.125)
    step_size_bias = jnp.clip(jax.random.uniform(arg_keys[6], (HEADS,), jnp.float32, -4.0, -1.0), -4.0, -1.0)
    head_decay_speed = jnp.clip(jnp.exp(jax.random.uniform(arg_keys[7], (HEADS,), jnp.float32, math.log(0.3), math.log(8.0))), 0.3, 8.0)
    proposal_decay_total = draw_proposal_decay_total(jax.random.fold_in(arg_keys[21], 71), 0)
    head_input_kernel = noise(arg_keys[9], (CONV, INNER), CONV ** -0.5, 3.0)
    state_maps_kernel = noise(arg_keys[10], (CONV, 2, BC_WIDTH), CONV ** -0.5, 3.0)
    head_direct_gain = jnp.clip(jax.random.uniform(arg_keys[11], (HEADS,), jnp.float32, 0.5, 1.5), 0.5, 1.5)
    grouped_norm_gain = jnp.clip(1.0 + 0.18 * jax.random.normal(arg_keys[12], (INNER,), jnp.float32), 0.099609375, 1.8984375).astype(jnp.bfloat16)
    output_weight = noise(arg_keys[13], (INNER, D), INNER ** -0.5, 0.109375, ((0, 2), (1, 32)))
    prior_state_value = noise(arg_keys[14], (BATCH, HEADS, HEAD_DIM, STATE), 0.3, 2.4, ((0, 128), (1, 2)), jnp.float32)
    previous_head_input = noise(arg_keys[15], (BATCH, PROPOSALS, INNER), 0.3, 2.390625, ((0, 128), (2, 2)))
    previous_input_maps = noise(arg_keys[16], (BATCH, PROPOSALS, BC_WIDTH), 0.7, 5.0, ((0, 128), (2, 2)))
    previous_log_decays = jnp.clip(-1.5 + 1.45 * jax.random.uniform(arg_keys[17], (BATCH, PROPOSALS, HEADS), jnp.float32) ** shard_levels(arg_keys[17], (BATCH, PROPOSALS, HEADS), ((0, 128), (2, 2)), -0.2, 0.2), -1.5, -0.05)
    prior_heads_window = noise(arg_keys[18], (BATCH, CONV - 1 + PROPOSALS, INNER), 1.0, 6.0, ((0, 128), (2, 2)))
    prior_maps_window = noise(arg_keys[19], (BATCH, CONV - 1 + PROPOSALS, 2, BC_WIDTH), 1.0, 6.0, ((0, 128), (3, 2)))
    accepted = touch_ends(jax.random.randint(arg_keys[20], (BATCH,), 1, PROPOSALS + 1), jax.random.fold_in(arg_keys[20], 1), 1, PROPOSALS).astype(jnp.int32)
    return dict(tokens=tokens, input_norm_gain=input_norm_gain, head_input_weight=head_input_weight, output_gate_weight=output_gate_weight, state_maps_weight=state_maps_weight, step_size_weight=step_size_weight, step_size_bias=step_size_bias, head_decay_speed=head_decay_speed, proposal_decay_total=proposal_decay_total, head_input_kernel=head_input_kernel, state_maps_kernel=state_maps_kernel, head_direct_gain=head_direct_gain, grouped_norm_gain=grouped_norm_gain, output_weight=output_weight, prior_state_value=prior_state_value, previous_head_input=previous_head_input, previous_input_maps=previous_input_maps, previous_log_decays=previous_log_decays, prior_heads_window=prior_heads_window, prior_maps_window=prior_maps_window, accepted=accepted)


eps = 1e-06

def pick_tail(history, accepted):
    rows = history.shape[1]
    keep = CONV - 1
    index = jnp.arange(rows, dtype=jnp.int32)
    offsets = jnp.arange(keep, dtype=jnp.int32)
    select = (index[None, None, :] == accepted[:, None, None] + offsets[None, :, None]).astype(jnp.float32)
    flat = history.astype(jnp.float32).reshape(history.shape[0], rows, -1)
    picked = jnp.einsum('skr,src->skc', select, flat, precision=lax.Precision.HIGHEST)
    return picked.reshape((history.shape[0], keep) + history.shape[2:])

def causal_conv(window, weight):
    length = window.shape[1] - CONV + 1
    total = weight[0] * window[:, 0:length]
    for offset in range(1, CONV):
        total = total + weight[offset] * window[:, offset:offset + length]
    return jax.nn.silu(total)

def local_mixer_output(unfiltered_heads, gate_logits, unfiltered_maps, step_logits, prior_heads_window, prior_maps_window, accepted, proposal_run, prior_state_value, previous_head_input, previous_input_maps, previous_log_decays, head_input_kernel, state_maps_kernel, step_size_bias, head_decay_speed, head_direct_gain, grouped_norm_gain):
    seqs, props, width = unfiltered_heads.shape
    heads = step_logits.shape[2]
    groups = unfiltered_maps.shape[3] // STATE
    repeat = heads // groups
    tail_x = pick_tail(prior_heads_window, accepted)
    tail_bc = pick_tail(prior_maps_window, accepted)
    window_x = jnp.concatenate([tail_x, unfiltered_heads.astype(jnp.float32)], axis=1)
    window_bc = jnp.concatenate([tail_bc, unfiltered_maps.astype(jnp.float32)], axis=1)
    current_heads_window = window_x.astype(jnp.bfloat16)
    current_maps_window = window_bc.astype(jnp.bfloat16)
    x_conv = causal_conv(window_x, head_input_kernel.astype(jnp.float32)).reshape(seqs, props, heads, HEAD_DIM)
    bc_conv = causal_conv(window_bc, state_maps_kernel.astype(jnp.float32)).reshape(seqs, props, 2, groups, STATE)
    b_conv = bc_conv[:, :, 0]
    c_conv = bc_conv[:, :, 1]
    positive_step_size = jax.nn.softplus(step_logits + step_size_bias)
    logarithm_decay = proposal_run - head_decay_speed * positive_step_size
    weighted = positive_step_size[..., None] * x_conv
    current_head_input = weighted.reshape(seqs, props, width).astype(jnp.bfloat16)
    current_input_maps = b_conv.reshape(seqs, props, groups * STATE).astype(jnp.bfloat16)
    past_heads = previous_head_input.astype(jnp.float32).reshape(seqs, props, heads, HEAD_DIM)
    past_keys = jnp.repeat(previous_input_maps.astype(jnp.float32).reshape(seqs, props, groups, STATE), repeat, axis=2)
    carried = prior_state_value
    for position in range(props):
        keep = (position < accepted).astype(jnp.float32)[:, None]
        factor = jnp.exp(keep * previous_log_decays[:, position])
        update = past_heads[:, position, :, :, None] * past_keys[:, position, :, None, :]
        carried = carried * factor[:, :, None, None] + keep[:, :, None, None] * update
    cumulative = jnp.cumsum(logarithm_decay, axis=1)
    c_heads = jnp.repeat(c_conv, repeat, axis=2)
    b_heads = jnp.repeat(b_conv, repeat, axis=2)
    from_state = jnp.exp(cumulative)[..., None] * jnp.einsum('sthn,shpn->sthp', c_heads, carried, precision=lax.Precision.HIGHEST)
    order = jnp.arange(props)
    causal = (order[:, None] >= order[None, :])[None, :, :, None]
    spread_log = cumulative[:, :, None, :] - cumulative[:, None, :, :]
    decay = jnp.where(causal, jnp.exp(jnp.where(causal, spread_log, 0.0)), 0.0)
    scores = jnp.einsum('sthn,suhn->stuh', c_heads, b_heads, precision=lax.Precision.HIGHEST) * decay
    within = jnp.einsum('stuh,suhp->sthp', scores, weighted, precision=lax.Precision.HIGHEST)
    heads_out = from_state + within + head_direct_gain[:, None] * x_conv
    gated = heads_out.reshape(seqs, props, width) * jax.nn.silu(gate_logits)
    grouped = gated.reshape(seqs, props, groups, width // groups)
    grouped = grouped * lax.rsqrt(lax.optimization_barrier(jnp.mean(grouped * grouped, axis=-1, keepdims=True)) + eps)
    normalized_input = (grouped.reshape(seqs, props, width) * grouped_norm_gain.astype(jnp.float32)).astype(jnp.bfloat16)
    return (normalized_input, carried, current_head_input, current_input_maps, logarithm_decay, current_heads_window, current_maps_window)

def reference(tokens, input_norm_gain, head_input_weight, output_gate_weight, state_maps_weight, step_size_weight, step_size_bias, head_decay_speed, proposal_decay_total, head_input_kernel, state_maps_kernel, head_direct_gain, grouped_norm_gain, output_weight, prior_state_value, previous_head_input, previous_input_maps, previous_log_decays, prior_heads_window, prior_maps_window, accepted):
    values = tokens.astype(jnp.float32)
    inv_rms = lax.rsqrt(lax.optimization_barrier(jnp.sum(values * values, axis=-1)) / D + eps).reshape(BATCH * PROPOSALS, 1)
    scaled = (values * input_norm_gain.astype(jnp.float32)).astype(jnp.bfloat16).reshape(BATCH * PROPOSALS, D)
    w_all = jnp.concatenate([head_input_weight, output_gate_weight, state_maps_weight.reshape(D, 2 * BC_WIDTH), step_size_weight], axis=1)
    feat_block = D // N_KV
    proj = jnp.zeros((BATCH * PROPOSALS, w_all.shape[1]), jnp.float32)
    for kv_part in range(N_KV):
        partial_value = jnp.dot(scaled[:, kv_part * feat_block:(kv_part + 1) * feat_block], w_all[kv_part * feat_block:(kv_part + 1) * feat_block], preferred_element_type=jnp.float32)
        proj = proj + partial_value.astype(jnp.bfloat16).astype(jnp.float32)
    proj_x = proj[:, 0:INNER]
    proj_gate = proj[:, INNER:2 * INNER]
    proj_bc = proj[:, 2 * INNER:2 * INNER + 2 * BC_WIDTH]
    proj_step = proj[:, 2 * INNER + 2 * BC_WIDTH:]
    unfiltered_heads = (proj_x * inv_rms).astype(jnp.bfloat16).reshape(BATCH, PROPOSALS, INNER)
    gate_logits = (proj_gate * inv_rms).reshape(BATCH, PROPOSALS, INNER)
    unfiltered_maps = (proj_bc * inv_rms).astype(jnp.bfloat16).reshape(BATCH, PROPOSALS, 2, BC_WIDTH)
    step_logits = (proj_step * inv_rms).reshape(BATCH, PROPOSALS, HEADS)

    def single_sequence(items):
        outs = local_mixer_output(*(item[None] for item in items), head_input_kernel, state_maps_kernel, step_size_bias, head_decay_speed, head_direct_gain, grouped_norm_gain)
        return tuple((out[0] for out in outs))
    normalized_input, accepted_state, current_head_input, current_input_maps, current_log_decays, current_heads_window, current_maps_window = lax.map(single_sequence, (unfiltered_heads, gate_logits, unfiltered_maps, step_logits, prior_heads_window, prior_maps_window, accepted, proposal_decay_total, prior_state_value, previous_head_input, previous_input_maps, previous_log_decays))
    block = INNER // N_TP
    flat = normalized_input.reshape(BATCH * PROPOSALS, INNER)
    total = jnp.zeros((BATCH * PROPOSALS, D), jnp.float32)
    for part_index in range(N_TP):
        partial_value = jnp.dot(flat[:, part_index * block:(part_index + 1) * block], output_weight[part_index * block:(part_index + 1) * block], preferred_element_type=jnp.float32)
        total = total + partial_value.astype(jnp.bfloat16).astype(jnp.float32)
    mixed = total.astype(jnp.bfloat16).reshape(BATCH, PROPOSALS, D)
    return (mixed, accepted_state, current_head_input, current_input_maps, current_log_decays, current_heads_window, current_maps_window)
```

```python
import functools

import jax
import jax.numpy as jnp
from jax import lax
from jax.experimental import pallas as pl
from jax.experimental.pallas import tpu as pltpu
from jax.sharding import PartitionSpec as P

MESH = pl.DeviceIdType.MESH
HI = lax.Precision.HIGHEST
f32, bf16, i32 = jnp.float32, jnp.bfloat16, jnp.int32

NX, NZ, NT = 4, 8, 2
PEERS = NX * NZ
D, STATE, HEAD_DIM = 2048, 128, 64
SEQS, PROPS, ROWS = 2, 4, 8
HEADS, GROUPS, PER = 24, 4, 6
WIDTH, GW = 1536, 384
BC = 512
eps = 1e-06


def iota(shape, dim):
    return lax.broadcasted_iota(i32, shape, dim)


def mm(a, b, ca=1, cb=0, precision=None):
    return lax.dot_general(
        a, b, (((ca,), (cb,)), ((), ())), precision=precision, preferred_element_type=f32
    )


def heads_selection(acc):
    shape = (48, 24)
    i, j = iota(shape, 0), iota(shape, 1)
    out = i >= 32
    b = jnp.where(out, i & 1, (i >> 2) & 1)
    pos = jnp.where(out, (i - 32) >> 1, (i & 3) + (i >> 3))
    acc_b = jnp.where(b == 0, acc[0], acc[1])
    old = (j < 14) & ((j & 1) == b) & ((j >> 1) == acc_b + pos)
    raw = (j >= 16) & (((j - 16) >> 2) == b) & (((j - 16) & 3) == pos - 3)
    pick = jnp.where(pos < 3, jnp.where(old, 1.0, 0.0), jnp.where(raw, 1.0, 0.0))
    return pick.astype(bf16)


def maps_selection(acc):
    shape = (96, 48)
    i, j = iota(shape, 0), iota(shape, 1)
    out = i >= 64
    o = i - 64
    ob = jnp.where(o >= 14, 1, 0)
    orem = o - 14 * ob
    b = jnp.where(out, ob, (i >> 2) & 1)
    pos = jnp.where(out, orem >> 1, (i & 3) + (i >> 4))
    kind = jnp.where(out, orem & 1, (i >> 3) & 1)
    acc_b = jnp.where(b == 0, acc[0], acc[1])
    jb = jnp.where(j >= 14, 1, 0)
    jrem = j - 14 * jb
    old = (j < 28) & (jb == b) & ((jrem & 1) == kind) & ((jrem >> 1) == acc_b + pos)
    jr = j - 32
    raw = (j >= 32) & ((jr >> 3) == kind) & (((jr >> 2) & 1) == b) & ((jr & 3) == pos - 3)
    pick = jnp.where(pos < 3, jnp.where(old, 1.0, 0.0), jnp.where(raw, 1.0, 0.0))
    return pick.astype(bf16)


def kernel(
    tok_h, gain_h, wx_h, wg_h, smw_h, sw_h, ssb_h, hds_h, pdt_h, hik_h, smk_h, hdg_h, gng_h, wo_h,
    psv_h, phi_h, pim_h, pld_h, phw_h, pmw_h, acc_s,
    mixed_o, state_o, chi_o, cim_o, cld_o, chw_o, cmw_o,
    tok, gain, wx, wg, smw, ssb, hds, pdt, hik, smk, hdg, gng, wo, psv, phi, pim, pld, phw, pmw,
    sw, bcs, tt, wb, wxr, wgr, s0, s1, s2, r0, r1, r2, wor, sb, nrm, fs, fr,
    lsem, ssem, rsem, osem,
):
    y, kv, t = lax.axis_index("dp"), lax.axis_index("kv"), lax.axis_index("tp")
    z, x = kv // NX, kv % NX

    def at(zz, xx, tt_):
        return dict(device_id=(y, zz * NX + xx, tt_), device_id_type=MESH)

    loads = {}
    plan = (
        (tok_h, tok), (gain_h, gain), (smw_h, smw), (wx_h, wx), (wg_h, wg),
        (sw_h.at[:, pl.ds(pl.multiple_of(z * 256, 256), 256)], sw.at[pl.ds(0, 48)]),
        (ssb_h, ssb), (hds_h, hds), (pdt_h, pdt),
        (hik_h.at[:, pl.ds(pl.multiple_of(t * WIDTH, 128), WIDTH)], hik),
        (smk_h.at[:, :, pl.ds(pl.multiple_of(t * BC, 128), BC)], smk),
        (hdg_h, hdg), (gng_h, gng), (wo_h, wo), (phi_h, phi), (pim_h, pim), (pld_h, pld),
        (phw_h, phw), (pmw_h, pmw), (psv_h, psv),
    )
    for n, (src, dst) in enumerate(plan):
        loads[n] = pltpu.make_async_copy(src, dst, lsem.at[n])
        loads[n].start()

    barrier = pltpu.get_barrier_semaphore()

    def greet(d, _):
        other = lax.rem(kv + d, PEERS)
        pl.semaphore_signal(barrier, inc=1, device_id=(y, other, t), device_id_type=MESH)
        return 0

    lax.fori_loop(1, PEERS, greet, 0)
    for d in range(NX):
        pl.semaphore_signal(barrier, inc=1, **at(z, lax.rem(x + d, NX), 1 - t))

    for n in (0, 1, 2):
        loads[n].wait()
    tok32 = tok[...].astype(f32).reshape(256, 64)
    sumsq = jnp.sum(tok32 * tok32, axis=1, keepdims=True)
    gains = gain[...].astype(f32).reshape(16, 128)
    gain_row = jnp.sum(
        jnp.where(iota((16, 128), 0) == kv // 2, gains, 0.0), axis=0, keepdims=True
    )
    gain_row = jnp.where(kv % 2 == 0, gain_row[:, :64], gain_row[:, 64:])
    tt[x] = (tok32 * gain_row).astype(bf16).T
    b_w, c_w = smw[:, 0, :], smw[:, 1, :]
    for g in range(GROUPS):
        bcs[g, :, 0:128] = b_w[:, g * 128 : g * 128 + 128]
        bcs[g, :, 128:256] = c_w[:, g * 128 : g * 128 + 128]
    wb[x] = bcs[x]
    sw[48:128] = jnp.zeros((80, 256), bf16)
    loads[3].wait()
    loads[4].wait()
    own = pl.ds(pl.multiple_of(x * GW, 128), GW)
    wxr[x] = wx[:, own]
    wgr[x] = wg[:, own]

    pl.semaphore_wait(barrier, PEERS - 1 + NX)

    for n, d in enumerate((2, 1, 3)):
        xp = lax.rem(x + d, NX)
        pltpu.make_async_remote_copy(
            tt.at[x], tt.at[x], ssem.at[0], rsem.at[0], **at(z, xp, t)
        ).start()
        pltpu.make_async_remote_copy(
            bcs.at[xp], wb.at[x], ssem.at[1], rsem.at[1], **at(z, xp, t)
        ).start()
    for n, (src, dst) in enumerate(((wx, wxr), (wg, wgr))):
        for d in (2, 1, 3):
            xp = lax.rem(x + d, NX)
            pltpu.make_async_remote_copy(
                src.at[:, pl.ds(pl.multiple_of(xp * GW, 128), GW)],
                dst.at[x],
                ssem.at[2 + n],
                rsem.at[2 + n],
                **at(z, xp, t),
            ).start()

    def arrived(buffer, count, sem):
        block = buffer.at[pl.ds(0, count)]
        pltpu.make_async_copy(block, block, sem).wait()

    def spread(c, src, dst):
        def one(d, _):
            other = lax.rem(kv + d, PEERS)
            pltpu.make_async_remote_copy(
                src.at[other],
                dst.at[x * NZ + z],
                ssem.at[4 + c],
                rsem.at[4 + c],
                device_id=(y, other, t),
                device_id_type=MESH,
            ).start()
            return 0

        lax.fori_loop(1, PEERS, one, 0)
        dst[x * NZ + z] = src[kv]

    loads[5].wait()
    arrived(tt, 3, rsem.at[0])
    arrived(wb, 3, rsem.at[1])
    lhs = tt[...].reshape(256, 256)
    part = mm(lhs, wb[...].reshape(256, 256), 0, 0)
    steps = mm(lhs, sw[...], 0, 1)
    high = sumsq.astype(bf16).astype(f32)
    lane = iota((256, 128), 1)
    steps = jnp.where(lane == 64, high, jnp.where(lane == 65, sumsq - high, steps))
    s0[:, :, 0:256] = part.reshape(PEERS, ROWS, 256).astype(bf16)
    s0[:, :, 256:384] = steps.reshape(PEERS, ROWS, 128).astype(bf16)
    spread(0, s0, r0)
    arrived(wxr, 3, rsem.at[2])
    s1[...] = mm(tt[...].reshape(256, 256), wxr[...].reshape(256, GW), 0, 0).reshape(
        PEERS, ROWS, GW
    ).astype(bf16)
    spread(1, s1, r1)
    arrived(wgr, 3, rsem.at[3])
    s2[...] = mm(tt[...].reshape(256, 256), wgr[...].reshape(256, GW), 0, 0).reshape(
        PEERS, ROWS, GW
    ).astype(bf16)
    spread(2, s2, r2)
    loads[13].wait()
    wor[x] = wo[...]
    for d in (2, 1, 3):
        pltpu.make_async_remote_copy(
            wo, wor.at[x], ssem.at[7], rsem.at[7], **at(z, lax.rem(x + d, NX), t)
        ).start()

    acc = (acc_s[0], acc_s[1])
    row = iota((ROWS, 1), 0)
    acc_row = jnp.where(row < PROPS, acc[0], acc[1])
    keep = jnp.where((row & 3) < acc_row, 1.0, 0.0)
    r8, c8 = iota((ROWS, ROWS), 0), iota((ROWS, ROWS), 1)
    same = (r8 >> 2) == (c8 >> 2)
    expand = jnp.where(iota((HEADS, WIDTH), 1) // HEAD_DIM == iota((HEADS, WIDTH), 0), 1.0, 0.0)
    for n in (14, 15, 16):
        loads[n].wait()
    kept = pld[...].reshape(ROWS, HEADS) * keep
    later = mm(jnp.where(same & (c8 > r8), 1.0, 0.0), kept, precision=HI)
    coef = mm(keep * jnp.exp(later), expand, precision=HI)
    scaled = coef * phi[...].astype(f32).reshape(ROWS, WIDTH)
    s_hi = scaled.astype(bf16)
    s_lo = (scaled - s_hi.astype(f32)).astype(bf16)
    updates = jnp.concatenate([s_hi.astype(f32), s_lo.astype(f32)], axis=0).astype(bf16)
    keys = pim[...].astype(f32).reshape(ROWS, BC)
    loads[19].wait()
    for b in range(SEQS):
        mine = (row >> 2) == b
        logs = mm(jnp.where(mine, kept, 0.0), jnp.ones((ROWS, STATE), f32), 0, 0, precision=HI)
        factor = jnp.exp(logs)
        keys_b = jnp.where(mine, keys, 0.0)
        keys_b = jnp.concatenate([keys_b, keys_b], axis=0).astype(bf16)
        for g in range(GROUPS):
            upd = mm(
                updates[:, g * GW : g * GW + GW], keys_b[:, g * STATE : g * STATE + STATE], 0, 0
            )
            new = (
                psv[b, g * PER : g * PER + PER] * factor[g * PER : g * PER + PER][:, None, :]
                + upd.reshape(PER, HEAD_DIM, STATE)
            )
            psv[b, g * PER : g * PER + PER] = new
            sb[b, g] = new.reshape(GW, STATE).astype(bf16)
    state_out = pltpu.make_async_copy(psv, state_o, osem.at[0])
    state_out.start()

    pick_x, pick_bc = heads_selection(acc), maps_selection(acc)
    for n in (6, 7, 8, 9, 10, 11, 12, 17, 18):
        loads[n].wait()
    old_x = phw[...].astype(f32).reshape(14, WIDTH)
    old_x = jnp.concatenate([old_x, jnp.zeros((2, WIDTH), f32)], axis=0)
    old_bc = pmw[...].astype(f32).reshape(28, BC)
    old_bc = jnp.concatenate([old_bc, jnp.zeros((4, BC), f32)], axis=0)
    taps_x = hik[...].astype(f32)
    taps_bc = smk[...].astype(f32).reshape(8, BC)

    def own_heads(ref):
        v = ref[...].reshape(1, 2 * HEADS)
        return jnp.where(t == 0, v[:, :HEADS], v[:, HEADS:])

    speed, direct, bias = own_heads(hds), own_heads(hdg), own_heads(ssb)
    gngv = gng[...].astype(f32).reshape(1, 2 * WIDTH)
    out_gain = jnp.where(t == 0, gngv[:, :WIDTH], gngv[:, WIDTH:])

    arrived(r0, PEERS - 1, rsem.at[4])
    sum0 = jnp.sum(r0[...].astype(f32).reshape(NX, NZ, ROWS, GW), axis=1)
    tail = sum0[:, :, 256:384]
    squares = jnp.sum(tail, axis=0)
    lane8 = iota((ROWS, 128), 1)
    squares = jnp.sum(
        jnp.where((lane8 == 64) | (lane8 == 65), squares, 0.0), axis=1, keepdims=True
    )
    inv = lax.rsqrt(squares / D + eps)
    raw_b = jnp.concatenate([sum0[g, :, 0:128] for g in range(GROUPS)], axis=1) * inv
    raw_c = jnp.concatenate([sum0[g, :, 128:256] for g in range(GROUPS)], axis=1) * inv
    win_bc = mm(pick_bc, jnp.concatenate([old_bc, raw_b, raw_c], axis=0).astype(bf16))
    cmw_v = win_bc[64:92].reshape(SEQS, 7, 2, BC).astype(bf16)
    b_conv = taps_bc[0:1] * win_bc[0:8]
    c_conv = taps_bc[1:2] * win_bc[8:16]
    for k in range(1, 4):
        b_conv = b_conv + taps_bc[2 * k : 2 * k + 1] * win_bc[16 * k : 16 * k + 8]
        c_conv = c_conv + taps_bc[2 * k + 1 : 2 * k + 2] * win_bc[16 * k + 8 : 16 * k + 16]
    b_conv = b_conv * lax.logistic(b_conv)
    c_conv = c_conv * lax.logistic(c_conv)
    step_pre = tail[0] * inv
    step_pre = jnp.where(t == 0, step_pre[:, :HEADS], step_pre[:, HEADS : 2 * HEADS]) + bias
    step = jnp.maximum(step_pre, 0.0) + jnp.log1p(jnp.exp(-jnp.abs(step_pre)))
    decays = pdt[...].reshape(ROWS, HEADS) - speed * step
    cum = mm(jnp.where(same & (c8 <= r8), 1.0, 0.0), decays, precision=HI)
    wide = mm(
        jnp.concatenate([cum, step, jnp.broadcast_to(direct, (ROWS, HEADS))], axis=0),
        expand,
        precision=HI,
    )
    cum_w, step_w, direct_w = wide[0:8], wide[8:16], wide[16:24]
    cim_o[...] = b_conv.reshape(SEQS, PROPS, BC).astype(bf16)
    cld_o[...] = decays.reshape(SEQS, PROPS, HEADS)
    cmw_o[...] = cmw_v
    from_state, pairs = [], []
    for g in range(GROUPS):
        lanes = slice(g * STATE, g * STATE + STATE)
        c_g = c_conv[:, lanes]
        y0 = mm(c_g.astype(bf16), sb[0, g], 1, 1)
        y1 = mm(c_g.astype(bf16), sb[1, g], 1, 1)
        from_state.append(jnp.where(row < PROPS, y0, y1))
        pairs.append(mm(c_g, b_conv[:, lanes], 1, 1, precision=HI))
    from_state = jnp.exp(cum_w) * jnp.concatenate(from_state, axis=1)

    arrived(r1, PEERS - 1, rsem.at[5])
    sum1 = jnp.sum(r1[...].astype(f32).reshape(NX, NZ, ROWS, GW), axis=1)
    raw_x = jnp.concatenate([sum1[g] for g in range(GROUPS)], axis=1) * inv
    win_x = mm(pick_x, jnp.concatenate([old_x, raw_x], axis=0).astype(bf16))
    chw_o[...] = win_x[32:46].reshape(7, SEQS, WIDTH).astype(bf16)
    x_conv = taps_x[0:1] * win_x[0:8]
    for k in range(1, 4):
        x_conv = x_conv + taps_x[k : k + 1] * win_x[8 * k : 8 * k + 8]
    x_conv = x_conv * lax.logistic(x_conv)
    weighted = step_w * x_conv
    chi_o[...] = weighted.reshape(SEQS, PROPS, WIDTH).astype(bf16)
    total = from_state + direct_w * x_conv
    for d in range(PROPS):
        score = [
            jnp.broadcast_to(
                jnp.sum(jnp.where(c8 == r8 - d, p, 0.0), axis=1, keepdims=True), (ROWS, GW)
            )
            for p in pairs
        ]
        score = jnp.concatenate(score, axis=1)
        if d == 0:
            total = total + score * weighted
        else:
            valid = (row & 3) >= d
            gap = jnp.where(valid, cum_w - pltpu.roll(cum_w, d, 0), 0.0)
            term = jnp.exp(gap) * score * pltpu.roll(weighted, d, 0)
            total = total + jnp.where(valid, term, 0.0)

    arrived(r2, PEERS - 1, rsem.at[6])
    sum2 = jnp.sum(r2[...].astype(f32).reshape(NX, NZ, ROWS, GW), axis=1)
    gate = jnp.concatenate([sum2[g] for g in range(GROUPS)], axis=1) * inv
    gated = total * (gate * lax.logistic(gate))
    normed = []
    for g in range(GROUPS):
        part_g = gated[:, g * GW : g * GW + GW]
        mean = jnp.sum(part_g * part_g, axis=1, keepdims=True) / GW
        normed.append(part_g * lax.rsqrt(mean + eps))
    nrm[z] = (jnp.concatenate(normed, axis=1) * out_gain).astype(bf16)
    for d in (4, 3, 5, 2, 6, 1, 7):
        pltpu.make_async_remote_copy(
            nrm.at[z], nrm.at[z], ssem.at[8], rsem.at[8], **at(lax.rem(z + d, NZ), x, t)
        ).start()

    arrived(wor, 3, rsem.at[7])
    arrived(nrm, 7, rsem.at[8])
    rows64 = nrm[...].astype(f32).reshape(64, WIDTH).astype(bf16)
    for d in (2, 1, 3, 0):
        xp = lax.rem(x + d, NX)
        fs[d] = mm(rows64, wor[xp], 1, 1).astype(bf16)
        if d == 0:
            fr[x * NT + t] = fs[0]
        else:
            pltpu.make_async_remote_copy(
                fs.at[d], fr.at[x * NT + t], ssem.at[9], rsem.at[9], **at(z, xp, t)
            ).start()
        pltpu.make_async_remote_copy(
            fs.at[d], fr.at[x * NT + t], ssem.at[9], rsem.at[9], **at(z, xp, 1 - t)
        ).start()
    arrived(fr, 7, rsem.at[9])
    done = fr[...].astype(f32).reshape(NX, NT, 64, 64)
    done = (done[:, 0] + done[:, 1]).reshape(NX, NZ, ROWS, 64)
    done = jnp.stack([done[:, n] for n in range(NZ)], axis=0)
    mixed_o[...] = done.reshape(64, PROPS, 64).astype(bf16)

    arrived(tt, 3, ssem.at[0])
    arrived(wb, 3, ssem.at[1])
    arrived(wxr, 3, ssem.at[2])
    arrived(wgr, 3, ssem.at[3])
    arrived(s0, PEERS - 1, ssem.at[4])
    arrived(s1, PEERS - 1, ssem.at[5])
    arrived(s2, PEERS - 1, ssem.at[6])
    arrived(wor, 3, ssem.at[7])
    arrived(nrm, 7, ssem.at[8])
    arrived(fr, 7, ssem.at[9])
    state_out.wait()


def local(
    tokens, input_norm_gain, head_input_weight, output_gate_weight, state_maps_weight,
    step_size_weight, step_size_bias, head_decay_speed, proposal_decay_total, head_input_kernel,
    state_maps_kernel, head_direct_gain, grouped_norm_gain, output_weight, prior_state_value,
    previous_head_input, previous_input_maps, previous_log_decays, prior_heads_window,
    prior_maps_window, accepted,
):
    anywhere = pl.BlockSpec(memory_space=pl.ANY)
    vmem = pl.BlockSpec(memory_space=pltpu.VMEM)
    V, DMA = pltpu.VMEM, pltpu.SemaphoreType.DMA
    outs = (
        jax.ShapeDtypeStruct((64, PROPS, 64), bf16),
        jax.ShapeDtypeStruct((SEQS, HEADS, HEAD_DIM, STATE), f32),
        jax.ShapeDtypeStruct((SEQS, PROPS, WIDTH), bf16),
        jax.ShapeDtypeStruct((SEQS, PROPS, BC), bf16),
        jax.ShapeDtypeStruct((SEQS, PROPS, HEADS), f32),
        jax.ShapeDtypeStruct((7, SEQS, WIDTH), bf16),
        jax.ShapeDtypeStruct((SEQS, 7, 2, BC), bf16),
    )
    mixed, state, chi, cim, cld, chw, cmw = pl.pallas_call(
        kernel,
        out_shape=outs,
        in_specs=[anywhere] * 20 + [pl.BlockSpec(memory_space=pltpu.SMEM)],
        out_specs=[vmem, anywhere, vmem, vmem, vmem, vmem, vmem],
        scratch_shapes=[
            V((64, PROPS, 64), bf16), V((D,), bf16), V((64, WIDTH), bf16), V((64, WIDTH), bf16),
            V((64, 2, BC), bf16), V((48,), f32), V((48,), f32), V((SEQS, PROPS, HEADS), f32),
            V((4, WIDTH), bf16), V((4, 2, BC), bf16), V((48,), f32), V((2 * WIDTH,), bf16),
            V((64, WIDTH), bf16), V((SEQS, HEADS, HEAD_DIM, STATE), f32),
            V((SEQS, PROPS, WIDTH), bf16), V((SEQS, PROPS, BC), bf16),
            V((SEQS, PROPS, HEADS), f32), V((7, SEQS, WIDTH), bf16), V((SEQS, 7, 2, BC), bf16),
            V((128, 256), bf16), V((NX, 64, 256), bf16), V((NX, 64, 256), bf16),
            V((NX, 64, 256), bf16), V((NX, 64, GW), bf16), V((NX, 64, GW), bf16),
            V((PEERS, ROWS, GW), bf16), V((PEERS, ROWS, GW), bf16), V((PEERS, ROWS, GW), bf16),
            V((PEERS, ROWS, GW), bf16), V((PEERS, ROWS, GW), bf16), V((PEERS, ROWS, GW), bf16),
            V((NX, 64, WIDTH), bf16), V((SEQS, GROUPS, GW, STATE), bf16),
            V((NZ, ROWS, WIDTH), bf16), V((NX, 64, 64), bf16), V((NX * NT, 64, 64), bf16),
            DMA((20,)), DMA((10,)), DMA((10,)), DMA((1,)),
        ],
        compiler_params=pltpu.CompilerParams(
            collective_id=0, has_side_effects=True, vmem_limit_bytes=40 * 1024 * 1024
        ),
    )(
        tokens, input_norm_gain, head_input_weight, output_gate_weight, state_maps_weight,
        step_size_weight.T, step_size_bias, head_decay_speed, proposal_decay_total,
        head_input_kernel, state_maps_kernel, head_direct_gain, grouped_norm_gain,
        output_weight.T, prior_state_value, previous_head_input, previous_input_maps,
        previous_log_decays, jnp.transpose(prior_heads_window, (1, 0, 2)), prior_maps_window,
        accepted,
    )
    return mixed, state, chi, cim, cld, jnp.transpose(chw, (1, 0, 2)), cmw


def solution(mesh):
    seq = ("dp", "kv")
    return jax.shard_map(
        local,
        mesh=mesh,
        in_specs=(
            P("dp", None, "kv"), P(), P("kv", "tp"), P("kv", "tp"), P("kv", None, "tp"), P(), P(),
            P(), P(seq, None, "tp"), P(), P(), P(), P(), P("tp", "kv"), P(seq, "tp", None, None),
            P(seq, None, "tp"), P(seq, None, "tp"), P(seq, None, "tp"), P(seq, None, "tp"),
            P(seq, None, None, "tp"), P(seq),
        ),
        out_specs=(
            P("dp", None, "kv"), P(seq, "tp", None, None), P(seq, None, "tp"), P(seq, None, "tp"),
            P(seq, None, "tp"), P(seq, None, "tp"), P(seq, None, None, "tp"),
        ),
        check_vma=False,
    )
```

```python
import functools

import jax
import jax.numpy as jnp
from jax import lax
from jax.experimental import pallas as pl
from jax.experimental.pallas import tpu as pltpu
from jax.sharding import PartitionSpec as P

MESH = pl.DeviceIdType.MESH
HI = lax.Precision.HIGHEST
f32, bf16, i32 = jnp.float32, jnp.bfloat16, jnp.int32

NX, NZ, NT = 4, 8, 2
PEERS = NX * NZ
D, STATE, HEAD_DIM = 2048, 128, 64
SEQS, PROPS, ROWS = 2, 4, 8
HEADS, GROUPS, PER = 24, 4, 6
WIDTH, GW = 1536, 384
BC = 512
eps = 1e-06


def iota(shape, dim):
    return lax.broadcasted_iota(i32, shape, dim)


def mm(a, b, ca=1, cb=0, precision=None):
    return lax.dot_general(
        a, b, (((ca,), (cb,)), ((), ())), precision=precision, preferred_element_type=f32
    )


def heads_selection(acc):
    shape = (48, 24)
    i, j = iota(shape, 0), iota(shape, 1)
    out = i >= 32
    b = jnp.where(out, i & 1, (i >> 2) & 1)
    pos = jnp.where(out, (i - 32) >> 1, (i & 3) + (i >> 3))
    acc_b = jnp.where(b == 0, acc[0], acc[1])
    old = (j < 14) & ((j & 1) == b) & ((j >> 1) == acc_b + pos)
    raw = (j >= 16) & (((j - 16) >> 2) == b) & (((j - 16) & 3) == pos - 3)
    pick = jnp.where(pos < 3, jnp.where(old, 1.0, 0.0), jnp.where(raw, 1.0, 0.0))
    return pick.astype(bf16)


def maps_selection(acc):
    shape = (96, 48)
    i, j = iota(shape, 0), iota(shape, 1)
    out = i >= 64
    o = i - 64
    ob = jnp.where(o >= 14, 1, 0)
    orem = o - 14 * ob
    b = jnp.where(out, ob, (i >> 2) & 1)
    pos = jnp.where(out, orem >> 1, (i & 3) + (i >> 4))
    kind = jnp.where(out, orem & 1, (i >> 3) & 1)
    acc_b = jnp.where(b == 0, acc[0], acc[1])
    jb = jnp.where(j >= 14, 1, 0)
    jrem = j - 14 * jb
    old = (j < 28) & (jb == b) & ((jrem & 1) == kind) & ((jrem >> 1) == acc_b + pos)
    jr = j - 32
    raw = (j >= 32) & ((jr >> 3) == kind) & (((jr >> 2) & 1) == b) & ((jr & 3) == pos - 3)
    pick = jnp.where(pos < 3, jnp.where(old, 1.0, 0.0), jnp.where(raw, 1.0, 0.0))
    return pick.astype(bf16)


def kernel(
    tok_h, gain_h, wx_h, wg_h, smw_h, sw_h, ssb_h, hds_h, pdt_h, hik_h, smk_h, hdg_h, gng_h, wo_h,
    psv_h, phi_h, pim_h, pld_h, phw_h, pmw_h, acc_h,
    fr, state_o, chi_o, cim_o, cld_o, chw_o, cmw_o,
    tok, gain, wx, wg, smw, ssb, hds, pdt, hik, smk, hdg, gng, wo, psv, phi, pim, pld, phw, pmw,
    sw, bcs, tt, wb, wxr, wgr, s0, s1, s2, r0, r1, r2, wor, sb, nrm, fs,
    chi, cim, cld, chw, cmw, acc_s, lsem, ssem, rsem, osem,
):
    y, kv, t = lax.axis_index("dp"), lax.axis_index("kv"), lax.axis_index("tp")
    z, x = kv // NX, kv % NX

    def at(zz, xx, tt_):
        return dict(device_id=(y, zz * NX + xx, tt_), device_id_type=MESH)

    loads = {}
    plan = (
        (tok_h, tok), (gain_h, gain), (smw_h, smw), (wx_h, wx), (wg_h, wg),
        (sw_h.at[:, pl.ds(pl.multiple_of(z * 256, 256), 256)], sw.at[pl.ds(0, 48)]),
        (ssb_h, ssb), (hds_h, hds), (pdt_h, pdt),
        (hik_h.at[:, pl.ds(pl.multiple_of(t * WIDTH, 128), WIDTH)], hik),
        (smk_h.at[:, :, pl.ds(pl.multiple_of(t * BC, 128), BC)], smk),
        (hdg_h, hdg), (gng_h, gng), (wo_h, wo), (phi_h, phi), (pim_h, pim), (pld_h, pld),
        (phw_h, phw), (pmw_h, pmw), (psv_h, psv), (acc_h, acc_s),
    )
    for n, (src, dst) in enumerate(plan):
        loads[n] = pltpu.make_async_copy(src, dst, lsem.at[n])
        loads[n].start()

    barrier = pltpu.get_barrier_semaphore()

    def greet(d, _):
        other = lax.rem(kv + d, PEERS)
        pl.semaphore_signal(barrier, inc=1, device_id=(y, other, t), device_id_type=MESH)
        return 0

    lax.fori_loop(1, PEERS, greet, 0)
    for d in range(NX):
        pl.semaphore_signal(barrier, inc=1, **at(z, lax.rem(x + d, NX), 1 - t))

    for n in (0, 1, 2):
        loads[n].wait()
    tok32 = tok[...].astype(f32).reshape(256, 64)
    sumsq = jnp.sum(tok32 * tok32, axis=1, keepdims=True)
    gains = gain[...].astype(f32).reshape(16, 128)
    gain_row = jnp.sum(
        jnp.where(iota((16, 128), 0) == kv // 2, gains, 0.0), axis=0, keepdims=True
    )
    gain_row = jnp.where(kv % 2 == 0, gain_row[:, :64], gain_row[:, 64:])
    tt[x] = (tok32 * gain_row).astype(bf16).T
    b_w, c_w = smw[:, 0, :], smw[:, 1, :]
    for g in range(GROUPS):
        bcs[g, :, 0:128] = b_w[:, g * 128 : g * 128 + 128]
        bcs[g, :, 128:256] = c_w[:, g * 128 : g * 128 + 128]
    wb[x] = bcs[x]
    sw[48:128] = jnp.zeros((80, 256), bf16)
    loads[3].wait()
    loads[4].wait()
    own = pl.ds(pl.multiple_of(x * GW, 128), GW)
    wxr[x] = wx[:, own]
    wgr[x] = wg[:, own]

    pl.semaphore_wait(barrier, PEERS - 1 + NX)

    for n, d in enumerate((2, 1, 3)):
        xp = lax.rem(x + d, NX)
        pltpu.make_async_remote_copy(
            tt.at[x], tt.at[x], ssem.at[0], rsem.at[0], **at(z, xp, t)
        ).start()
        pltpu.make_async_remote_copy(
            bcs.at[xp], wb.at[x], ssem.at[1], rsem.at[1], **at(z, xp, t)
        ).start()
    for n, (src, dst) in enumerate(((wx, wxr), (wg, wgr))):
        for d in (2, 1, 3):
            xp = lax.rem(x + d, NX)
            pltpu.make_async_remote_copy(
                src.at[:, pl.ds(pl.multiple_of(xp * GW, 128), GW)],
                dst.at[x],
                ssem.at[2 + n],
                rsem.at[2 + n],
                **at(z, xp, t),
            ).start()

    def arrived(buffer, count, sem):
        block = buffer.at[pl.ds(0, count)]
        pltpu.make_async_copy(block, block, sem).wait()

    def spread(c, src, dst):
        def one(d, _):
            other = lax.rem(kv + d, PEERS)
            pltpu.make_async_remote_copy(
                src.at[other],
                dst.at[x * NZ + z],
                ssem.at[4 + c],
                rsem.at[4 + c],
                device_id=(y, other, t),
                device_id_type=MESH,
            ).start()
            return 0

        lax.fori_loop(1, PEERS, one, 0)
        dst[x * NZ + z] = src[kv]

    loads[5].wait()
    arrived(tt, 3, rsem.at[0])
    arrived(wb, 3, rsem.at[1])
    lhs = tt[...].reshape(256, 256)
    part = mm(lhs, wb[...].reshape(256, 256), 0, 0)
    steps = mm(lhs, sw[...], 0, 1)
    high = sumsq.astype(bf16).astype(f32)
    lane = iota((256, 128), 1)
    steps = jnp.where(lane == 64, high, jnp.where(lane == 65, sumsq - high, steps))
    s0[:, :, 0:256] = part.reshape(PEERS, ROWS, 256).astype(bf16)
    s0[:, :, 256:384] = steps.reshape(PEERS, ROWS, 128).astype(bf16)
    spread(0, s0, r0)
    arrived(wxr, 3, rsem.at[2])
    s1[...] = mm(tt[...].reshape(256, 256), wxr[...].reshape(256, GW), 0, 0).reshape(
        PEERS, ROWS, GW
    ).astype(bf16)
    spread(1, s1, r1)
    arrived(wgr, 3, rsem.at[3])
    s2[...] = mm(tt[...].reshape(256, 256), wgr[...].reshape(256, GW), 0, 0).reshape(
        PEERS, ROWS, GW
    ).astype(bf16)
    spread(2, s2, r2)
    loads[13].wait()
    wor[x] = wo[...]
    for d in (2, 1, 3):
        pltpu.make_async_remote_copy(
            wo, wor.at[x], ssem.at[7], rsem.at[7], **at(z, lax.rem(x + d, NX), t)
        ).start()

    loads[20].wait()
    acc = (acc_s[0], acc_s[1])
    row = iota((ROWS, 1), 0)
    acc_row = jnp.where(row < PROPS, acc[0], acc[1])
    keep = jnp.where((row & 3) < acc_row, 1.0, 0.0)
    r8, c8 = iota((ROWS, ROWS), 0), iota((ROWS, ROWS), 1)
    same = (r8 >> 2) == (c8 >> 2)
    expand = jnp.where(iota((HEADS, WIDTH), 1) // HEAD_DIM == iota((HEADS, WIDTH), 0), 1.0, 0.0)
    for n in (14, 15, 16):
        loads[n].wait()
    kept = pld[...].reshape(ROWS, HEADS) * keep
    later = mm(jnp.where(same & (c8 > r8), 1.0, 0.0), kept, precision=HI)
    coef = mm(keep * jnp.exp(later), expand, precision=HI)
    scaled = coef * phi[...].astype(f32).reshape(ROWS, WIDTH)
    s_hi = scaled.astype(bf16)
    s_lo = (scaled - s_hi.astype(f32)).astype(bf16)
    updates = jnp.concatenate([s_hi.astype(f32), s_lo.astype(f32)], axis=0).astype(bf16)
    keys = pim[...].astype(f32).reshape(ROWS, BC)
    loads[19].wait()
    for b in range(SEQS):
        mine = (row >> 2) == b
        logs = mm(jnp.where(mine, kept, 0.0), jnp.ones((ROWS, STATE), f32), 0, 0, precision=HI)
        factor = jnp.exp(logs)
        keys_b = jnp.where(mine, keys, 0.0)
        keys_b = jnp.concatenate([keys_b, keys_b], axis=0).astype(bf16)
        for g in range(GROUPS):
            upd = mm(
                updates[:, g * GW : g * GW + GW], keys_b[:, g * STATE : g * STATE + STATE], 0, 0
            )
            new = (
                psv[b, g * PER : g * PER + PER] * factor[g * PER : g * PER + PER][:, None, :]
                + upd.reshape(PER, HEAD_DIM, STATE)
            )
            psv[b, g * PER : g * PER + PER] = new
            sb[b, g] = new.reshape(GW, STATE).astype(bf16)
    outs = []

    def put(n, src, dst):
        outs.append(pltpu.make_async_copy(src, dst, osem.at[n]))
        outs[-1].start()

    put(0, psv, state_o)

    pick_x, pick_bc = heads_selection(acc), maps_selection(acc)
    for n in (6, 7, 8, 9, 10, 11, 12, 17, 18):
        loads[n].wait()
    old_x = phw[...].astype(f32).reshape(14, WIDTH)
    old_x = jnp.concatenate([old_x, jnp.zeros((2, WIDTH), f32)], axis=0)
    old_bc = pmw[...].astype(f32).reshape(28, BC)
    old_bc = jnp.concatenate([old_bc, jnp.zeros((4, BC), f32)], axis=0)
    taps_x = hik[...].astype(f32)
    taps_bc = smk[...].astype(f32).reshape(8, BC)

    def own_heads(ref):
        v = ref[...].reshape(1, 2 * HEADS)
        return jnp.where(t == 0, v[:, :HEADS], v[:, HEADS:])

    speed, direct, bias = own_heads(hds), own_heads(hdg), own_heads(ssb)
    gngv = gng[...].astype(f32).reshape(1, 2 * WIDTH)
    out_gain = jnp.where(t == 0, gngv[:, :WIDTH], gngv[:, WIDTH:])

    arrived(r0, PEERS - 1, rsem.at[4])
    sum0 = jnp.sum(r0[...].astype(f32).reshape(NX, NZ, ROWS, GW), axis=1)
    tail = sum0[:, :, 256:384]
    squares = jnp.sum(tail, axis=0)
    lane8 = iota((ROWS, 128), 1)
    squares = jnp.sum(
        jnp.where((lane8 == 64) | (lane8 == 65), squares, 0.0), axis=1, keepdims=True
    )
    inv = lax.rsqrt(squares / D + eps)
    raw_b = jnp.concatenate([sum0[g, :, 0:128] for g in range(GROUPS)], axis=1) * inv
    raw_c = jnp.concatenate([sum0[g, :, 128:256] for g in range(GROUPS)], axis=1) * inv
    win_bc = mm(pick_bc, jnp.concatenate([old_bc, raw_b, raw_c], axis=0).astype(bf16))
    cmw[...] = win_bc[64:92].reshape(SEQS, 7, 2, BC).astype(bf16)
    put(1, cmw, cmw_o)
    b_conv = taps_bc[0:1] * win_bc[0:8]
    c_conv = taps_bc[1:2] * win_bc[8:16]
    for k in range(1, 4):
        b_conv = b_conv + taps_bc[2 * k : 2 * k + 1] * win_bc[16 * k : 16 * k + 8]
        c_conv = c_conv + taps_bc[2 * k + 1 : 2 * k + 2] * win_bc[16 * k + 8 : 16 * k + 16]
    b_conv = b_conv * lax.logistic(b_conv)
    c_conv = c_conv * lax.logistic(c_conv)
    step_pre = tail[0] * inv
    step_pre = jnp.where(t == 0, step_pre[:, :HEADS], step_pre[:, HEADS : 2 * HEADS]) + bias
    step = jnp.maximum(step_pre, 0.0) + jnp.log1p(jnp.exp(-jnp.abs(step_pre)))
    decays = pdt[...].reshape(ROWS, HEADS) - speed * step
    cum = mm(jnp.where(same & (c8 <= r8), 1.0, 0.0), decays, precision=HI)
    wide = mm(
        jnp.concatenate([cum, step, jnp.broadcast_to(direct, (ROWS, HEADS))], axis=0),
        expand,
        precision=HI,
    )
    cum_w, step_w, direct_w = wide[0:8], wide[8:16], wide[16:24]
    cim[...] = b_conv.reshape(SEQS, PROPS, BC).astype(bf16)
    put(2, cim, cim_o)
    cld[...] = decays.reshape(SEQS, PROPS, HEADS)
    put(3, cld, cld_o)
    from_state, pairs = [], []
    for g in range(GROUPS):
        lanes = slice(g * STATE, g * STATE + STATE)
        c_g = c_conv[:, lanes]
        y0 = mm(c_g.astype(bf16), sb[0, g], 1, 1)
        y1 = mm(c_g.astype(bf16), sb[1, g], 1, 1)
        from_state.append(jnp.where(row < PROPS, y0, y1))
        pairs.append(mm(c_g, b_conv[:, lanes], 1, 1, precision=HI))
    from_state = jnp.exp(cum_w) * jnp.concatenate(from_state, axis=1)

    arrived(r1, PEERS - 1, rsem.at[5])
    sum1 = jnp.sum(r1[...].astype(f32).reshape(NX, NZ, ROWS, GW), axis=1)
    raw_x = jnp.concatenate([sum1[g] for g in range(GROUPS)], axis=1) * inv
    win_x = mm(pick_x, jnp.concatenate([old_x, raw_x], axis=0).astype(bf16))
    chw[...] = win_x[32:46].reshape(7, SEQS, WIDTH).astype(bf16)
    put(4, chw, chw_o)
    x_conv = taps_x[0:1] * win_x[0:8]
    for k in range(1, 4):
        x_conv = x_conv + taps_x[k : k + 1] * win_x[8 * k : 8 * k + 8]
    x_conv = x_conv * lax.logistic(x_conv)
    weighted = step_w * x_conv
    chi[...] = weighted.reshape(SEQS, PROPS, WIDTH).astype(bf16)
    put(5, chi, chi_o)
    total = from_state + direct_w * x_conv
    for d in range(PROPS):
        score = [
            jnp.broadcast_to(
                jnp.sum(jnp.where(c8 == r8 - d, p, 0.0), axis=1, keepdims=True), (ROWS, GW)
            )
            for p in pairs
        ]
        score = jnp.concatenate(score, axis=1)
        if d == 0:
            total = total + score * weighted
        else:
            valid = (row & 3) >= d
            gap = jnp.where(valid, cum_w - pltpu.roll(cum_w, d, 0), 0.0)
            term = jnp.exp(gap) * score * pltpu.roll(weighted, d, 0)
            total = total + jnp.where(valid, term, 0.0)

    arrived(r2, PEERS - 1, rsem.at[6])
    sum2 = jnp.sum(r2[...].astype(f32).reshape(NX, NZ, ROWS, GW), axis=1)
    gate = jnp.concatenate([sum2[g] for g in range(GROUPS)], axis=1) * inv
    gated = total * (gate * lax.logistic(gate))
    normed = []
    for g in range(GROUPS):
        part_g = gated[:, g * GW : g * GW + GW]
        mean = jnp.sum(part_g * part_g, axis=1, keepdims=True) / GW
        normed.append(part_g * lax.rsqrt(mean + eps))
    nrm[z] = (jnp.concatenate(normed, axis=1) * out_gain).astype(bf16)
    for d in (4, 3, 5, 2, 6, 1, 7):
        pltpu.make_async_remote_copy(
            nrm.at[z], nrm.at[z], ssem.at[8], rsem.at[8], **at(lax.rem(z + d, NZ), x, t)
        ).start()

    arrived(wor, 3, rsem.at[7])
    arrived(nrm, 7, rsem.at[8])
    rows64 = nrm[...].astype(f32).reshape(64, WIDTH).astype(bf16)
    for d in (2, 1, 3, 0):
        xp = lax.rem(x + d, NX)
        fs[d] = mm(rows64, wor[xp], 1, 1).astype(bf16)
        if d == 0:
            put(6, fs.at[0], fr.at[x * NT + t])
        else:
            pltpu.make_async_remote_copy(
                fs.at[d], fr.at[x * NT + t], ssem.at[9], rsem.at[9], **at(z, xp, t)
            ).start()
        pltpu.make_async_remote_copy(
            fs.at[d], fr.at[x * NT + t], ssem.at[9], rsem.at[9], **at(z, xp, 1 - t)
        ).start()
    arrived(fr, 7, rsem.at[9])

    arrived(tt, 3, ssem.at[0])
    arrived(wb, 3, ssem.at[1])
    arrived(wxr, 3, ssem.at[2])
    arrived(wgr, 3, ssem.at[3])
    arrived(s0, PEERS - 1, ssem.at[4])
    arrived(s1, PEERS - 1, ssem.at[5])
    arrived(s2, PEERS - 1, ssem.at[6])
    arrived(wor, 3, ssem.at[7])
    arrived(nrm, 7, ssem.at[8])
    arrived(fr, 7, ssem.at[9])
    for copy in outs:
        copy.wait()


def finish(fr_h, *refs):
    ins, outs, fr, mixed = refs[:6], refs[7:13], refs[13], refs[14]
    mids, sems = refs[15:21], refs[21]
    mixed_o = refs[6]
    first = [pltpu.make_async_copy(fr_h, fr, sems.at[0])]
    first += [pltpu.make_async_copy(a, b, sems.at[n + 1]) for n, (a, b) in enumerate(zip(ins, mids))]
    for copy in first:
        copy.start()
    second = [pltpu.make_async_copy(a, b, sems.at[n + 7]) for n, (a, b) in enumerate(zip(mids, outs))]
    first[0].wait()
    done = fr[...].astype(f32).reshape(NX, NT, 64, 64)
    done = (done[:, 0] + done[:, 1]).reshape(NX, NZ, ROWS, 64)
    done = jnp.stack([done[:, n] for n in range(NZ)], axis=0)
    mixed[...] = done.reshape(64, PROPS, 64).astype(bf16)
    last = pltpu.make_async_copy(mixed, mixed_o, sems.at[13])
    last.start()
    for a, b in zip(first[1:], second):
        a.wait()
        b.start()
    for copy in second:
        copy.wait()
    last.wait()


def local(
    tokens, input_norm_gain, head_input_weight, output_gate_weight, state_maps_weight,
    step_size_weight, step_size_bias, head_decay_speed, proposal_decay_total, head_input_kernel,
    state_maps_kernel, head_direct_gain, grouped_norm_gain, output_weight, prior_state_value,
    previous_head_input, previous_input_maps, previous_log_decays, prior_heads_window,
    prior_maps_window, accepted,
):
    anywhere = pl.BlockSpec(memory_space=pl.ANY)
    V, DMA = pltpu.VMEM, pltpu.SemaphoreType.DMA
    outs = (
        jax.ShapeDtypeStruct((NX * NT, 64, 64), bf16),
        jax.ShapeDtypeStruct((SEQS, HEADS, HEAD_DIM, STATE), f32),
        jax.ShapeDtypeStruct((SEQS, PROPS, WIDTH), bf16),
        jax.ShapeDtypeStruct((SEQS, PROPS, BC), bf16),
        jax.ShapeDtypeStruct((SEQS, PROPS, HEADS), f32),
        jax.ShapeDtypeStruct((7, SEQS, WIDTH), bf16),
        jax.ShapeDtypeStruct((SEQS, 7, 2, BC), bf16),
    )
    results = pl.pallas_call(
        kernel,
        out_shape=outs,
        in_specs=[anywhere] * 21,
        out_specs=[anywhere] * 7,
        scratch_shapes=[
            V((64, PROPS, 64), bf16), V((D,), bf16), V((64, WIDTH), bf16), V((64, WIDTH), bf16),
            V((64, 2, BC), bf16), V((48,), f32), V((48,), f32), V((SEQS, PROPS, HEADS), f32),
            V((4, WIDTH), bf16), V((4, 2, BC), bf16), V((48,), f32), V((2 * WIDTH,), bf16),
            V((64, WIDTH), bf16), V((SEQS, HEADS, HEAD_DIM, STATE), f32),
            V((SEQS, PROPS, WIDTH), bf16), V((SEQS, PROPS, BC), bf16),
            V((SEQS, PROPS, HEADS), f32), V((7, SEQS, WIDTH), bf16), V((SEQS, 7, 2, BC), bf16),
            V((128, 256), bf16), V((NX, 64, 256), bf16), V((NX, 64, 256), bf16),
            V((NX, 64, 256), bf16), V((NX, 64, GW), bf16), V((NX, 64, GW), bf16),
            V((PEERS, ROWS, GW), bf16), V((PEERS, ROWS, GW), bf16), V((PEERS, ROWS, GW), bf16),
            V((PEERS, ROWS, GW), bf16), V((PEERS, ROWS, GW), bf16), V((PEERS, ROWS, GW), bf16),
            V((NX, 64, WIDTH), bf16), V((SEQS, GROUPS, GW, STATE), bf16),
            V((NZ, ROWS, WIDTH), bf16), V((NX, 64, 64), bf16),
            V((SEQS, PROPS, WIDTH), bf16), V((SEQS, PROPS, BC), bf16),
            V((SEQS, PROPS, HEADS), f32), V((7, SEQS, WIDTH), bf16), V((SEQS, 7, 2, BC), bf16),
            pltpu.SMEM((SEQS,), i32), DMA((21,)), DMA((10,)), DMA((10,)), DMA((7,)),
        ],
        compiler_params=pltpu.CompilerParams(
            collective_id=0, has_side_effects=True, vmem_limit_bytes=60 * 1024 * 1024
        ),
    )(
        tokens, input_norm_gain, head_input_weight, output_gate_weight, state_maps_weight,
        step_size_weight.T, step_size_bias, head_decay_speed, proposal_decay_total,
        head_input_kernel, state_maps_kernel, head_direct_gain, grouped_norm_gain,
        output_weight.T, prior_state_value, previous_head_input, previous_input_maps,
        previous_log_decays, jnp.transpose(prior_heads_window, (1, 0, 2)), prior_maps_window,
        accepted,
    )
    finals = (jax.ShapeDtypeStruct((64, PROPS, 64), bf16), *outs[1:])
    mixed, state, chi, cim, cld, chw, cmw = pl.pallas_call(
        finish,
        out_shape=finals,
        in_specs=[anywhere] * 7,
        out_specs=[anywhere] * 7,
        scratch_shapes=[
            V((NX * NT, 64, 64), bf16), V((64, PROPS, 64), bf16),
            *(V(o.shape, o.dtype) for o in outs[1:]), DMA((14,)),
        ],
    )(*results)
    return mixed, state, chi, cim, cld, jnp.transpose(chw, (1, 0, 2)), cmw


def solution(mesh):
    seq = ("dp", "kv")
    return jax.shard_map(
        local,
        mesh=mesh,
        in_specs=(
            P("dp", None, "kv"), P(), P("kv", "tp"), P("kv", "tp"), P("kv", None, "tp"), P(), P(),
            P(), P(seq, None, "tp"), P(), P(), P(), P(), P("tp", "kv"), P(seq, "tp", None, None),
            P(seq, None, "tp"), P(seq, None, "tp"), P(seq, None, "tp"), P(seq, None, "tp"),
            P(seq, None, None, "tp"), P(seq),
        ),
        out_specs=(
            P("dp", None, "kv"), P(seq, "tp", None, None), P(seq, None, "tp"), P(seq, None, "tp"),
            P(seq, None, "tp"), P(seq, None, "tp"), P(seq, None, None, "tp"),
        ),
        check_vma=False,
    )
```

```python
import functools

import jax
import jax.numpy as jnp
from jax import lax
from jax.experimental import pallas as pl
from jax.experimental.pallas import tpu as pltpu
from jax.sharding import PartitionSpec as P

MESH = pl.DeviceIdType.MESH
HI = lax.Precision.HIGHEST
f32, bf16, i32 = jnp.float32, jnp.bfloat16, jnp.int32

NX, NY, NZ, NT = 4, 4, 8, 2
PEERS = NX * NZ
D, STATE, HEAD_DIM = 2048, 128, 64
SEQS, PROPS, ROWS = 2, 4, 8
HEADS, GROUPS, PER = 24, 4, 6
WIDTH, GW = 1536, 384
BC = 512
eps = 1e-06


def iota(shape, dim):
    return lax.broadcasted_iota(i32, shape, dim)


def mm(a, b, ca=1, cb=0, precision=None):
    return lax.dot_general(
        a, b, (((ca,), (cb,)), ((), ())), precision=precision, preferred_element_type=f32
    )


def heads_selection(acc):
    shape = (48, 24)
    i, j = iota(shape, 0), iota(shape, 1)
    out = i >= 32
    b = jnp.where(out, i & 1, (i >> 2) & 1)
    pos = jnp.where(out, (i - 32) >> 1, (i & 3) + (i >> 3))
    acc_b = jnp.where(b == 0, acc[0], acc[1])
    old = (j < 14) & ((j & 1) == b) & ((j >> 1) == acc_b + pos)
    raw = (j >= 16) & (((j - 16) >> 2) == b) & (((j - 16) & 3) == pos - 3)
    pick = jnp.where(pos < 3, jnp.where(old, 1.0, 0.0), jnp.where(raw, 1.0, 0.0))
    return pick.astype(bf16)


def maps_selection(acc):
    shape = (96, 48)
    i, j = iota(shape, 0), iota(shape, 1)
    out = i >= 64
    o = i - 64
    ob = jnp.where(o >= 14, 1, 0)
    orem = o - 14 * ob
    b = jnp.where(out, ob, (i >> 2) & 1)
    pos = jnp.where(out, orem >> 1, (i & 3) + (i >> 4))
    kind = jnp.where(out, orem & 1, (i >> 3) & 1)
    acc_b = jnp.where(b == 0, acc[0], acc[1])
    jb = jnp.where(j >= 14, 1, 0)
    jrem = j - 14 * jb
    old = (j < 28) & (jb == b) & ((jrem & 1) == kind) & ((jrem >> 1) == acc_b + pos)
    jr = j - 32
    raw = (j >= 32) & ((jr >> 3) == kind) & (((jr >> 2) & 1) == b) & ((jr & 3) == pos - 3)
    pick = jnp.where(pos < 3, jnp.where(old, 1.0, 0.0), jnp.where(raw, 1.0, 0.0))
    return pick.astype(bf16)


def kernel(
    tok_h, gain_h, wx_h, wg_h, smw_h, sw_h, ssb_h, hds_h, pdt_h, hik_h, smk_h, hdg_h, gng_h, wo_h,
    psv_h, phi_h, pim_h, pld_h, phw_h, pmw_h, acc_h,
    fr, state_o, chi_o, cim_o, cld_o, chw_o, cmw_o,
    tok, gain, wxg, smw, ssb, hds, pdt, hik, smk, hdg, gng, wo, psv, phi, pim, pld, phw, pmw,
    sw, bcs, tt, lhs, wr, send, got, steps_out, steps_in, wor, sb, nrm, fs,
    chi, cim, cld, chw, cmw, acc_s, lsem, ssem, rsem, osem, level_sem,
):
    y, kv, t = lax.axis_index("dp"), lax.axis_index("kv"), lax.axis_index("tp")
    z, x = kv // NX, kv % NX
    pair, half = z // 2, z % 2

    def at(zz, xx, tt_):
        return dict(device_id=(y, zz * NX + xx, tt_), device_id_type=MESH)

    def over(d):
        return dict(device_id=(lax.rem(y + d, NY), kv, t), device_id_type=MESH)

    loads = {}
    plan = (
        (tok_h, tok), (gain_h, gain), (smw_h, smw), (wx_h, wxg.at[0]), (wg_h, wxg.at[1]),
        (sw_h.at[:, pl.ds(pl.multiple_of(pair * 512, 512), 512)], sw.at[pl.ds(0, 48)]),
        (ssb_h, ssb), (hds_h, hds), (pdt_h, pdt),
        (hik_h.at[:, pl.ds(pl.multiple_of(t * WIDTH, 128), WIDTH)], hik),
        (smk_h.at[:, :, pl.ds(pl.multiple_of(t * BC, 128), BC)], smk),
        (hdg_h, hdg), (gng_h, gng), (wo_h, wo), (phi_h, phi), (pim_h, pim), (pld_h, pld),
        (phw_h, phw), (pmw_h, pmw), (psv_h, psv), (acc_h, acc_s),
    )
    for n, (src, dst) in enumerate(plan):
        loads[n] = pltpu.make_async_copy(src, dst, lsem.at[n])
        loads[n].start()

    barrier = pltpu.get_barrier_semaphore()

    row_peers = [(0, 2), (0, 1), (0, 3)]
    up_peers = [(1, 2), (1, 1), (1, 3), (1, 0)]
    down_peers = [(NZ - 1, dx) for _, dx in up_peers]

    def near(dz, dx):
        return lax.rem(x + dx, NX), at(lax.rem(z + dz, NZ), lax.rem(x + dx, NX), t)

    for dz, dx in row_peers + up_peers + down_peers:
        pl.semaphore_signal(barrier, inc=1, **near(dz, dx)[1])
    for d in range(NX):
        pl.semaphore_signal(barrier, inc=1, **at(z, lax.rem(x + d, NX), 1 - t))
    for d in range(1, NY):
        pl.semaphore_signal(barrier, inc=1, **over(d))

    for n in (0, 1, 2):
        loads[n].wait()
    tok32 = tok[...].astype(f32).reshape(256, 64)
    gains = gain[...].astype(f32).reshape(16, 128)
    gain_row = jnp.sum(
        jnp.where(iota((16, 128), 0) == kv // 2, gains, 0.0), axis=0, keepdims=True
    )
    gain_row = jnp.where(kv % 2 == 0, gain_row[:, :64], gain_row[:, 64:])
    tt[x, 0:64] = (tok32 * gain_row).astype(bf16).T
    sumsq = jnp.sum(jnp.square(tok32.T), axis=0, keepdims=True)
    high = sumsq.astype(bf16).astype(f32)
    line = iota((16, 256), 0)
    tt[x, 64:80] = jnp.where(
        line == 0, high, jnp.where(line == 1, sumsq - high, 0.0)
    ).astype(bf16)
    for n in range(2):
        part = smw[:, n, :]
        for g in range(GROUPS):
            bcs[n * GROUPS + g] = part[:, g * STATE : g * STATE + STATE]
    sw[48:128] = jnp.zeros((80, 512), bf16)

    def columns(c, h, xx):
        if c == 0:
            return bcs.at[h * NX + xx]
        return wxg.at[
            h if c == 1 else 1 - h, :, pl.ds(pl.multiple_of(xx * GW + (c - 1) * 128, 128), 128)
        ]

    loads[3].wait()
    loads[4].wait()
    for c in range(4):
        wr[c, x] = columns(c, half, x)[...]

    pl.semaphore_wait(barrier, 11 + NX + NY - 1)

    lanes_t = pl.ds(pl.multiple_of(t * 128, 128), 128)
    for peers, base in ((up_peers, 8), (down_peers, 4), (row_peers, 0)):
        for dz, dx in peers:
            pltpu.make_async_remote_copy(
                tt.at[x, :, lanes_t],
                tt.at[base + x, :, lanes_t],
                ssem.at[4],
                rsem.at[4],
                **near(dz, dx)[1],
            ).start()
    for c in range(4):
        for peers, h, base in (
            (down_peers if c < 2 else up_peers, 1 - half, 4),
            (row_peers, half, 0),
        ):
            for dz, dx in peers:
                xx, to = near(dz, dx)
                pltpu.make_async_remote_copy(
                    columns(c, h, xx), wr.at[c, base + x], ssem.at[c], rsem.at[c], **to
                ).start()

    def pass_on(level):
        for n, dz in enumerate((1, NZ - 1)):
            pl.semaphore_signal(level_sem.at[level, n], inc=1, **near(dz, 0)[1])

    def hear(level):
        for n in range(2):
            pl.semaphore_wait(level_sem.at[level, n], 1)

    pass_on(0)

    def arrived(buffer, count, sem):
        block = buffer.at[pl.ds(0, count)]
        pltpu.make_async_copy(block, block, sem).wait()

    from_me = (x * 2 + half) * 4 + pair

    def spread(src, dst, index, n):
        def one(d, _):
            other = lax.rem(kv + d, PEERS)
            pltpu.make_async_remote_copy(
                src.at[other],
                dst.at[index],
                ssem.at[n],
                rsem.at[n],
                device_id=(y, other, t),
                device_id_type=MESH,
            ).start()
            return 0

        lax.fori_loop(1, PEERS, one, 0)
        dst[index] = src[kv]

    loads[20].wait()
    acc = (acc_s[0], acc_s[1])
    row = iota((ROWS, 1), 0)
    acc_row = jnp.where(row < PROPS, acc[0], acc[1])
    keep = jnp.where((row & 3) < acc_row, 1.0, 0.0)
    r8, c8 = iota((ROWS, ROWS), 0), iota((ROWS, ROWS), 1)
    same = (r8 >> 2) == (c8 >> 2)
    expand = jnp.where(iota((HEADS, WIDTH), 1) // HEAD_DIM == iota((HEADS, WIDTH), 0), 1.0, 0.0)
    for n in (14, 15, 16):
        loads[n].wait()
    kept = pld[...].reshape(ROWS, HEADS) * keep
    later = mm(jnp.where(same & (c8 > r8), 1.0, 0.0), kept, precision=HI)
    coef = mm(keep * jnp.exp(later), expand, precision=HI)
    scaled = coef * phi[...].astype(f32).reshape(ROWS, WIDTH)
    s_hi = scaled.astype(bf16)
    s_lo = (scaled - s_hi.astype(f32)).astype(bf16)
    updates = jnp.concatenate([s_hi.astype(f32), s_lo.astype(f32)], axis=0).astype(bf16)
    keys = pim[...].astype(f32).reshape(ROWS, BC)
    loads[19].wait()
    for b in range(SEQS):
        mine = (row >> 2) == b
        logs = mm(jnp.where(mine, kept, 0.0), jnp.ones((ROWS, STATE), f32), 0, 0, precision=HI)
        factor = jnp.exp(logs)
        keys_b = jnp.where(mine, keys, 0.0)
        keys_b = jnp.concatenate([keys_b, keys_b], axis=0).astype(bf16)
        for g in range(GROUPS):
            upd = mm(
                updates[:, g * GW : g * GW + GW], keys_b[:, g * STATE : g * STATE + STATE], 0, 0
            )
            new = (
                psv[b, g * PER : g * PER + PER] * factor[g * PER : g * PER + PER][:, None, :]
                + upd.reshape(PER, HEAD_DIM, STATE)
            )
            psv[b, g * PER : g * PER + PER] = new
            sb[b, g] = new.reshape(GW, STATE).astype(bf16)
    outs = []

    def put(n, src, dst):
        outs.append(pltpu.make_async_copy(src, dst, osem.at[n]))
        outs[-1].start()

    put(0, psv, state_o)

    for level in range(3):
        hear(level)
        if level < 2:
            pass_on(level + 1)

    loads[13].wait()
    wor[x] = wo[...]
    mine = pl.ds(pl.multiple_of(y * 16, 16), 16)
    quarters = wor.at[:, pl.ds(0, 16)]
    three_quarters = wor.at[:, pl.ds(0, 48)]

    steps_mine = (half == 0) & (x == pair)
    halves = tt.at[:, :, pl.ds(0, 128)]
    arrived(halves, 11, rsem.at[4])
    blocks = [tt.at[pl.ds(4, 8), :, lanes_t]]
    blocks += [tt.at[lax.rem(x + d, NX), :, lanes_t] for d in range(1, NX)]
    for block in blocks:
        pltpu.make_async_remote_copy(
            block, block, ssem.at[14], rsem.at[14], **at(z, x, 1 - t)
        ).start()
    arrived(halves, 11, rsem.at[14])
    lhs[...] = tt[:, 0:64].reshape(768, 256).T
    for c in range(4):
        if c == 0:
            loads[5].wait()
        arrived(wr.at[c], 7, rsem.at[c])
        if c < 2:
            part = mm(lhs[:, 0:512], wr[c].reshape(512, 128))
        else:
            part = mm(lhs[:, 0:256], wr[c, 0:4].reshape(256, 128))
            part = part + mm(lhs[:, 512:768], wr[c, 4:8].reshape(256, 128))
        send[c] = part.reshape(PEERS, ROWS, 128).astype(bf16)
        spread(send.at[c], got.at[c], from_me, 5 + c)
        if c == 1:
            for d in (2, 1, 3):
                pltpu.make_async_remote_copy(
                    wo.at[mine], wor.at[x, mine], ssem.at[10], rsem.at[10],
                    **at(z, lax.rem(x + d, NX), t),
                ).start()
        if c == 0:

            @pl.when(steps_mine)
            def _():
                steps = mm(lhs[:, 0:512], sw[...], 1, 1)
                squares = jnp.sum(tt[0:8, 64:80].astype(f32), axis=0)
                pick = jnp.where(
                    (iota((16, 128), 1) == 64) & (iota((16, 128), 0) < 2), 1.0, 0.0
                )
                squares = mm(squares, pick, 0, 0, precision=HI)
                total = squares[:, 64:65]
                high = total.astype(bf16).astype(f32)
                lane = iota((256, 128), 1)
                steps = jnp.where(lane == 64, high, jnp.where(lane == 65, total - high, steps))
                steps_out[...] = steps.reshape(PEERS, ROWS, 128).astype(bf16)
                spread(steps_out, steps_in, pair, 9)

    arrived(quarters, 3, rsem.at[10])
    for d in (2, 1, 3):
        for e in (2, 1, 3):
            block = wor.at[lax.rem(x + d, NX), mine]
            pltpu.make_async_remote_copy(
                block, block, ssem.at[13], rsem.at[13], **over(e)
            ).start()

    pick_x, pick_bc = heads_selection(acc), maps_selection(acc)
    for n in (6, 7, 8, 9, 10, 11, 12, 17, 18):
        loads[n].wait()
    old_x = phw[...].astype(f32).reshape(14, WIDTH)
    old_x = jnp.concatenate([old_x, jnp.zeros((2, WIDTH), f32)], axis=0)
    old_bc = pmw[...].astype(f32).reshape(28, BC)
    old_bc = jnp.concatenate([old_bc, jnp.zeros((4, BC), f32)], axis=0)
    taps_x = hik[...].astype(f32)
    taps_bc = smk[...].astype(f32).reshape(8, BC)

    def own_heads(ref):
        v = ref[...].reshape(1, 2 * HEADS)
        return jnp.where(t == 0, v[:, :HEADS], v[:, HEADS:])

    speed, direct, bias = own_heads(hds), own_heads(hdg), own_heads(ssb)
    gngv = gng[...].astype(f32).reshape(1, 2 * WIDTH)
    out_gain = jnp.where(t == 0, gngv[:, :WIDTH], gngv[:, WIDTH:])

    def total(c):
        return jnp.sum(got[c].astype(f32).reshape(NX, 2, 4, ROWS, 128), axis=2)

    arrived(got.at[0], PEERS - 1, rsem.at[5])

    @pl.when(steps_mine)
    def _():
        arrived(steps_in, 3, rsem.at[9])

    @pl.when(jnp.logical_not(steps_mine))
    def _():
        arrived(steps_in, 4, rsem.at[9])

    tail = jnp.sum(steps_in[...].astype(f32), axis=0)
    lane8 = iota((ROWS, 128), 1)
    squares = jnp.sum(jnp.where((lane8 == 64) | (lane8 == 65), tail, 0.0), axis=1, keepdims=True)
    inv = lax.rsqrt(squares / D + eps)
    sum0 = total(0)
    raw_b = jnp.concatenate([sum0[g, 0] for g in range(GROUPS)], axis=1) * inv
    raw_c = jnp.concatenate([sum0[g, 1] for g in range(GROUPS)], axis=1) * inv
    win_bc = mm(pick_bc, jnp.concatenate([old_bc, raw_b, raw_c], axis=0).astype(bf16))
    cmw[...] = win_bc[64:92].reshape(SEQS, 7, 2, BC).astype(bf16)
    put(1, cmw, cmw_o)
    b_conv = taps_bc[0:1] * win_bc[0:8]
    c_conv = taps_bc[1:2] * win_bc[8:16]
    for k in range(1, 4):
        b_conv = b_conv + taps_bc[2 * k : 2 * k + 1] * win_bc[16 * k : 16 * k + 8]
        c_conv = c_conv + taps_bc[2 * k + 1 : 2 * k + 2] * win_bc[16 * k + 8 : 16 * k + 16]
    b_conv = b_conv * lax.logistic(b_conv)
    c_conv = c_conv * lax.logistic(c_conv)
    step_pre = tail * inv
    step_pre = jnp.where(t == 0, step_pre[:, :HEADS], step_pre[:, HEADS : 2 * HEADS]) + bias
    step = jnp.maximum(step_pre, 0.0) + jnp.log1p(jnp.exp(-jnp.abs(step_pre)))
    decays = pdt[...].reshape(ROWS, HEADS) - speed * step
    cum = mm(jnp.where(same & (c8 <= r8), 1.0, 0.0), decays, precision=HI)
    wide = mm(
        jnp.concatenate([cum, step, jnp.broadcast_to(direct, (ROWS, HEADS))], axis=0),
        expand,
        precision=HI,
    )
    cim[...] = b_conv.reshape(SEQS, PROPS, BC).astype(bf16)
    put(2, cim, cim_o)
    cld[...] = decays.reshape(SEQS, PROPS, HEADS)
    put(3, cld, cld_o)
    from_state, pairs = [], []
    for g in range(GROUPS):
        lanes = slice(g * STATE, g * STATE + STATE)
        c_g = c_conv[:, lanes]
        y0 = mm(c_g.astype(bf16), sb[0, g], 1, 1)
        y1 = mm(c_g.astype(bf16), sb[1, g], 1, 1)
        from_state.append(jnp.where(row < PROPS, y0, y1))
        pairs.append(mm(c_g, b_conv[:, lanes], 1, 1, precision=HI))
    from_state = jnp.exp(wide[0:8]) * jnp.concatenate(from_state, axis=1)
    scores = []
    for d in range(PROPS):
        score = [
            jnp.broadcast_to(
                jnp.sum(jnp.where(c8 == r8 - d, p, 0.0), axis=1, keepdims=True), (ROWS, 128)
            )
            for p in pairs
        ]
        scores.append(jnp.concatenate(score, axis=1))

    def third(v, c):
        starts = [g * GW + (c - 1) * 128 for g in range(GROUPS)]
        return jnp.concatenate([v[:, n : n + 128] for n in starts], axis=1)

    def whole(thirds):
        return jnp.concatenate(
            [v[:, g * 128 : g * 128 + 128] for g in range(GROUPS) for v in thirds], axis=1
        )

    windows, inputs, gated = [], [], []
    for c in range(1, 4):
        wide_c, taps_c, old_c = third(wide, c), third(taps_x, c), third(old_x, c)
        cum_w, step_w, direct_w = wide_c[0:8], wide_c[8:16], wide_c[16:24]
        decay_w = [None]
        for d in range(1, PROPS):
            gap = jnp.where((row & 3) >= d, cum_w - pltpu.roll(cum_w, d, 0), 0.0)
            decay_w.append(jnp.exp(gap) * scores[d])
        arrived(got.at[c], PEERS - 1, rsem.at[5 + c])
        sum_c = total(c)
        heads_at = 0 if c == 1 else 1
        raw_x = jnp.concatenate([sum_c[g, heads_at] for g in range(GROUPS)], axis=1) * inv
        gate = jnp.concatenate([sum_c[g, 1 - heads_at] for g in range(GROUPS)], axis=1) * inv
        win_x = mm(pick_x, jnp.concatenate([old_c, raw_x], axis=0).astype(bf16))
        windows.append(win_x[32:46])
        x_conv = taps_c[0:1] * win_x[0:8]
        for k in range(1, 4):
            x_conv = x_conv + taps_c[k : k + 1] * win_x[8 * k : 8 * k + 8]
        x_conv = x_conv * lax.logistic(x_conv)
        weighted = step_w * x_conv
        inputs.append(weighted)
        heads = third(from_state, c) + direct_w * x_conv + scores[0] * weighted
        for d in range(1, PROPS):
            term = decay_w[d] * pltpu.roll(weighted, d, 0)
            heads = heads + jnp.where((row & 3) >= d, term, 0.0)
        gated.append(heads * (gate * lax.logistic(gate)))

    gated = whole(gated)
    normed = []
    for g in range(GROUPS):
        part_g = gated[:, g * GW : g * GW + GW]
        mean = jnp.sum(part_g * part_g, axis=1, keepdims=True) / GW
        normed.append(part_g * lax.rsqrt(mean + eps))
    nrm[z] = (jnp.concatenate(normed, axis=1) * out_gain).astype(bf16)
    for d in (4, 3, 5, 2, 6, 1, 7):
        pltpu.make_async_remote_copy(
            nrm.at[z], nrm.at[z], ssem.at[11], rsem.at[11], **at(lax.rem(z + d, NZ), x, t)
        ).start()
    chw[...] = whole(windows).reshape(7, SEQS, WIDTH).astype(bf16)
    put(4, chw, chw_o)
    chi[...] = whole(inputs).reshape(SEQS, PROPS, WIDTH).astype(bf16)
    put(5, chi, chi_o)

    arrived(three_quarters, 3, rsem.at[13])
    arrived(nrm, 7, rsem.at[11])
    rows64 = nrm[...].astype(f32).reshape(64, WIDTH).astype(bf16)
    for d in (2, 1, 3, 0):
        xp = lax.rem(x + d, NX)
        part = mm(rows64, wor[xp], 1, 1)
        fs[d] = jnp.concatenate([part[:32], part[32:]], axis=1).astype(bf16)
        if d == 0:
            put(6, fs.at[0], fr.at[x * NT + t])
        else:
            pltpu.make_async_remote_copy(
                fs.at[d], fr.at[x * NT + t], ssem.at[12], rsem.at[12], **at(z, xp, t)
            ).start()
        pltpu.make_async_remote_copy(
            fs.at[d], fr.at[x * NT + t], ssem.at[12], rsem.at[12], **at(z, xp, 1 - t)
        ).start()
    arrived(fr, 7, rsem.at[12])

    arrived(halves, 11, ssem.at[4])
    arrived(halves, 11, ssem.at[14])
    for c in range(4):
        arrived(wr.at[c], 7, ssem.at[c])
        arrived(send.at[c], PEERS - 1, ssem.at[5 + c])

    @pl.when(steps_mine)
    def _():
        arrived(steps_out, PEERS - 1, ssem.at[9])

    arrived(quarters, 3, ssem.at[10])
    arrived(three_quarters, 3, ssem.at[13])
    arrived(nrm, 7, ssem.at[11])
    arrived(fr, 7, ssem.at[12])
    for copy in outs:
        copy.wait()


def finish(fr_h, *refs):
    ins, outs, fr, mixed, mids, sems = (
        refs[:6], refs[7:13], refs[13], refs[14], refs[15:21], refs[21],
    )
    mixed_o = refs[6]

    def pieces(ref, n):
        if n > 0:
            return [ref]
        return [ref.at[b, pl.ds(h, 12)] for b in range(SEQS) for h in (0, 12)]

    trio = [
        piece
        for n in (1, 2, 3, 4, 5, 0)
        for piece in zip(pieces(ins[n], n), pieces(mids[n], n), pieces(outs[n], n))
    ]
    head = pltpu.make_async_copy(fr_h, fr, sems.at[0])
    head.start()
    first = [pltpu.make_async_copy(a, b, sems.at[1 + n]) for n, (a, b, _) in enumerate(trio)]
    second = [pltpu.make_async_copy(b, c, sems.at[10 + n]) for n, (_, b, c) in enumerate(trio)]
    for copy in first:
        copy.start()
    head.wait()
    done = fr[...].astype(f32).reshape(NX, NT, 32, 128)
    done = (done[:, 0] + done[:, 1]).reshape(NX, 4, ROWS, 128)
    done = jnp.stack(
        [done[:, n % 4, :, :64] if n < 4 else done[:, n % 4, :, 64:] for n in range(NZ)], axis=0
    )
    mixed[...] = done.reshape(64, PROPS, 64).astype(bf16)
    last = pltpu.make_async_copy(mixed, mixed_o, sems.at[19])
    last.start()
    for a, b in zip(first, second):
        a.wait()
        b.start()
    for copy in second:
        copy.wait()
    last.wait()


def local(
    tokens, input_norm_gain, head_input_weight, output_gate_weight, state_maps_weight,
    step_size_weight, step_size_bias, head_decay_speed, proposal_decay_total, head_input_kernel,
    state_maps_kernel, head_direct_gain, grouped_norm_gain, output_weight, prior_state_value,
    previous_head_input, previous_input_maps, previous_log_decays, prior_heads_window,
    prior_maps_window, accepted,
):
    anywhere = pl.BlockSpec(memory_space=pl.ANY)
    V, DMA = pltpu.VMEM, pltpu.SemaphoreType.DMA
    outs = (
        jax.ShapeDtypeStruct((NX * NT, 32, 128), bf16),
        jax.ShapeDtypeStruct((SEQS, HEADS, HEAD_DIM, STATE), f32),
        jax.ShapeDtypeStruct((SEQS, PROPS, WIDTH), bf16),
        jax.ShapeDtypeStruct((SEQS, PROPS, BC), bf16),
        jax.ShapeDtypeStruct((SEQS, PROPS, HEADS), f32),
        jax.ShapeDtypeStruct((7, SEQS, WIDTH), bf16),
        jax.ShapeDtypeStruct((SEQS, 7, 2, BC), bf16),
    )
    results = pl.pallas_call(
        kernel,
        out_shape=outs,
        in_specs=[anywhere] * 21,
        out_specs=[anywhere] * 7,
        scratch_shapes=[
            V((64, PROPS, 64), bf16), V((D,), bf16), V((2, 64, WIDTH), bf16),
            V((64, 2, BC), bf16), V((48,), f32), V((48,), f32), V((SEQS, PROPS, HEADS), f32),
            V((4, WIDTH), bf16), V((4, 2, BC), bf16), V((48,), f32), V((2 * WIDTH,), bf16),
            V((64, WIDTH), bf16), V((SEQS, HEADS, HEAD_DIM, STATE), f32),
            V((SEQS, PROPS, WIDTH), bf16), V((SEQS, PROPS, BC), bf16),
            V((SEQS, PROPS, HEADS), f32), V((7, SEQS, WIDTH), bf16), V((SEQS, 7, 2, BC), bf16),
            V((128, 512), bf16), V((8, 64, 128), bf16), V((12, 80, 256), bf16),
            V((256, 768), bf16), V((4, 8, 64, 128), bf16), V((4, PEERS, ROWS, 128), bf16),
            V((4, PEERS, ROWS, 128), bf16), V((PEERS, ROWS, 128), bf16), V((4, ROWS, 128), bf16),
            V((NX, 64, WIDTH), bf16), V((SEQS, GROUPS, GW, STATE), bf16),
            V((NZ, ROWS, WIDTH), bf16), V((NX, 32, 128), bf16),
            V((SEQS, PROPS, WIDTH), bf16), V((SEQS, PROPS, BC), bf16),
            V((SEQS, PROPS, HEADS), f32), V((7, SEQS, WIDTH), bf16), V((SEQS, 7, 2, BC), bf16),
            pltpu.SMEM((SEQS,), i32), DMA((21,)), DMA((15,)), DMA((15,)), DMA((7,)),
            pltpu.SemaphoreType.REGULAR((3, 2)),
        ],
        compiler_params=pltpu.CompilerParams(
            collective_id=0, has_side_effects=True, vmem_limit_bytes=60 * 1024 * 1024
        ),
    )(
        tokens, input_norm_gain, head_input_weight, output_gate_weight, state_maps_weight,
        step_size_weight.T, step_size_bias, head_decay_speed, proposal_decay_total,
        head_input_kernel, state_maps_kernel, head_direct_gain, grouped_norm_gain,
        output_weight.T, prior_state_value, previous_head_input, previous_input_maps,
        previous_log_decays, jnp.transpose(prior_heads_window, (1, 0, 2)), prior_maps_window,
        accepted,
    )
    finals = (jax.ShapeDtypeStruct((64, PROPS, 64), bf16), *outs[1:])
    mixed, state, chi, cim, cld, chw, cmw = pl.pallas_call(
        finish,
        out_shape=finals,
        in_specs=[anywhere] * 7,
        out_specs=[anywhere] * 7,
        scratch_shapes=[
            V((NX * NT, 32, 128), bf16), V((64, PROPS, 64), bf16),
            *(V(o.shape, o.dtype) for o in outs[1:]), DMA((20,)),
        ],
    )(*results)
    return mixed, state, chi, cim, cld, jnp.transpose(chw, (1, 0, 2)), cmw


def solution(mesh):
    seq = ("dp", "kv")
    return jax.shard_map(
        local,
        mesh=mesh,
        in_specs=(
            P("dp", None, "kv"), P(), P("kv", "tp"), P("kv", "tp"), P("kv", None, "tp"), P(), P(),
            P(), P(seq, None, "tp"), P(), P(), P(), P(), P("tp", "kv"), P(seq, "tp", None, None),
            P(seq, None, "tp"), P(seq, None, "tp"), P(seq, None, "tp"), P(seq, None, "tp"),
            P(seq, None, None, "tp"), P(seq),
        ),
        out_specs=(
            P("dp", None, "kv"), P(seq, "tp", None, None), P(seq, None, "tp"), P(seq, None, "tp"),
            P(seq, None, "tp"), P(seq, None, "tp"), P(seq, None, None, "tp"),
        ),
        check_vma=False,
    )
```

```python
import functools

import jax
import jax.numpy as jnp
from jax import lax
from jax.experimental import pallas as pl
from jax.experimental.pallas import tpu as pltpu
from jax.sharding import PartitionSpec as P

MESH = pl.DeviceIdType.MESH
HI = lax.Precision.HIGHEST
f32, bf16, i32 = jnp.float32, jnp.bfloat16, jnp.int32

NX, NY, NZ, NT = 4, 4, 8, 2
PEERS = NX * NZ
D, STATE, HEAD_DIM = 2048, 128, 64
SEQS, PROPS, ROWS = 2, 4, 8
HEADS, GROUPS, PER = 24, 4, 6
WIDTH, GW = 1536, 384
BC = 512
eps = 1e-06


def iota(shape, dim):
    return lax.broadcasted_iota(i32, shape, dim)


def mm(a, b, ca=1, cb=0, precision=None):
    return lax.dot_general(
        a, b, (((ca,), (cb,)), ((), ())), precision=precision, preferred_element_type=f32
    )


def heads_selection(acc):
    shape = (48, 24)
    i, j = iota(shape, 0), iota(shape, 1)
    out = i >= 32
    b = jnp.where(out, i & 1, (i >> 2) & 1)
    pos = jnp.where(out, (i - 32) >> 1, (i & 3) + (i >> 3))
    acc_b = jnp.where(b == 0, acc[0], acc[1])
    old = (j < 14) & ((j & 1) == b) & ((j >> 1) == acc_b + pos)
    raw = (j >= 16) & (((j - 16) >> 2) == b) & (((j - 16) & 3) == pos - 3)
    pick = jnp.where(pos < 3, jnp.where(old, 1.0, 0.0), jnp.where(raw, 1.0, 0.0))
    return pick.astype(bf16)


def maps_selection(acc):
    shape = (96, 48)
    i, j = iota(shape, 0), iota(shape, 1)
    out = i >= 64
    o = i - 64
    ob = jnp.where(o >= 14, 1, 0)
    orem = o - 14 * ob
    b = jnp.where(out, ob, (i >> 2) & 1)
    pos = jnp.where(out, orem >> 1, (i & 3) + (i >> 4))
    kind = jnp.where(out, orem & 1, (i >> 3) & 1)
    acc_b = jnp.where(b == 0, acc[0], acc[1])
    jb = jnp.where(j >= 14, 1, 0)
    jrem = j - 14 * jb
    old = (j < 28) & (jb == b) & ((jrem & 1) == kind) & ((jrem >> 1) == acc_b + pos)
    jr = j - 32
    raw = (j >= 32) & ((jr >> 3) == kind) & (((jr >> 2) & 1) == b) & ((jr & 3) == pos - 3)
    pick = jnp.where(pos < 3, jnp.where(old, 1.0, 0.0), jnp.where(raw, 1.0, 0.0))
    return pick.astype(bf16)


def kernel(
    tok_h, gain_h, wx_h, wg_h, smw_h, sw_h, ssb_h, hds_h, pdt_h, hik_h, smk_h, hdg_h, gng_h, wo_h,
    psv_h, phi_h, pim_h, pld_h, phw_h, pmw_h, acc_h,
    fr, state_o, chi_o, cim_o, cld_o, chw_o, cmw_o,
    tok, gain, wxg, smw, ssb, hds, pdt, hik, smk, hdg, gng, wo, psv, phi, pim, pld, phw, pmw,
    sw, bcs, tt, squares_out, squares_in, lhs, wr, send, got, steps_out, steps_in, wor, sb, nrm, last, fs,
    chi, cim, cld, chw, cmw, acc_s, lsem, ssem, rsem, osem, level_sem,
):
    y, kv, t = lax.axis_index("dp"), lax.axis_index("kv"), lax.axis_index("tp")
    z, x = kv // NX, kv % NX
    pair, half = z // 2, z % 2

    def at(zz, xx, tt_):
        return dict(device_id=(y, zz * NX + xx, tt_), device_id_type=MESH)

    def over(d):
        return dict(device_id=(lax.rem(y + d, NY), kv, t), device_id_type=MESH)

    loads = {}
    plan = (
        (tok_h, tok), (gain_h, gain), (smw_h, smw), (wx_h, wxg.at[0]), (wg_h, wxg.at[1]),
        (sw_h.at[:, pl.ds(pl.multiple_of(pair * 512, 512), 512)], sw.at[pl.ds(0, 48)]),
        (ssb_h, ssb), (hds_h, hds), (pdt_h, pdt),
        (hik_h.at[:, pl.ds(pl.multiple_of(t * WIDTH, 128), WIDTH)], hik),
        (smk_h.at[:, :, pl.ds(pl.multiple_of(t * BC, 128), BC)], smk),
        (hdg_h, hdg), (gng_h, gng), (wo_h, wo), (phi_h, phi), (pim_h, pim), (pld_h, pld),
        (phw_h, phw), (pmw_h, pmw), (psv_h, psv), (acc_h, acc_s),
    )
    for n, (src, dst) in enumerate(plan):
        loads[n] = pltpu.make_async_copy(src, dst, lsem.at[n])
    for n in (0, 1, 2):
        loads[n].start()

    barrier = pltpu.get_barrier_semaphore()

    row_peers = [(0, 2), (0, 1), (0, 3)]
    up_peers = [(1, 2), (1, 1), (1, 3), (1, 0)]
    down_peers = [(NZ - 1, dx) for _, dx in up_peers]

    def near(dz, dx):
        return lax.rem(x + dx, NX), at(lax.rem(z + dz, NZ), lax.rem(x + dx, NX), t)

    for dz, dx in row_peers + up_peers + down_peers:
        pl.semaphore_signal(barrier, inc=1, **near(dz, dx)[1])
    for d in range(NX):
        pl.semaphore_signal(barrier, inc=1, **at(z, lax.rem(x + d, NX), 1 - t))
    for d in range(1, NY):
        pl.semaphore_signal(barrier, inc=1, **over(d))
    for d in range(1, NX):
        pl.semaphore_signal(barrier, inc=1, **at(lax.rem(z + 2 * d, NZ), x, t))
    for n in range(3, len(plan)):
        loads[n].start()

    for n in (0, 1, 2):
        loads[n].wait()
    tok32 = tok[...].astype(f32).reshape(256, 64)
    gains = gain[...].astype(f32).reshape(16, 128)
    gain_row = jnp.sum(
        jnp.where(iota((16, 128), 0) == kv // 2, gains, 0.0), axis=0, keepdims=True
    )
    gain_row = jnp.where(kv % 2 == 0, gain_row[:, :64], gain_row[:, 64:])
    tt[x, 0:64] = (tok32 * gain_row).astype(bf16).T
    sumsq = jnp.sum(jnp.square(tok32.T), axis=0, keepdims=True)
    high = sumsq.astype(bf16).astype(f32)
    line = iota((16, 256), 0)
    squares_out[...] = jnp.where(
        line == 0, high, jnp.where(line == 1, sumsq - high, 0.0)
    ).astype(bf16)
    for n in range(2):
        part = smw[:, n, :]
        for g in range(GROUPS):
            bcs[n * GROUPS + g] = part[:, g * STATE : g * STATE + STATE]
    sw[48:128] = jnp.zeros((80, 512), bf16)

    def columns(c, h, xx):
        if c == 0:
            return bcs.at[h * NX + xx]
        return wxg.at[
            h if c == 1 else 1 - h, :, pl.ds(pl.multiple_of(xx * GW + (c - 1) * 128, 128), 128)
        ]

    loads[3].wait()
    loads[4].wait()
    for c in range(4):
        wr[c, x] = columns(c, half, x)[...]

    pl.semaphore_wait(barrier, 11 + NX + NY - 1 + NX - 1)

    def pass_on(level):
        for n, dz in enumerate((1, NZ - 1)):
            pl.semaphore_signal(level_sem.at[level, n], inc=1, **near(dz, 0)[1])

    def hear(level):
        for n in range(2):
            pl.semaphore_wait(level_sem.at[level, n], 1)

    pass_on(0)

    @pl.when(t == 1)
    def _():
        for peers, base in ((up_peers, 8), (down_peers, 4), (row_peers, 0)):
            for dz, dx in peers:
                pltpu.make_async_remote_copy(
                    tt.at[x], tt.at[base + x], ssem.at[4], rsem.at[4], **near(dz, dx)[1]
                ).start()

    def send_weights(c):
        for peers, h, base in (
            (down_peers if c < 2 else up_peers, 1 - half, 4),
            (row_peers, half, 0),
        ):
            for dz, dx in peers:
                xx, to = near(dz, dx)
                pltpu.make_async_remote_copy(
                    columns(c, h, xx), wr.at[c, base + x], ssem.at[c], rsem.at[c], **to
                ).start()

    steps_mine = (half == 0) & (x == pair)

    @pl.when(jnp.logical_not(steps_mine))
    def _():
        pltpu.make_async_remote_copy(
            squares_out, squares_in.at[half * NX + x], ssem.at[15], rsem.at[15],
            **at(2 * pair, pair, t),
        ).start()

    def arrived(buffer, count, sem):
        block = buffer.at[pl.ds(0, count)]
        pltpu.make_async_copy(block, block, sem).wait()

    loads[20].wait()
    acc = (acc_s[0], acc_s[1])
    row = iota((ROWS, 1), 0)
    acc_row = jnp.where(row < PROPS, acc[0], acc[1])
    keep = jnp.where((row & 3) < acc_row, 1.0, 0.0)
    r8, c8 = iota((ROWS, ROWS), 0), iota((ROWS, ROWS), 1)
    same = (r8 >> 2) == (c8 >> 2)
    expand = jnp.where(iota((HEADS, WIDTH), 1) // HEAD_DIM == iota((HEADS, WIDTH), 0), 1.0, 0.0)
    for n in (14, 15, 16):
        loads[n].wait()
    kept = pld[...].reshape(ROWS, HEADS) * keep
    later = mm(jnp.where(same & (c8 > r8), 1.0, 0.0), kept, precision=HI)
    coef = mm(keep * jnp.exp(later), expand, precision=HI)
    scaled = coef * phi[...].astype(f32).reshape(ROWS, WIDTH)
    s_hi = scaled.astype(bf16)
    s_lo = (scaled - s_hi.astype(f32)).astype(bf16)
    updates = jnp.concatenate([s_hi.astype(f32), s_lo.astype(f32)], axis=0).astype(bf16)
    keys = pim[...].astype(f32).reshape(ROWS, BC)
    loads[19].wait()
    for b in range(SEQS):
        of_b = (row >> 2) == b
        logs = mm(jnp.where(of_b, kept, 0.0), jnp.ones((ROWS, STATE), f32), 0, 0, precision=HI)
        factor = jnp.exp(logs)
        keys_b = jnp.where(of_b, keys, 0.0)
        keys_b = jnp.concatenate([keys_b, keys_b], axis=0).astype(bf16)
        for g in range(GROUPS):
            upd = mm(
                updates[:, g * GW : g * GW + GW], keys_b[:, g * STATE : g * STATE + STATE], 0, 0
            )
            new = (
                psv[b, g * PER : g * PER + PER] * factor[g * PER : g * PER + PER][:, None, :]
                + upd.reshape(PER, HEAD_DIM, STATE)
            )
            psv[b, g * PER : g * PER + PER] = new
            sb[b, g] = new.reshape(GW, STATE).astype(bf16)
    outs = []

    def put(n, src, dst):
        outs.append(pltpu.make_async_copy(src, dst, osem.at[n]))
        outs[-1].start()

    put(0, psv, state_o)

    @pl.when(t == 1)
    def _():
        arrived(tt, 11, ssem.at[4])

    for c in range(4):
        send_weights(c)
    loads[13].wait()
    wor[0] = wo[...]
    mine = pl.ds(pl.multiple_of(y * 16, 16), 16)
    for d in (2, 1, 3):
        pltpu.make_async_remote_copy(
            wo.at[mine], wor.at[NX - d, mine], ssem.at[10], rsem.at[10],
            **at(lax.rem(z + 2 * d, NZ), x, t),
        ).start()
    quarters = wor.at[:, pl.ds(0, 16)]
    three_quarters = wor.at[:, pl.ds(0, 48)]

    from_me = (x * 2 + half) * 4 + pair

    def spread(src, dst, index, n):
        def one(d, _):
            other = lax.rem(kv + d, PEERS)
            pltpu.make_async_remote_copy(
                src.at[other],
                dst.at[index],
                ssem.at[n],
                rsem.at[n],
                device_id=(y, other, t),
                device_id_type=MESH,
            ).start()
            return 0

        lax.fori_loop(1, PEERS, one, 0)
        dst[index] = src[kv]

    for level in range(3):
        hear(level)
        if level < 2:
            pass_on(level + 1)


    @pl.when(t == 1)
    def _():
        arrived(tt, 11, rsem.at[4])
        blocks = [tt.at[pl.ds(4, 8)]]
        blocks += [tt.at[lax.rem(x + d, NX)] for d in range(1, NX)]
        for block in blocks:
            pltpu.make_async_remote_copy(
                block, block, ssem.at[14], rsem.at[14], **at(z, x, 1 - t)
            ).start()

    @pl.when(t == 0)
    def _():
        arrived(tt, 11, rsem.at[14])

    lhs[...] = tt[...].reshape(768, 256).T
    loads[5].wait()

    @pl.when(steps_mine)
    def _():
        steps = mm(lhs[:, 0:512], sw[...], 1, 1)
        arrived(squares_in, 7, rsem.at[15])
        squares_in[half * NX + x] = squares_out[...]
        squares = jnp.sum(squares_in[...].astype(f32), axis=0)
        pick = jnp.where(
            (iota((16, 128), 1) == 64) & (iota((16, 128), 0) < 2), 1.0, 0.0
        )
        squares = mm(squares, pick, 0, 0, precision=HI)
        total = squares[:, 64:65]
        high = total.astype(bf16).astype(f32)
        lane = iota((256, 128), 1)
        steps = jnp.where(lane == 64, high, jnp.where(lane == 65, total - high, steps))
        steps_out[...] = steps.reshape(PEERS, ROWS, 128).astype(bf16)
        spread(steps_out, steps_in, pair, 9)

    for c in range(4):
        arrived(wr.at[c], 7, rsem.at[c])
        if c < 2:
            part = mm(lhs[:, 0:512], wr[c].reshape(512, 128))
        else:
            part = mm(lhs[:, 0:256], wr[c, 0:4].reshape(256, 128))
            part = part + mm(lhs[:, 512:768], wr[c, 4:8].reshape(256, 128))
        send[c] = part.reshape(PEERS, ROWS, 128).astype(bf16)
        spread(send.at[c], got.at[c], from_me, 5 + c)
    arrived(quarters, 3, rsem.at[10])
    for d in (2, 1, 3):
        for e in (2, 1, 3):
            block = wor.at[d, mine]
            pltpu.make_async_remote_copy(
                block, block, ssem.at[13], rsem.at[13], **over(e)
            ).start()

    pick_x, pick_bc = heads_selection(acc), maps_selection(acc)
    for n in (6, 7, 8, 9, 10, 11, 12, 17, 18):
        loads[n].wait()
    old_x = phw[...].astype(f32).reshape(14, WIDTH)
    old_x = jnp.concatenate([old_x, jnp.zeros((2, WIDTH), f32)], axis=0)
    old_bc = pmw[...].astype(f32).reshape(28, BC)
    old_bc = jnp.concatenate([old_bc, jnp.zeros((4, BC), f32)], axis=0)
    taps_x = hik[...].astype(f32)
    taps_bc = smk[...].astype(f32).reshape(8, BC)

    def own_heads(ref):
        v = ref[...].reshape(1, 2 * HEADS)
        return jnp.where(t == 0, v[:, :HEADS], v[:, HEADS:])

    speed, direct, bias = own_heads(hds), own_heads(hdg), own_heads(ssb)
    gngv = gng[...].astype(f32).reshape(1, 2 * WIDTH)
    out_gain = jnp.where(t == 0, gngv[:, :WIDTH], gngv[:, WIDTH:])

    def total(c):
        return jnp.sum(got[c].astype(f32).reshape(NX, 2, 4, ROWS, 128), axis=2)

    arrived(got.at[0], PEERS - 1, rsem.at[5])

    @pl.when(steps_mine)
    def _():
        arrived(steps_in, 3, rsem.at[9])

    @pl.when(jnp.logical_not(steps_mine))
    def _():
        arrived(steps_in, 4, rsem.at[9])

    tail = jnp.sum(steps_in[...].astype(f32), axis=0)
    lane8 = iota((ROWS, 128), 1)
    squares = jnp.sum(jnp.where((lane8 == 64) | (lane8 == 65), tail, 0.0), axis=1, keepdims=True)
    inv = lax.rsqrt(squares / D + eps)
    sum0 = total(0)
    raw_b = jnp.concatenate([sum0[g, 0] for g in range(GROUPS)], axis=1) * inv
    raw_c = jnp.concatenate([sum0[g, 1] for g in range(GROUPS)], axis=1) * inv
    win_bc = mm(pick_bc, jnp.concatenate([old_bc, raw_b, raw_c], axis=0).astype(bf16))
    cmw[...] = win_bc[64:92].reshape(SEQS, 7, 2, BC).astype(bf16)
    put(1, cmw, cmw_o)
    b_conv = taps_bc[0:1] * win_bc[0:8]
    c_conv = taps_bc[1:2] * win_bc[8:16]
    for k in range(1, 4):
        b_conv = b_conv + taps_bc[2 * k : 2 * k + 1] * win_bc[16 * k : 16 * k + 8]
        c_conv = c_conv + taps_bc[2 * k + 1 : 2 * k + 2] * win_bc[16 * k + 8 : 16 * k + 16]
    b_conv = b_conv * lax.logistic(b_conv)
    c_conv = c_conv * lax.logistic(c_conv)
    step_pre = tail * inv
    step_pre = jnp.where(t == 0, step_pre[:, :HEADS], step_pre[:, HEADS : 2 * HEADS]) + bias
    step = jnp.maximum(step_pre, 0.0) + jnp.log1p(jnp.exp(-jnp.abs(step_pre)))
    decays = pdt[...].reshape(ROWS, HEADS) - speed * step
    cum = mm(jnp.where(same & (c8 <= r8), 1.0, 0.0), decays, precision=HI)
    wide = mm(
        jnp.concatenate([cum, step, jnp.broadcast_to(direct, (ROWS, HEADS))], axis=0),
        expand,
        precision=HI,
    )
    cim[...] = b_conv.reshape(SEQS, PROPS, BC).astype(bf16)
    put(2, cim, cim_o)
    cld[...] = decays.reshape(SEQS, PROPS, HEADS)
    put(3, cld, cld_o)
    from_state, pairs = [], []
    for g in range(GROUPS):
        lanes = slice(g * STATE, g * STATE + STATE)
        c_g = c_conv[:, lanes]
        y0 = mm(c_g.astype(bf16), sb[0, g], 1, 1)
        y1 = mm(c_g.astype(bf16), sb[1, g], 1, 1)
        from_state.append(jnp.where(row < PROPS, y0, y1))
        pairs.append(mm(c_g, b_conv[:, lanes], 1, 1, precision=HI))
    from_state = jnp.exp(wide[0:8]) * jnp.concatenate(from_state, axis=1)
    scores = []
    for d in range(PROPS):
        score = [
            jnp.broadcast_to(
                jnp.sum(jnp.where(c8 == r8 - d, p, 0.0), axis=1, keepdims=True), (ROWS, 128)
            )
            for p in pairs
        ]
        scores.append(jnp.concatenate(score, axis=1))

    def third(v, c):
        starts = [g * GW + (c - 1) * 128 for g in range(GROUPS)]
        return jnp.concatenate([v[:, n : n + 128] for n in starts], axis=1)

    def whole(thirds):
        return jnp.concatenate(
            [v[:, g * 128 : g * 128 + 128] for g in range(GROUPS) for v in thirds], axis=1
        )

    slot = half * NX + x

    def to_pair(block, n):
        for dx, dp in ((2, 1), (2, 0), (1, 1), (3, 1), (1, 0), (3, 0), (0, 1)):
            pltpu.make_async_remote_copy(
                block, block, ssem.at[n], rsem.at[n],
                **at(2 * pair + lax.rem(half + dp, 2), lax.rem(x + dx, NX), t),
            ).start()

    windows, inputs = [], []
    energy = [0.0] * GROUPS
    for c in range(1, 4):
        wide_c, taps_c, old_c = third(wide, c), third(taps_x, c), third(old_x, c)
        cum_w, step_w, direct_w = wide_c[0:8], wide_c[8:16], wide_c[16:24]
        decay_w = [None]
        for d in range(1, PROPS):
            gap = jnp.where((row & 3) >= d, cum_w - pltpu.roll(cum_w, d, 0), 0.0)
            decay_w.append(jnp.exp(gap) * scores[d])
        arrived(got.at[c], PEERS - 1, rsem.at[5 + c])
        sum_c = total(c)
        heads_at = 0 if c == 1 else 1
        raw_x = jnp.concatenate([sum_c[g, heads_at] for g in range(GROUPS)], axis=1) * inv
        gate = jnp.concatenate([sum_c[g, 1 - heads_at] for g in range(GROUPS)], axis=1) * inv
        win_x = mm(pick_x, jnp.concatenate([old_c, raw_x], axis=0).astype(bf16))
        windows.append(win_x[32:46])
        x_conv = taps_c[0:1] * win_x[0:8]
        for k in range(1, 4):
            x_conv = x_conv + taps_c[k : k + 1] * win_x[8 * k : 8 * k + 8]
        x_conv = x_conv * lax.logistic(x_conv)
        weighted = step_w * x_conv
        inputs.append(weighted)
        heads = third(from_state, c) + direct_w * x_conv + scores[0] * weighted
        for d in range(1, PROPS):
            term = decay_w[d] * pltpu.roll(weighted, d, 0)
            heads = heads + jnp.where((row & 3) >= d, term, 0.0)
        gated = heads * (gate * lax.logistic(gate))
        for g in range(GROUPS):
            part_g = gated[:, g * 128 : g * 128 + 128]
            energy[g] = energy[g] + jnp.sum(part_g * part_g, axis=1, keepdims=True)
        gated = gated * third(out_gain, c)
        if c < 3:
            nrm[c - 1, slot] = gated.astype(bf16)
            to_pair(nrm.at[c - 1, slot], 15 + c)
            continue
        factors = jnp.zeros((ROWS, 128), f32)
        for g in range(GROUPS):
            factor = lax.rsqrt(energy[g] / GW + eps)
            high = factor.astype(bf16).astype(f32)
            factors = jnp.where(lane8 == g, high, factors)
            factors = jnp.where(lane8 == GROUPS + g, factor - high, factors)
        last[slot] = jnp.concatenate([gated, factors], axis=1).astype(bf16)
        to_pair(last.at[slot], 18)
    chw[...] = whole(windows).reshape(7, SEQS, WIDTH).astype(bf16)
    put(4, chw, chw_o)
    chi[...] = whole(inputs).reshape(SEQS, PROPS, WIDTH).astype(bf16)
    put(5, chi, chi_o)

    arrived(three_quarters, 3, rsem.at[13])
    columns_of = wor[...].reshape(256, WIDTH)
    products = [jnp.zeros((64, 256), f32)] * GROUPS
    for c in range(1, 4):
        if c < 3:
            arrived(nrm.at[c - 1], 7, rsem.at[15 + c])
            rows64 = nrm[c - 1].astype(f32).reshape(64, 512).astype(bf16)
        else:
            arrived(last, 7, rsem.at[18])
            rows64 = last[:, :, 0:512].astype(f32).reshape(64, 512).astype(bf16)
        for g in range(GROUPS):
            start = g * GW + (c - 1) * 128
            products[g] = products[g] + mm(
                rows64[:, g * 128 : g * 128 + 128], columns_of[:, start : start + 128], 1, 1
            )
    factors = last[:, :, 512:640].astype(f32).reshape(64, 128)
    factors = factors + pltpu.roll(factors, 128 - GROUPS, 1)
    partial = factors[:, 0:1] * products[0]
    for g in range(1, GROUPS):
        partial = partial + factors[:, g : g + 1] * products[g]
    first_lanes = iota((32, 128), 1) < 64
    for d in (2, 3, 1, 0):
        both = partial[:, 128 * (d // 2) : 128 * (d // 2) + 128]
        turned = pltpu.roll(both, 64, 1)
        low, high = (both, turned) if d % 2 == 0 else (turned, both)
        fs[d] = jnp.where(first_lanes, low[:32], high[32:]).astype(bf16)
        zz, there = lax.rem(z + 2 * d, NZ), fr.at[pair * NT + t]
        if d == 0:
            put(6, fs.at[0], there)
        else:
            pltpu.make_async_remote_copy(
                fs.at[d], there, ssem.at[12], rsem.at[12], **at(zz, x, t)
            ).start()
        pltpu.make_async_remote_copy(
            fs.at[d], there, ssem.at[12], rsem.at[12], **at(zz, x, 1 - t)
        ).start()
    arrived(fr, 7, rsem.at[12])

    @pl.when(t == 1)
    def _():
        arrived(tt, 11, ssem.at[14])

    @pl.when(jnp.logical_not(steps_mine))
    def _():
        pltpu.make_async_copy(squares_out, squares_out, ssem.at[15]).wait()

    for c in range(4):
        arrived(wr.at[c], 7, ssem.at[c])
        arrived(send.at[c], PEERS - 1, ssem.at[5 + c])

    @pl.when(steps_mine)
    def _():
        arrived(steps_out, PEERS - 1, ssem.at[9])

    arrived(quarters, 3, ssem.at[10])
    arrived(three_quarters, 3, ssem.at[13])
    for c in range(2):
        arrived(nrm.at[c], 7, ssem.at[16 + c])
    arrived(last, 7, ssem.at[18])
    arrived(fr, 7, ssem.at[12])
    for copy in outs:
        copy.wait()


def finish(fr_h, *refs):
    ins, outs, fr, mixed, mids, sems = (
        refs[:6], refs[7:13], refs[13], refs[14], refs[15:21], refs[21],
    )
    mixed_o = refs[6]

    def pieces(ref, n):
        if n > 0:
            return [ref]
        return [ref.at[b, pl.ds(h, 6)] for b in range(SEQS) for h in range(0, HEADS, 6)]

    trio = [
        piece
        for n in (1, 2, 3, 4, 5, 0)
        for piece in zip(pieces(ins[n], n), pieces(mids[n], n), pieces(outs[n], n))
    ]
    head = pltpu.make_async_copy(fr_h, fr, sems.at[0])
    head.start()
    first = [pltpu.make_async_copy(a, b, sems.at[1 + n]) for n, (a, b, _) in enumerate(trio)]
    second = [pltpu.make_async_copy(b, c, sems.at[14 + n]) for n, (_, b, c) in enumerate(trio)]
    for copy in first:
        copy.start()
    head.wait()
    done = fr[...].astype(f32).reshape(4, NT, 32, 128)
    done = done[:, 0] + done[:, 1]
    done = jnp.stack([done[:, :, :64], done[:, :, 64:]], axis=1)
    mixed[...] = done.reshape(64, PROPS, 64).astype(bf16)
    last = pltpu.make_async_copy(mixed, mixed_o, sems.at[27])
    last.start()
    for a, b in zip(first, second):
        a.wait()
        b.start()
    for copy in second:
        copy.wait()
    last.wait()


def local(
    tokens, input_norm_gain, head_input_weight, output_gate_weight, state_maps_weight,
    step_size_weight, step_size_bias, head_decay_speed, proposal_decay_total, head_input_kernel,
    state_maps_kernel, head_direct_gain, grouped_norm_gain, output_weight, prior_state_value,
    previous_head_input, previous_input_maps, previous_log_decays, prior_heads_window,
    prior_maps_window, accepted,
):
    anywhere = pl.BlockSpec(memory_space=pl.ANY)
    V, DMA = pltpu.VMEM, pltpu.SemaphoreType.DMA
    outs = (
        jax.ShapeDtypeStruct((NX * NT, 32, 128), bf16),
        jax.ShapeDtypeStruct((SEQS, HEADS, HEAD_DIM, STATE), f32),
        jax.ShapeDtypeStruct((SEQS, PROPS, WIDTH), bf16),
        jax.ShapeDtypeStruct((SEQS, PROPS, BC), bf16),
        jax.ShapeDtypeStruct((SEQS, PROPS, HEADS), f32),
        jax.ShapeDtypeStruct((7, SEQS, WIDTH), bf16),
        jax.ShapeDtypeStruct((SEQS, 7, 2, BC), bf16),
    )
    results = pl.pallas_call(
        kernel,
        out_shape=outs,
        in_specs=[anywhere] * 21,
        out_specs=[anywhere] * 7,
        scratch_shapes=[
            V((64, PROPS, 64), bf16), V((D,), bf16), V((2, 64, WIDTH), bf16),
            V((64, 2, BC), bf16), V((48,), f32), V((48,), f32), V((SEQS, PROPS, HEADS), f32),
            V((4, WIDTH), bf16), V((4, 2, BC), bf16), V((48,), f32), V((2 * WIDTH,), bf16),
            V((64, WIDTH), bf16), V((SEQS, HEADS, HEAD_DIM, STATE), f32),
            V((SEQS, PROPS, WIDTH), bf16), V((SEQS, PROPS, BC), bf16),
            V((SEQS, PROPS, HEADS), f32), V((7, SEQS, WIDTH), bf16), V((SEQS, 7, 2, BC), bf16),
            V((128, 512), bf16), V((8, 64, 128), bf16), V((12, 64, 256), bf16), V((16, 256), bf16), V((8, 16, 256), bf16),
            V((256, 768), bf16), V((4, 8, 64, 128), bf16), V((4, PEERS, ROWS, 128), bf16),
            V((4, PEERS, ROWS, 128), bf16), V((PEERS, ROWS, 128), bf16), V((4, ROWS, 128), bf16),
            V((NX, 64, WIDTH), bf16), V((SEQS, GROUPS, GW, STATE), bf16),
            V((2, 8, ROWS, 512), bf16), V((8, ROWS, 640), bf16), V((NX, 32, 128), bf16),
            V((SEQS, PROPS, WIDTH), bf16), V((SEQS, PROPS, BC), bf16),
            V((SEQS, PROPS, HEADS), f32), V((7, SEQS, WIDTH), bf16), V((SEQS, 7, 2, BC), bf16),
            pltpu.SMEM((SEQS,), i32), DMA((21,)), DMA((19,)), DMA((19,)), DMA((7,)),
            pltpu.SemaphoreType.REGULAR((3, 2)),
        ],
        compiler_params=pltpu.CompilerParams(
            collective_id=0, has_side_effects=True, vmem_limit_bytes=60 * 1024 * 1024
        ),
    )(
        tokens, input_norm_gain, head_input_weight, output_gate_weight, state_maps_weight,
        step_size_weight.T, step_size_bias, head_decay_speed, proposal_decay_total,
        head_input_kernel, state_maps_kernel, head_direct_gain, grouped_norm_gain,
        output_weight.T, prior_state_value, previous_head_input, previous_input_maps,
        previous_log_decays, jnp.transpose(prior_heads_window, (1, 0, 2)), prior_maps_window,
        accepted,
    )
    finals = (jax.ShapeDtypeStruct((64, PROPS, 64), bf16), *outs[1:])
    mixed, state, chi, cim, cld, chw, cmw = pl.pallas_call(
        finish,
        out_shape=finals,
        in_specs=[anywhere] * 7,
        out_specs=[anywhere] * 7,
        scratch_shapes=[
            V((NX * NT, 32, 128), bf16), V((64, PROPS, 64), bf16),
            *(V(o.shape, o.dtype) for o in outs[1:]), DMA((28,)),
        ],
    )(*results)
    return mixed, state, chi, cim, cld, jnp.transpose(chw, (1, 0, 2)), cmw


def solution(mesh):
    seq = ("dp", "kv")
    return jax.shard_map(
        local,
        mesh=mesh,
        in_specs=(
            P("dp", None, "kv"), P(), P("kv", "tp"), P("kv", "tp"), P("kv", None, "tp"), P(), P(),
            P(), P(seq, None, "tp"), P(), P(), P(), P(), P("tp", "kv"), P(seq, "tp", None, None),
            P(seq, None, "tp"), P(seq, None, "tp"), P(seq, None, "tp"), P(seq, None, "tp"),
            P(seq, None, None, "tp"), P(seq),
        ),
        out_specs=(
            P("dp", None, "kv"), P(seq, "tp", None, None), P(seq, None, "tp"), P(seq, None, "tp"),
            P(seq, None, "tp"), P(seq, None, "tp"), P(seq, None, None, "tp"),
        ),
        check_vma=False,
    )
```

```python
import functools

import jax
import jax.numpy as jnp
from jax import lax
from jax.experimental import pallas as pl
from jax.experimental.pallas import tpu as pltpu
from jax.sharding import PartitionSpec as P

MESH = pl.DeviceIdType.MESH
HI = lax.Precision.HIGHEST
f32, bf16, i32 = jnp.float32, jnp.bfloat16, jnp.int32

NX, NY, NZ, NT = 4, 4, 8, 2
PEERS = NX * NZ
D, STATE, HEAD_DIM = 2048, 128, 64
SEQS, PROPS, ROWS = 2, 4, 8
HEADS, GROUPS, PER = 24, 4, 6
WIDTH, GW = 1536, 384
BC = 512
eps = 1e-06


def iota(shape, dim):
    return lax.broadcasted_iota(i32, shape, dim)


def mm(a, b, ca=1, cb=0, precision=None):
    return lax.dot_general(
        a, b, (((ca,), (cb,)), ((), ())), precision=precision, preferred_element_type=f32
    )


def heads_selection(acc):
    shape = (48, 24)
    i, j = iota(shape, 0), iota(shape, 1)
    out = i >= 32
    b = jnp.where(out, i & 1, (i >> 2) & 1)
    pos = jnp.where(out, (i - 32) >> 1, (i & 3) + (i >> 3))
    acc_b = jnp.where(b == 0, acc[0], acc[1])
    old = (j < 14) & ((j & 1) == b) & ((j >> 1) == acc_b + pos)
    raw = (j >= 16) & (((j - 16) >> 2) == b) & (((j - 16) & 3) == pos - 3)
    pick = jnp.where(pos < 3, jnp.where(old, 1.0, 0.0), jnp.where(raw, 1.0, 0.0))
    return pick.astype(bf16)


def maps_selection(acc):
    shape = (96, 48)
    i, j = iota(shape, 0), iota(shape, 1)
    out = i >= 64
    o = i - 64
    ob = jnp.where(o >= 14, 1, 0)
    orem = o - 14 * ob
    b = jnp.where(out, ob, (i >> 2) & 1)
    pos = jnp.where(out, orem >> 1, (i & 3) + (i >> 4))
    kind = jnp.where(out, orem & 1, (i >> 3) & 1)
    acc_b = jnp.where(b == 0, acc[0], acc[1])
    jb = jnp.where(j >= 14, 1, 0)
    jrem = j - 14 * jb
    old = (j < 28) & (jb == b) & ((jrem & 1) == kind) & ((jrem >> 1) == acc_b + pos)
    jr = j - 32
    raw = (j >= 32) & ((jr >> 3) == kind) & (((jr >> 2) & 1) == b) & ((jr & 3) == pos - 3)
    pick = jnp.where(pos < 3, jnp.where(old, 1.0, 0.0), jnp.where(raw, 1.0, 0.0))
    return pick.astype(bf16)


def kernel(
    tok_h, gain_h, wx_h, wg_h, smw_h, sw_h, ssb_h, hds_h, pdt_h, hik_h, smk_h, hdg_h, gng_h, wo_h,
    psv_h, phi_h, pim_h, pld_h, phw_h, pmw_h, acc_h,
    fr, state, chi, cim, cld, chw, cmw,
    tok, gain, wxg, smw, ssb, hds, pdt, hik, smk, hdg, gng, wo, psv, phi, pim, pld, phw, pmw,
    sw, bcs, tt, squares_out, squares_in, lhs, wr, send, got, steps_out, steps_in, wor, sb, nrm, last, fs,
    acc_s, lsem, ssem, rsem, level_sem,
):
    y, kv, t = lax.axis_index("dp"), lax.axis_index("kv"), lax.axis_index("tp")
    z, x = kv // NX, kv % NX
    pair, half = z // 2, z % 2

    def at(zz, xx, tt_):
        return dict(device_id=(y, zz * NX + xx, tt_), device_id_type=MESH)

    def over(d):
        return dict(device_id=(lax.rem(y + d, NY), kv, t), device_id_type=MESH)

    def served(e):
        return lax.rem(z + (2 * half - 1) * e + NZ, NZ)

    def server(e):
        return lax.rem(z + (1 - 2 * ((half + e) % 2)) * e + NZ, NZ)

    loads = {}
    plan = (
        (tok_h, tok), (gain_h, gain), (smw_h, smw), (wx_h, wxg.at[0]), (wg_h, wxg.at[1]),
        (sw_h.at[:, pl.ds(pl.multiple_of(pair * 512, 512), 512)], sw.at[pl.ds(0, 48)]),
        (ssb_h, ssb), (hds_h, hds), (pdt_h, pdt),
        (hik_h.at[:, pl.ds(pl.multiple_of(t * WIDTH, 128), WIDTH)], hik),
        (smk_h.at[:, :, pl.ds(pl.multiple_of(t * BC, 128), BC)], smk),
        (hdg_h, hdg), (gng_h, gng), (wo_h, wo), (phi_h, phi), (pim_h, pim), (pld_h, pld),
        (phw_h, phw), (pmw_h, pmw), (psv_h, psv), (acc_h, acc_s),
    )
    for n, (src, dst) in enumerate(plan):
        loads[n] = pltpu.make_async_copy(src, dst, lsem.at[n])
    for n in (0, 1, 2):
        loads[n].start()

    barrier = pltpu.get_barrier_semaphore()

    row_peers = [(0, 2), (0, 1), (0, 3)]
    up_peers = [(1, 2), (1, 1), (1, 3), (1, 0)]
    down_peers = [(NZ - 1, dx) for _, dx in up_peers]

    def near(dz, dx):
        return lax.rem(x + dx, NX), at(lax.rem(z + dz, NZ), lax.rem(x + dx, NX), t)

    for dz, dx in row_peers + up_peers + down_peers:
        pl.semaphore_signal(barrier, inc=1, **near(dz, dx)[1])
    for d in range(NX):
        pl.semaphore_signal(barrier, inc=1, **at(z, lax.rem(x + d, NX), 1 - t))
    for d in range(1, NY):
        pl.semaphore_signal(barrier, inc=1, **over(d))
    for e in (2, 3):
        pl.semaphore_signal(barrier, inc=1, **at(served(e), x, t))
    for n in range(3, len(plan)):
        loads[n].start()

    for n in (0, 1, 2):
        loads[n].wait()
    tok32 = tok[...].astype(f32).reshape(256, 64)
    gains = gain[...].astype(f32).reshape(16, 128)
    gain_row = jnp.sum(
        jnp.where(iota((16, 128), 0) == kv // 2, gains, 0.0), axis=0, keepdims=True
    )
    gain_row = jnp.where(kv % 2 == 0, gain_row[:, :64], gain_row[:, 64:])
    tt[x, 0:64] = (tok32 * gain_row).astype(bf16).T
    sumsq = jnp.sum(jnp.square(tok32.T), axis=0, keepdims=True)
    high = sumsq.astype(bf16).astype(f32)
    line = iota((16, 256), 0)
    squares_out[...] = jnp.where(
        line == 0, high, jnp.where(line == 1, sumsq - high, 0.0)
    ).astype(bf16)
    for n in range(2):
        part = smw[:, n, :]
        for g in range(GROUPS):
            bcs[n * GROUPS + g] = part[:, g * STATE : g * STATE + STATE]
    sw[48:128] = jnp.zeros((80, 512), bf16)

    def columns(c, h, xx):
        if c == 0:
            return bcs.at[h * NX + xx]
        return wxg.at[
            h if c == 1 else 1 - h, :, pl.ds(pl.multiple_of(xx * GW + (c - 1) * 128, 128), 128)
        ]

    loads[3].wait()
    loads[4].wait()
    for c in range(4):
        wr[c, x] = columns(c, half, x)[...]

    pl.semaphore_wait(barrier, 11 + NX + NY - 1 + 2)

    def pass_on(level):
        for n, dz in enumerate((1, NZ - 1)):
            pl.semaphore_signal(level_sem.at[level, n], inc=1, **near(dz, 0)[1])

    def hear(level):
        for n in range(2):
            pl.semaphore_wait(level_sem.at[level, n], 1)

    pass_on(0)

    @pl.when(t == 1)
    def _():
        for peers, base in ((up_peers, 8), (down_peers, 4), (row_peers, 0)):
            for dz, dx in peers:
                pltpu.make_async_remote_copy(
                    tt.at[x], tt.at[base + x], ssem.at[4], rsem.at[4], **near(dz, dx)[1]
                ).start()

    def send_weights(c):
        for peers, h, base in (
            (down_peers if c < 2 else up_peers, 1 - half, 4),
            (row_peers, half, 0),
        ):
            for dz, dx in peers:
                xx, to = near(dz, dx)
                pltpu.make_async_remote_copy(
                    columns(c, h, xx), wr.at[c, base + x], ssem.at[c], rsem.at[c], **to
                ).start()

    loads[13].wait()
    wor[0] = wo[...]
    mine = pl.ds(pl.multiple_of(y * 16, 16), 16)

    def send_output_weights():
        for e in (3, 2, 1):
            pltpu.make_async_remote_copy(
                wo.at[mine], wor.at[e, mine], ssem.at[10], rsem.at[10], **at(server(e), x, t)
            ).start()

    @pl.when(t == 0)
    def _():
        send_output_weights()

    steps_mine = (half == 0) & (x == pair)

    @pl.when(jnp.logical_not(steps_mine))
    def _():
        pltpu.make_async_remote_copy(
            squares_out, squares_in.at[half * NX + x], ssem.at[15], rsem.at[15],
            **at(2 * pair, pair, t),
        ).start()

    def arrived(buffer, count, sem):
        block = buffer.at[pl.ds(0, count)]
        pltpu.make_async_copy(block, block, sem).wait()

    loads[20].wait()
    acc = (acc_s[0], acc_s[1])
    row = iota((ROWS, 1), 0)
    acc_row = jnp.where(row < PROPS, acc[0], acc[1])
    keep = jnp.where((row & 3) < acc_row, 1.0, 0.0)
    r8, c8 = iota((ROWS, ROWS), 0), iota((ROWS, ROWS), 1)
    same = (r8 >> 2) == (c8 >> 2)
    expand = jnp.where(iota((HEADS, WIDTH), 1) // HEAD_DIM == iota((HEADS, WIDTH), 0), 1.0, 0.0)
    for n in (14, 15, 16):
        loads[n].wait()
    kept = pld[...].reshape(ROWS, HEADS) * keep
    later = mm(jnp.where(same & (c8 > r8), 1.0, 0.0), kept, precision=HI)
    coef = mm(keep * jnp.exp(later), expand, precision=HI)
    scaled = coef * phi[...].astype(f32).reshape(ROWS, WIDTH)
    s_hi = scaled.astype(bf16)
    s_lo = (scaled - s_hi.astype(f32)).astype(bf16)
    updates = jnp.concatenate([s_hi.astype(f32), s_lo.astype(f32)], axis=0).astype(bf16)
    keys = pim[...].astype(f32).reshape(ROWS, BC)
    loads[19].wait()
    for b in range(SEQS):
        of_b = (row >> 2) == b
        logs = mm(jnp.where(of_b, kept, 0.0), jnp.ones((ROWS, STATE), f32), 0, 0, precision=HI)
        factor = jnp.exp(logs)
        keys_b = jnp.where(of_b, keys, 0.0)
        keys_b = jnp.concatenate([keys_b, keys_b], axis=0).astype(bf16)
        for g in range(GROUPS):
            upd = mm(
                updates[:, g * GW : g * GW + GW], keys_b[:, g * STATE : g * STATE + STATE], 0, 0
            )
            new = (
                psv[b, g * PER : g * PER + PER] * factor[g * PER : g * PER + PER][:, None, :]
                + upd.reshape(PER, HEAD_DIM, STATE)
            )
            state[b, g * PER : g * PER + PER] = new
            sb[b, g] = new.reshape(GW, STATE).astype(bf16)

    @pl.when(t == 1)
    def _():
        arrived(tt, 11, ssem.at[4])

    for c in range(4):
        send_weights(c)
    @pl.when(t == 1)
    def _():
        send_output_weights()

    quarters = wor.at[:, pl.ds(0, 16)]
    three_quarters = wor.at[:, pl.ds(0, 48)]

    from_me = (x * 2 + half) * 4 + pair

    def spread(src, dst, index, n):
        def one(d, _):
            other = lax.rem(kv + d, PEERS)
            pltpu.make_async_remote_copy(
                src.at[other],
                dst.at[index],
                ssem.at[n],
                rsem.at[n],
                device_id=(y, other, t),
                device_id_type=MESH,
            ).start()
            return 0

        lax.fori_loop(1, PEERS, one, 0)
        dst[index] = src[kv]

    for level in range(3):
        hear(level)
        if level < 2:
            pass_on(level + 1)


    @pl.when(t == 1)
    def _():
        arrived(tt, 11, rsem.at[4])
        blocks = [tt.at[pl.ds(4, 8)]]
        blocks += [tt.at[lax.rem(x + d, NX)] for d in range(1, NX)]
        for block in blocks:
            pltpu.make_async_remote_copy(
                block, block, ssem.at[14], rsem.at[14], **at(z, x, 1 - t)
            ).start()

    @pl.when(t == 0)
    def _():
        arrived(tt, 11, rsem.at[14])

    lhs[...] = tt[...].reshape(768, 256).T
    loads[5].wait()

    @pl.when(steps_mine)
    def _():
        steps = mm(lhs[:, 0:512], sw[...], 1, 1)
        arrived(squares_in, 7, rsem.at[15])
        squares_in[half * NX + x] = squares_out[...]
        squares = jnp.sum(squares_in[...].astype(f32), axis=0)
        pick = jnp.where(
            (iota((16, 128), 1) == 64) & (iota((16, 128), 0) < 2), 1.0, 0.0
        )
        squares = mm(squares, pick, 0, 0, precision=HI)
        total = squares[:, 64:65]
        high = total.astype(bf16).astype(f32)
        lane = iota((256, 128), 1)
        steps = jnp.where(lane == 64, high, jnp.where(lane == 65, total - high, steps))
        steps_out[...] = steps.reshape(PEERS, ROWS, 128).astype(bf16)
        spread(steps_out, steps_in, pair, 9)

    for c in range(4):
        arrived(wr.at[c], 7, rsem.at[c])
        if c < 2:
            part = mm(lhs[:, 0:512], wr[c].reshape(512, 128))
        else:
            part = mm(lhs[:, 0:256], wr[c, 0:4].reshape(256, 128))
            part = part + mm(lhs[:, 512:768], wr[c, 4:8].reshape(256, 128))
        send[c] = part.reshape(PEERS, ROWS, 128).astype(bf16)
        spread(send.at[c], got.at[c], from_me, 5 + c)
    arrived(quarters, 3, rsem.at[10])
    for d in (2, 1, 3):
        for e in (2, 1, 3):
            block = wor.at[d, mine]
            pltpu.make_async_remote_copy(
                block, block, ssem.at[13], rsem.at[13], **over(e)
            ).start()

    pick_x, pick_bc = heads_selection(acc), maps_selection(acc)
    for n in (6, 7, 8, 9, 10, 11, 12, 17, 18):
        loads[n].wait()
    old_x = phw[...].astype(f32).reshape(14, WIDTH)
    old_x = jnp.concatenate([old_x, jnp.zeros((2, WIDTH), f32)], axis=0)
    old_bc = pmw[...].astype(f32).reshape(28, BC)
    old_bc = jnp.concatenate([old_bc, jnp.zeros((4, BC), f32)], axis=0)
    taps_x = hik[...].astype(f32)
    taps_bc = smk[...].astype(f32).reshape(8, BC)

    def own_heads(ref):
        v = ref[...].reshape(1, 2 * HEADS)
        return jnp.where(t == 0, v[:, :HEADS], v[:, HEADS:])

    speed, direct, bias = own_heads(hds), own_heads(hdg), own_heads(ssb)
    gngv = gng[...].astype(f32).reshape(1, 2 * WIDTH)
    out_gain = jnp.where(t == 0, gngv[:, :WIDTH], gngv[:, WIDTH:])

    def total(c):
        return jnp.sum(got[c].astype(f32).reshape(NX, 2, 4, ROWS, 128), axis=2)

    arrived(got.at[0], PEERS - 1, rsem.at[5])

    @pl.when(steps_mine)
    def _():
        arrived(steps_in, 3, rsem.at[9])

    @pl.when(jnp.logical_not(steps_mine))
    def _():
        arrived(steps_in, 4, rsem.at[9])

    tail = jnp.sum(steps_in[...].astype(f32), axis=0)
    lane8 = iota((ROWS, 128), 1)
    squares = jnp.sum(jnp.where((lane8 == 64) | (lane8 == 65), tail, 0.0), axis=1, keepdims=True)
    inv = lax.rsqrt(squares / D + eps)
    sum0 = total(0)
    raw_b = jnp.concatenate([sum0[g, 0] for g in range(GROUPS)], axis=1) * inv
    raw_c = jnp.concatenate([sum0[g, 1] for g in range(GROUPS)], axis=1) * inv
    win_bc = mm(pick_bc, jnp.concatenate([old_bc, raw_b, raw_c], axis=0).astype(bf16))
    cmw[...] = win_bc[64:92].reshape(SEQS, 7, 2, BC).astype(bf16)
    b_conv = taps_bc[0:1] * win_bc[0:8]
    c_conv = taps_bc[1:2] * win_bc[8:16]
    for k in range(1, 4):
        b_conv = b_conv + taps_bc[2 * k : 2 * k + 1] * win_bc[16 * k : 16 * k + 8]
        c_conv = c_conv + taps_bc[2 * k + 1 : 2 * k + 2] * win_bc[16 * k + 8 : 16 * k + 16]
    b_conv = b_conv * lax.logistic(b_conv)
    c_conv = c_conv * lax.logistic(c_conv)
    step_pre = tail * inv
    step_pre = jnp.where(t == 0, step_pre[:, :HEADS], step_pre[:, HEADS : 2 * HEADS]) + bias
    step = jnp.maximum(step_pre, 0.0) + jnp.log1p(jnp.exp(-jnp.abs(step_pre)))
    decays = pdt[...].reshape(ROWS, HEADS) - speed * step
    cum = mm(jnp.where(same & (c8 <= r8), 1.0, 0.0), decays, precision=HI)
    wide = mm(
        jnp.concatenate([cum, step, jnp.broadcast_to(direct, (ROWS, HEADS))], axis=0),
        expand,
        precision=HI,
    )
    cim[...] = b_conv.reshape(SEQS, PROPS, BC).astype(bf16)
    cld[...] = decays.reshape(SEQS, PROPS, HEADS)
    from_state, pairs = [], []
    for g in range(GROUPS):
        lanes = slice(g * STATE, g * STATE + STATE)
        c_g = c_conv[:, lanes]
        y0 = mm(c_g.astype(bf16), sb[0, g], 1, 1)
        y1 = mm(c_g.astype(bf16), sb[1, g], 1, 1)
        from_state.append(jnp.where(row < PROPS, y0, y1))
        pairs.append(mm(c_g, b_conv[:, lanes], 1, 1, precision=HI))
    from_state = jnp.exp(wide[0:8]) * jnp.concatenate(from_state, axis=1)
    scores = []
    for d in range(PROPS):
        score = [
            jnp.broadcast_to(
                jnp.sum(jnp.where(c8 == r8 - d, p, 0.0), axis=1, keepdims=True), (ROWS, 128)
            )
            for p in pairs
        ]
        scores.append(jnp.concatenate(score, axis=1))

    def third(v, c):
        starts = [g * GW + (c - 1) * 128 for g in range(GROUPS)]
        return jnp.concatenate([v[:, n : n + 128] for n in starts], axis=1)

    def whole(thirds):
        return jnp.concatenate(
            [v[:, g * 128 : g * 128 + 128] for g in range(GROUPS) for v in thirds], axis=1
        )

    slot = half * NX + x

    def to_pair(block, n):
        for dx, dp in ((2, 1), (2, 0), (1, 1), (3, 1), (1, 0), (3, 0), (0, 1)):
            pltpu.make_async_remote_copy(
                block, block, ssem.at[n], rsem.at[n],
                **at(2 * pair + lax.rem(half + dp, 2), lax.rem(x + dx, NX), t),
            ).start()

    windows, inputs = [], []
    energy = [0.0] * GROUPS
    for c in range(1, 4):
        wide_c, taps_c, old_c = third(wide, c), third(taps_x, c), third(old_x, c)
        cum_w, step_w, direct_w = wide_c[0:8], wide_c[8:16], wide_c[16:24]
        decay_w = [None]
        for d in range(1, PROPS):
            gap = jnp.where((row & 3) >= d, cum_w - pltpu.roll(cum_w, d, 0), 0.0)
            decay_w.append(jnp.exp(gap) * scores[d])
        arrived(got.at[c], PEERS - 1, rsem.at[5 + c])
        sum_c = total(c)
        heads_at = 0 if c == 1 else 1
        raw_x = jnp.concatenate([sum_c[g, heads_at] for g in range(GROUPS)], axis=1) * inv
        gate = jnp.concatenate([sum_c[g, 1 - heads_at] for g in range(GROUPS)], axis=1) * inv
        win_x = mm(pick_x, jnp.concatenate([old_c, raw_x], axis=0).astype(bf16))
        windows.append(win_x[32:46])
        x_conv = taps_c[0:1] * win_x[0:8]
        for k in range(1, 4):
            x_conv = x_conv + taps_c[k : k + 1] * win_x[8 * k : 8 * k + 8]
        x_conv = x_conv * lax.logistic(x_conv)
        weighted = step_w * x_conv
        inputs.append(weighted)
        heads = third(from_state, c) + direct_w * x_conv + scores[0] * weighted
        for d in range(1, PROPS):
            term = decay_w[d] * pltpu.roll(weighted, d, 0)
            heads = heads + jnp.where((row & 3) >= d, term, 0.0)
        gated = heads * (gate * lax.logistic(gate))
        for g in range(GROUPS):
            part_g = gated[:, g * 128 : g * 128 + 128]
            energy[g] = energy[g] + jnp.sum(part_g * part_g, axis=1, keepdims=True)
        gated = gated * third(out_gain, c)
        if c < 3:
            nrm[c - 1, slot] = gated.astype(bf16)
            to_pair(nrm.at[c - 1, slot], 15 + c)
            continue
        factors = jnp.zeros((ROWS, 128), f32)
        for g in range(GROUPS):
            factor = lax.rsqrt(energy[g] / GW + eps)
            high = factor.astype(bf16).astype(f32)
            factors = jnp.where(lane8 == g, high, factors)
            factors = jnp.where(lane8 == GROUPS + g, factor - high, factors)
        last[slot] = jnp.concatenate([gated, factors], axis=1).astype(bf16)
        to_pair(last.at[slot], 18)
    chw[...] = whole(windows).reshape(7, SEQS, WIDTH).astype(bf16)
    chi[...] = whole(inputs).reshape(SEQS, PROPS, WIDTH).astype(bf16)

    arrived(three_quarters, 3, rsem.at[13])
    columns_of = wor[...].reshape(256, WIDTH)
    products = [jnp.zeros((64, 256), f32)] * GROUPS
    for c in range(1, 4):
        if c < 3:
            arrived(nrm.at[c - 1], 7, rsem.at[15 + c])
            rows64 = nrm[c - 1].astype(f32).reshape(64, 512).astype(bf16)
        else:
            arrived(last, 7, rsem.at[18])
            rows64 = last[:, :, 0:512].astype(f32).reshape(64, 512).astype(bf16)
        for g in range(GROUPS):
            start = g * GW + (c - 1) * 128
            products[g] = products[g] + mm(
                rows64[:, g * 128 : g * 128 + 128], columns_of[:, start : start + 128], 1, 1
            )
    factors = last[:, :, 512:640].astype(f32).reshape(64, 128)
    factors = factors + pltpu.roll(factors, 128 - GROUPS, 1)
    partial = factors[:, 0:1] * products[0]
    for g in range(1, GROUPS):
        partial = partial + factors[:, g : g + 1] * products[g]
    first_lanes = iota((32, 128), 1) < 64
    for d in (3, 2, 1, 0):
        both = partial[:, 128 * (d // 2) : 128 * (d // 2) + 128]
        turned = pltpu.roll(both, 64, 1)
        low, high = (both, turned) if d % 2 == 0 else (turned, both)
        fs[d] = jnp.where(first_lanes, low[:32], high[32:]).astype(bf16)
        zz, there = served(d), fr.at[pair * NT + t]
        if d == 0:
            fr[pair * NT + t] = fs[0]
        else:
            pltpu.make_async_remote_copy(
                fs.at[d], there, ssem.at[12], rsem.at[12], **at(zz, x, t)
            ).start()
        pltpu.make_async_remote_copy(
            fs.at[d], there, ssem.at[12], rsem.at[12], **at(zz, x, 1 - t)
        ).start()
    arrived(fr, 7, rsem.at[12])

    @pl.when(t == 1)
    def _():
        arrived(tt, 11, ssem.at[14])

    @pl.when(jnp.logical_not(steps_mine))
    def _():
        pltpu.make_async_copy(squares_out, squares_out, ssem.at[15]).wait()

    for c in range(4):
        arrived(wr.at[c], 7, ssem.at[c])
        arrived(send.at[c], PEERS - 1, ssem.at[5 + c])

    @pl.when(steps_mine)
    def _():
        arrived(steps_out, PEERS - 1, ssem.at[9])

    arrived(quarters, 3, ssem.at[10])
    arrived(three_quarters, 3, ssem.at[13])
    for c in range(2):
        arrived(nrm.at[c], 7, ssem.at[16 + c])
    arrived(last, 7, ssem.at[18])
    arrived(fr, 7, ssem.at[12])


def finish(fr, *refs):
    ins, outs, mixed, sems = refs[:6], refs[6:13], refs[13], refs[14]
    copies = [
        pltpu.make_async_copy(a, b, sems.at[n]) for n, (a, b) in enumerate(zip(ins, outs[1:]))
    ]
    for copy in copies:
        copy.start()
    done = fr[...].astype(f32).reshape(4, NT, 32, 128)
    done = done[:, 0] + done[:, 1]
    done = jnp.stack([done[:, :, :64], done[:, :, 64:]], axis=1)
    mixed[...] = done.reshape(64, PROPS, 64).astype(bf16)
    copies.append(pltpu.make_async_copy(mixed, outs[0], sems.at[6]))
    copies[-1].start()
    for copy in copies:
        copy.wait()


def local(
    tokens, input_norm_gain, head_input_weight, output_gate_weight, state_maps_weight,
    step_size_weight, step_size_bias, head_decay_speed, proposal_decay_total, head_input_kernel,
    state_maps_kernel, head_direct_gain, grouped_norm_gain, output_weight, prior_state_value,
    previous_head_input, previous_input_maps, previous_log_decays, prior_heads_window,
    prior_maps_window, accepted,
):
    anywhere = pl.BlockSpec(memory_space=pl.ANY)
    vmem = pl.BlockSpec(memory_space=pltpu.VMEM)
    V, DMA = pltpu.VMEM, pltpu.SemaphoreType.DMA
    outs = (
        jax.ShapeDtypeStruct((NX * NT, 32, 128), bf16),
        jax.ShapeDtypeStruct((SEQS, HEADS, HEAD_DIM, STATE), f32),
        jax.ShapeDtypeStruct((SEQS, PROPS, WIDTH), bf16),
        jax.ShapeDtypeStruct((SEQS, PROPS, BC), bf16),
        jax.ShapeDtypeStruct((SEQS, PROPS, HEADS), f32),
        jax.ShapeDtypeStruct((7, SEQS, WIDTH), bf16),
        jax.ShapeDtypeStruct((SEQS, 7, 2, BC), bf16),
    )
    def in_hbm(v):
        return pltpu.with_memory_space_constraint(v, pltpu.HBM)

    results = pl.pallas_call(
        kernel,
        out_shape=outs,
        in_specs=[anywhere] * 21,
        out_specs=[vmem] * 7,
        scratch_shapes=[
            V((64, PROPS, 64), bf16), V((D,), bf16), V((2, 64, WIDTH), bf16),
            V((64, 2, BC), bf16), V((48,), f32), V((48,), f32), V((SEQS, PROPS, HEADS), f32),
            V((4, WIDTH), bf16), V((4, 2, BC), bf16), V((48,), f32), V((2 * WIDTH,), bf16),
            V((64, WIDTH), bf16), V((SEQS, HEADS, HEAD_DIM, STATE), f32),
            V((SEQS, PROPS, WIDTH), bf16), V((SEQS, PROPS, BC), bf16),
            V((SEQS, PROPS, HEADS), f32), V((7, SEQS, WIDTH), bf16), V((SEQS, 7, 2, BC), bf16),
            V((128, 512), bf16), V((8, 64, 128), bf16), V((12, 64, 256), bf16), V((16, 256), bf16), V((8, 16, 256), bf16),
            V((256, 768), bf16), V((4, 8, 64, 128), bf16), V((4, PEERS, ROWS, 128), bf16),
            V((4, PEERS, ROWS, 128), bf16), V((PEERS, ROWS, 128), bf16), V((4, ROWS, 128), bf16),
            V((NX, 64, WIDTH), bf16), V((SEQS, GROUPS, GW, STATE), bf16),
            V((2, 8, ROWS, 512), bf16), V((8, ROWS, 640), bf16), V((NX, 32, 128), bf16),
            pltpu.SMEM((SEQS,), i32), DMA((21,)), DMA((19,)), DMA((19,)),
            pltpu.SemaphoreType.REGULAR((3, 2)),
        ],
        compiler_params=pltpu.CompilerParams(
            collective_id=0, has_side_effects=True, vmem_limit_bytes=40 * 1024 * 1024
        ),
    )(*(in_hbm(v) for v in (
        tokens, input_norm_gain, head_input_weight, output_gate_weight, state_maps_weight,
        step_size_weight.T, step_size_bias, head_decay_speed, proposal_decay_total,
        head_input_kernel, state_maps_kernel, head_direct_gain, grouped_norm_gain,
        output_weight.T, prior_state_value, previous_head_input, previous_input_maps,
        previous_log_decays, jnp.transpose(prior_heads_window, (1, 0, 2)), prior_maps_window,
        accepted,
    )))
    finals = (jax.ShapeDtypeStruct((64, PROPS, 64), bf16), *outs[1:])
    mixed, state, chi, cim, cld, chw, cmw = pl.pallas_call(
        finish,
        out_shape=finals,
        in_specs=[vmem] * 7,
        out_specs=[anywhere] * 7,
        scratch_shapes=[V((64, PROPS, 64), bf16), DMA((7,))],
        compiler_params=pltpu.CompilerParams(vmem_limit_bytes=8 * 1024 * 1024),
    )(*results)
    return mixed, state, chi, cim, cld, jnp.transpose(chw, (1, 0, 2)), cmw


def solution(mesh):
    seq = ("dp", "kv")
    return jax.shard_map(
        local,
        mesh=mesh,
        in_specs=(
            P("dp", None, "kv"), P(), P("kv", "tp"), P("kv", "tp"), P("kv", None, "tp"), P(), P(),
            P(), P(seq, None, "tp"), P(), P(), P(), P(), P("tp", "kv"), P(seq, "tp", None, None),
            P(seq, None, "tp"), P(seq, None, "tp"), P(seq, None, "tp"), P(seq, None, "tp"),
            P(seq, None, None, "tp"), P(seq),
        ),
        out_specs=(
            P("dp", None, "kv"), P(seq, "tp", None, None), P(seq, None, "tp"), P(seq, None, "tp"),
            P(seq, None, "tp"), P(seq, None, "tp"), P(seq, None, None, "tp"),
        ),
        check_vma=False,
    )
```

```python
import functools

import jax
import jax.numpy as jnp
from jax import lax
from jax.experimental import pallas as pl
from jax.experimental.pallas import tpu as pltpu
from jax.sharding import PartitionSpec as P

MESH = pl.DeviceIdType.MESH
HI = lax.Precision.HIGHEST
f32, bf16, i32 = jnp.float32, jnp.bfloat16, jnp.int32

NX, NY, NZ, NT = 4, 4, 8, 2
PEERS = NX * NZ
D, STATE, HEAD_DIM = 2048, 128, 64
SEQS, PROPS, ROWS = 2, 4, 8
HEADS, GROUPS, PER = 24, 4, 6
WIDTH, GW = 1536, 384
BC = 512
eps = 1e-06


def iota(shape, dim):
    return lax.broadcasted_iota(i32, shape, dim)


def mm(a, b, ca=1, cb=0, precision=None):
    return lax.dot_general(
        a, b, (((ca,), (cb,)), ((), ())), precision=precision, preferred_element_type=f32
    )


def heads_selection(acc):
    shape = (48, 24)
    i, j = iota(shape, 0), iota(shape, 1)
    out = i >= 32
    b = jnp.where(out, i & 1, (i >> 2) & 1)
    pos = jnp.where(out, (i - 32) >> 1, (i & 3) + (i >> 3))
    acc_b = jnp.where(b == 0, acc[0], acc[1])
    old = (j < 14) & ((j & 1) == b) & ((j >> 1) == acc_b + pos)
    raw = (j >= 16) & (((j - 16) >> 2) == b) & (((j - 16) & 3) == pos - 3)
    pick = jnp.where(pos < 3, jnp.where(old, 1.0, 0.0), jnp.where(raw, 1.0, 0.0))
    return pick.astype(bf16)


def maps_selection(acc):
    shape = (96, 48)
    i, j = iota(shape, 0), iota(shape, 1)
    out = i >= 64
    o = i - 64
    ob = jnp.where(o >= 14, 1, 0)
    orem = o - 14 * ob
    b = jnp.where(out, ob, (i >> 2) & 1)
    pos = jnp.where(out, orem >> 1, (i & 3) + (i >> 4))
    kind = jnp.where(out, orem & 1, (i >> 3) & 1)
    acc_b = jnp.where(b == 0, acc[0], acc[1])
    jb = jnp.where(j >= 14, 1, 0)
    jrem = j - 14 * jb
    old = (j < 28) & (jb == b) & ((jrem & 1) == kind) & ((jrem >> 1) == acc_b + pos)
    jr = j - 32
    raw = (j >= 32) & ((jr >> 3) == kind) & (((jr >> 2) & 1) == b) & ((jr & 3) == pos - 3)
    pick = jnp.where(pos < 3, jnp.where(old, 1.0, 0.0), jnp.where(raw, 1.0, 0.0))
    return pick.astype(bf16)


def kernel(
    tok_h, gain_h, wx_h, wg_h, smw_h, sw_h, ssb_h, hds_h, pdt_h, hik_h, smk_h, hdg_h, gng_h, wo_h,
    psv_h, phi_h, pim_h, pld_h, phw_h, pmw_h, acc_h,
    fr, state, chi, cim, cld, chw, cmw,
    tok, gain, wxg, smw, ssb, hds, pdt, hik, smk, hdg, gng, wo, psv, phi, pim, pld, phw, pmw,
    sw, bcs, tt, squares_out, squares_in, lhs, wr, send, got, steps_out, steps_in, wor, sb, nrm, last, fs,
    acc_s, lsem, ssem, rsem, level_sem,
):
    y, kv, t = lax.axis_index("dp"), lax.axis_index("kv"), lax.axis_index("tp")
    z, x = kv // NX, kv % NX
    pair, half = z // 2, z % 2

    def at(zz, xx, tt_):
        return dict(device_id=(y, zz * NX + xx, tt_), device_id_type=MESH)

    def over(d):
        return dict(device_id=(lax.rem(y + d, NY), kv, t), device_id_type=MESH)

    def served(e):
        return lax.rem(z + (2 * half - 1) * e + NZ, NZ)

    def server(e):
        return lax.rem(z + (1 - 2 * ((half + e) % 2)) * e + NZ, NZ)

    loads = {}
    plan = (
        (tok_h, tok), (gain_h, gain), (smw_h, smw), (wx_h, wxg.at[0]), (wg_h, wxg.at[1]),
        (sw_h.at[:, pl.ds(pl.multiple_of(pair * 512, 512), 512)], sw.at[pl.ds(0, 48)]),
        (ssb_h, ssb), (hds_h, hds), (pdt_h, pdt),
        (hik_h.at[:, pl.ds(pl.multiple_of(t * WIDTH, 128), WIDTH)], hik),
        (smk_h.at[:, :, pl.ds(pl.multiple_of(t * BC, 128), BC)], smk),
        (hdg_h, hdg), (gng_h, gng), (wo_h, wo), (phi_h, phi), (pim_h, pim), (pld_h, pld),
        (phw_h, phw), (pmw_h, pmw), (psv_h, psv), (acc_h, acc_s),
    )
    for n, (src, dst) in enumerate(plan):
        loads[n] = pltpu.make_async_copy(src, dst, lsem.at[n])
    for n in (0, 1, 2):
        loads[n].start()

    barrier = pltpu.get_barrier_semaphore()

    row_peers = [(0, 2), (0, 1), (0, 3)]
    up_peers = [(1, 2), (1, 1), (1, 3), (1, 0)]
    down_peers = [(NZ - 1, dx) for _, dx in up_peers]

    def near(dz, dx):
        return lax.rem(x + dx, NX), at(lax.rem(z + dz, NZ), lax.rem(x + dx, NX), t)

    for dz, dx in row_peers + up_peers + down_peers:
        pl.semaphore_signal(barrier, inc=1, **near(dz, dx)[1])
    for d in range(NX):
        pl.semaphore_signal(barrier, inc=1, **at(z, lax.rem(x + d, NX), 1 - t))
    for d in range(1, NY):
        pl.semaphore_signal(barrier, inc=1, **over(d))
    for e in (2, 3):
        pl.semaphore_signal(barrier, inc=1, **at(served(e), x, t))
    for n in range(3, len(plan)):
        loads[n].start()

    for n in (0, 1, 2):
        loads[n].wait()
    tok32 = tok[...].astype(f32).reshape(256, 64)
    gains = gain[...].astype(f32).reshape(16, 128)
    gain_row = jnp.sum(
        jnp.where(iota((16, 128), 0) == kv // 2, gains, 0.0), axis=0, keepdims=True
    )
    gain_row = jnp.where(kv % 2 == 0, gain_row[:, :64], gain_row[:, 64:])
    tt[x, 0:64] = (tok32 * gain_row).astype(bf16).T
    sumsq = jnp.sum(jnp.square(tok32.T), axis=0, keepdims=True)
    high = sumsq.astype(bf16).astype(f32)
    line = iota((16, 256), 0)
    squares_out[...] = jnp.where(
        line == 0, high, jnp.where(line == 1, sumsq - high, 0.0)
    ).astype(bf16)
    for n in range(2):
        part = smw[:, n, :]
        for g in range(GROUPS):
            bcs[n * GROUPS + g] = part[:, g * STATE : g * STATE + STATE]
    sw[48:128] = jnp.zeros((80, 512), bf16)

    def columns(c, h, xx):
        if c == 0:
            return bcs.at[h * NX + xx]
        return wxg.at[
            h if c == 1 else 1 - h, :, pl.ds(pl.multiple_of(xx * GW + (c - 1) * 128, 128), 128)
        ]

    loads[3].wait()
    loads[4].wait()
    for c in range(4):
        wr[c, x] = columns(c, half, x)[...]

    pl.semaphore_wait(barrier, 11 + NX + NY - 1 + 2)

    def pass_on(level):
        for n, dz in enumerate((1, NZ - 1)):
            pl.semaphore_signal(level_sem.at[level, n], inc=1, **near(dz, 0)[1])

    def hear(level):
        for n in range(2):
            pl.semaphore_wait(level_sem.at[level, n], 1)

    pass_on(0)

    @pl.when(t == 1)
    def _():
        for peers, base in ((up_peers, 8), (down_peers, 4), (row_peers, 0)):
            for dz, dx in peers:
                pltpu.make_async_remote_copy(
                    tt.at[x], tt.at[base + x], ssem.at[4], rsem.at[4], **near(dz, dx)[1]
                ).start()

    def send_weights(c):
        for peers, h, base in (
            (down_peers if c < 2 else up_peers, 1 - half, 4),
            (row_peers, half, 0),
        ):
            for dz, dx in peers:
                xx, to = near(dz, dx)
                pltpu.make_async_remote_copy(
                    columns(c, h, xx), wr.at[c, base + x], ssem.at[c], rsem.at[c], **to
                ).start()

    loads[13].wait()
    wor[0] = wo[...]
    mine = pl.ds(pl.multiple_of(y * 16, 16), 16)

    def send_output_weights():
        for e in (3, 2, 1):
            pltpu.make_async_remote_copy(
                wo.at[mine], wor.at[e, mine], ssem.at[10], rsem.at[10], **at(server(e), x, t)
            ).start()

    @pl.when(t == 0)
    def _():
        send_output_weights()

    steps_mine = (half == 0) & (x == pair)

    @pl.when(jnp.logical_not(steps_mine))
    def _():
        pltpu.make_async_remote_copy(
            squares_out, squares_in.at[half * NX + x], ssem.at[15], rsem.at[15],
            **at(2 * pair, pair, t),
        ).start()

    def arrived(buffer, count, sem):
        block = buffer.at[pl.ds(0, count)]
        pltpu.make_async_copy(block, block, sem).wait()

    loads[20].wait()
    acc = (acc_s[0], acc_s[1])
    row = iota((ROWS, 1), 0)
    acc_row = jnp.where(row < PROPS, acc[0], acc[1])
    keep = jnp.where((row & 3) < acc_row, 1.0, 0.0)
    r8, c8 = iota((ROWS, ROWS), 0), iota((ROWS, ROWS), 1)
    same = (r8 >> 2) == (c8 >> 2)
    expand = jnp.where(iota((HEADS, WIDTH), 1) // HEAD_DIM == iota((HEADS, WIDTH), 0), 1.0, 0.0)
    for n in (14, 15, 16):
        loads[n].wait()
    kept = pld[...].reshape(ROWS, HEADS) * keep
    later = mm(jnp.where(same & (c8 > r8), 1.0, 0.0), kept, precision=HI)
    coef = mm(keep * jnp.exp(later), expand, precision=HI)
    scaled = coef * phi[...].astype(f32).reshape(ROWS, WIDTH)
    s_hi = scaled.astype(bf16)
    s_lo = (scaled - s_hi.astype(f32)).astype(bf16)
    updates = jnp.concatenate([s_hi.astype(f32), s_lo.astype(f32)], axis=0).astype(bf16)
    keys = pim[...].astype(f32).reshape(ROWS, BC)
    loads[19].wait()
    for b in range(SEQS):
        of_b = (row >> 2) == b
        logs = mm(jnp.where(of_b, kept, 0.0), jnp.ones((ROWS, STATE), f32), 0, 0, precision=HI)
        factor = jnp.exp(logs)
        keys_b = jnp.where(of_b, keys, 0.0)
        keys_b = jnp.concatenate([keys_b, keys_b], axis=0).astype(bf16)
        for g in range(GROUPS):
            upd = mm(
                updates[:, g * GW : g * GW + GW], keys_b[:, g * STATE : g * STATE + STATE], 0, 0
            )
            new = (
                psv[b, g * PER : g * PER + PER] * factor[g * PER : g * PER + PER][:, None, :]
                + upd.reshape(PER, HEAD_DIM, STATE)
            )
            state[b, g * PER : g * PER + PER] = new
            sb[b, g] = new.reshape(GW, STATE).astype(bf16)

    for c in range(4):
        send_weights(c)
    @pl.when(t == 1)
    def _():
        send_output_weights()

    quarters = wor.at[:, pl.ds(0, 16)]
    three_quarters = wor.at[:, pl.ds(0, 48)]

    from_me = (x * 2 + half) * 4 + pair

    def spread(src, dst, index, n):
        def one(d, _):
            other = lax.rem(kv + d, PEERS)
            pltpu.make_async_remote_copy(
                src.at[other],
                dst.at[index],
                ssem.at[n],
                rsem.at[n],
                device_id=(y, other, t),
                device_id_type=MESH,
            ).start()
            return 0

        lax.fori_loop(1, PEERS, one, 0)
        dst[index] = src[kv]

    for level in range(3):
        hear(level)
        if level < 2:
            pass_on(level + 1)


    @pl.when(t == 1)
    def _():
        arrived(tt, 11, rsem.at[4])
        blocks = [tt.at[pl.ds(4, 8)]]
        blocks += [tt.at[lax.rem(x + d, NX)] for d in range(1, NX)]
        for block in blocks:
            pltpu.make_async_remote_copy(
                block, block, ssem.at[14], rsem.at[14], **at(z, x, 1 - t)
            ).start()

    @pl.when(t == 0)
    def _():
        arrived(tt, 11, rsem.at[14])

    lhs[...] = tt[...].reshape(768, 256).T
    loads[5].wait()

    @pl.when(steps_mine)
    def _():
        steps = mm(lhs[:, 0:512], sw[...], 1, 1)
        arrived(squares_in, 7, rsem.at[15])
        squares_in[half * NX + x] = squares_out[...]
        squares = jnp.sum(squares_in[...].astype(f32), axis=0)
        pick = jnp.where(
            (iota((16, 128), 1) == 64) & (iota((16, 128), 0) < 2), 1.0, 0.0
        )
        squares = mm(squares, pick, 0, 0, precision=HI)
        total = squares[:, 64:65]
        high = total.astype(bf16).astype(f32)
        lane = iota((256, 128), 1)
        steps = jnp.where(lane == 64, high, jnp.where(lane == 65, total - high, steps))
        steps_out[...] = steps.reshape(PEERS, ROWS, 128).astype(bf16)
        spread(steps_out, steps_in, pair, 9)

    for c in range(4):
        arrived(wr.at[c], 7, rsem.at[c])
        if c < 2:
            part = mm(lhs[:, 0:512], wr[c].reshape(512, 128))
        else:
            part = mm(lhs[:, 0:256], wr[c, 0:4].reshape(256, 128))
            part = part + mm(lhs[:, 512:768], wr[c, 4:8].reshape(256, 128))
        send[c] = part.reshape(PEERS, ROWS, 128).astype(bf16)
        spread(send.at[c], got.at[c], from_me, 5 + c)
    arrived(quarters, 3, rsem.at[10])
    for d in (2, 1, 3):
        for e in (2, 1, 3):
            block = wor.at[d, mine]
            pltpu.make_async_remote_copy(
                block, block, ssem.at[13], rsem.at[13], **over(e)
            ).start()

    pick_x, pick_bc = heads_selection(acc), maps_selection(acc)
    for n in (6, 7, 8, 9, 10, 11, 12, 17, 18):
        loads[n].wait()
    old_x = phw[...].astype(f32).reshape(14, WIDTH)
    old_x = jnp.concatenate([old_x, jnp.zeros((2, WIDTH), f32)], axis=0)
    old_bc = pmw[...].astype(f32).reshape(28, BC)
    old_bc = jnp.concatenate([old_bc, jnp.zeros((4, BC), f32)], axis=0)
    taps_x = hik[...].astype(f32)
    taps_bc = smk[...].astype(f32).reshape(8, BC)

    def own_heads(ref):
        v = ref[...].reshape(1, 2 * HEADS)
        return jnp.where(t == 0, v[:, :HEADS], v[:, HEADS:])

    speed, direct, bias = own_heads(hds), own_heads(hdg), own_heads(ssb)
    gngv = gng[...].astype(f32).reshape(1, 2 * WIDTH)
    out_gain = jnp.where(t == 0, gngv[:, :WIDTH], gngv[:, WIDTH:])

    def total(c):
        return jnp.sum(got[c].astype(f32).reshape(NX, 2, 4, ROWS, 128), axis=2)

    arrived(got.at[0], PEERS - 1, rsem.at[5])

    @pl.when(steps_mine)
    def _():
        arrived(steps_in, 3, rsem.at[9])

    @pl.when(jnp.logical_not(steps_mine))
    def _():
        arrived(steps_in, 4, rsem.at[9])

    tail = jnp.sum(steps_in[...].astype(f32), axis=0)
    lane8 = iota((ROWS, 128), 1)
    squares = jnp.sum(jnp.where((lane8 == 64) | (lane8 == 65), tail, 0.0), axis=1, keepdims=True)
    inv = lax.rsqrt(squares / D + eps)
    sum0 = total(0)
    raw_b = jnp.concatenate([sum0[g, 0] for g in range(GROUPS)], axis=1) * inv
    raw_c = jnp.concatenate([sum0[g, 1] for g in range(GROUPS)], axis=1) * inv
    win_bc = mm(pick_bc, jnp.concatenate([old_bc, raw_b, raw_c], axis=0).astype(bf16))
    cmw[...] = win_bc[64:92].reshape(SEQS, 7, 2, BC).astype(bf16)
    b_conv = taps_bc[0:1] * win_bc[0:8]
    c_conv = taps_bc[1:2] * win_bc[8:16]
    for k in range(1, 4):
        b_conv = b_conv + taps_bc[2 * k : 2 * k + 1] * win_bc[16 * k : 16 * k + 8]
        c_conv = c_conv + taps_bc[2 * k + 1 : 2 * k + 2] * win_bc[16 * k + 8 : 16 * k + 16]
    b_conv = b_conv * lax.logistic(b_conv)
    c_conv = c_conv * lax.logistic(c_conv)
    step_pre = tail * inv
    step_pre = jnp.where(t == 0, step_pre[:, :HEADS], step_pre[:, HEADS : 2 * HEADS]) + bias
    step = jnp.maximum(step_pre, 0.0) + jnp.log1p(jnp.exp(-jnp.abs(step_pre)))
    decays = pdt[...].reshape(ROWS, HEADS) - speed * step
    cum = mm(jnp.where(same & (c8 <= r8), 1.0, 0.0), decays, precision=HI)
    wide = mm(
        jnp.concatenate([cum, step, jnp.broadcast_to(direct, (ROWS, HEADS))], axis=0),
        expand,
        precision=HI,
    )
    cim[...] = b_conv.reshape(SEQS, PROPS, BC).astype(bf16)
    cld[...] = decays.reshape(SEQS, PROPS, HEADS)
    from_state, pairs = [], []
    for g in range(GROUPS):
        lanes = slice(g * STATE, g * STATE + STATE)
        c_g = c_conv[:, lanes]
        y0 = mm(c_g.astype(bf16), sb[0, g], 1, 1)
        y1 = mm(c_g.astype(bf16), sb[1, g], 1, 1)
        from_state.append(jnp.where(row < PROPS, y0, y1))
        pairs.append(mm(c_g, b_conv[:, lanes], 1, 1, precision=HI))
    from_state = jnp.exp(wide[0:8]) * jnp.concatenate(from_state, axis=1)
    scores = []
    for d in range(PROPS):
        score = [
            jnp.broadcast_to(
                jnp.sum(jnp.where(c8 == r8 - d, p, 0.0), axis=1, keepdims=True), (ROWS, 128)
            )
            for p in pairs
        ]
        scores.append(jnp.concatenate(score, axis=1))

    def third(v, c):
        starts = [g * GW + (c - 1) * 128 for g in range(GROUPS)]
        return jnp.concatenate([v[:, n : n + 128] for n in starts], axis=1)

    def whole(thirds):
        return jnp.concatenate(
            [v[:, g * 128 : g * 128 + 128] for g in range(GROUPS) for v in thirds], axis=1
        )

    slot = half * NX + x

    def to_pair(block, n):
        for dx, dp in ((2, 1), (2, 0), (1, 1), (3, 1), (1, 0), (3, 0), (0, 1)):
            pltpu.make_async_remote_copy(
                block, block, ssem.at[n], rsem.at[n],
                **at(2 * pair + lax.rem(half + dp, 2), lax.rem(x + dx, NX), t),
            ).start()

    windows, inputs = [], []
    energy = [0.0] * GROUPS
    for c in range(1, 4):
        wide_c, taps_c, old_c = third(wide, c), third(taps_x, c), third(old_x, c)
        cum_w, step_w, direct_w = wide_c[0:8], wide_c[8:16], wide_c[16:24]
        decay_w = [None]
        for d in range(1, PROPS):
            gap = jnp.where((row & 3) >= d, cum_w - pltpu.roll(cum_w, d, 0), 0.0)
            decay_w.append(jnp.exp(gap) * scores[d])
        arrived(got.at[c], PEERS - 1, rsem.at[5 + c])
        sum_c = total(c)
        heads_at = 0 if c == 1 else 1
        raw_x = jnp.concatenate([sum_c[g, heads_at] for g in range(GROUPS)], axis=1) * inv
        gate = jnp.concatenate([sum_c[g, 1 - heads_at] for g in range(GROUPS)], axis=1) * inv
        win_x = mm(pick_x, jnp.concatenate([old_c, raw_x], axis=0).astype(bf16))
        windows.append(win_x[32:46])
        x_conv = taps_c[0:1] * win_x[0:8]
        for k in range(1, 4):
            x_conv = x_conv + taps_c[k : k + 1] * win_x[8 * k : 8 * k + 8]
        x_conv = x_conv * lax.logistic(x_conv)
        weighted = step_w * x_conv
        inputs.append(weighted)
        heads = third(from_state, c) + direct_w * x_conv + scores[0] * weighted
        for d in range(1, PROPS):
            term = decay_w[d] * pltpu.roll(weighted, d, 0)
            heads = heads + jnp.where((row & 3) >= d, term, 0.0)
        gated = heads * (gate * lax.logistic(gate))
        for g in range(GROUPS):
            part_g = gated[:, g * 128 : g * 128 + 128]
            energy[g] = energy[g] + jnp.sum(part_g * part_g, axis=1, keepdims=True)
        gated = gated * third(out_gain, c)
        if c < 3:
            nrm[c - 1, slot] = gated.astype(bf16)
            to_pair(nrm.at[c - 1, slot], 15 + c)
            continue
        factors = jnp.zeros((ROWS, 128), f32)
        for g in range(GROUPS):
            factor = lax.rsqrt(energy[g] / GW + eps)
            high = factor.astype(bf16).astype(f32)
            factors = jnp.where(lane8 == g, high, factors)
            factors = jnp.where(lane8 == GROUPS + g, factor - high, factors)
        last[slot] = jnp.concatenate([gated, factors], axis=1).astype(bf16)
        to_pair(last.at[slot], 18)
    chw[...] = whole(windows).reshape(7, SEQS, WIDTH).astype(bf16)
    chi[...] = whole(inputs).reshape(SEQS, PROPS, WIDTH).astype(bf16)

    arrived(three_quarters, 3, rsem.at[13])
    columns_of = wor[...].reshape(256, WIDTH)
    products = [jnp.zeros((64, 256), f32)] * GROUPS
    for c in range(1, 4):
        if c < 3:
            arrived(nrm.at[c - 1], 7, rsem.at[15 + c])
            rows64 = nrm[c - 1].astype(f32).reshape(64, 512).astype(bf16)
        else:
            arrived(last, 7, rsem.at[18])
            rows64 = last[:, :, 0:512].astype(f32).reshape(64, 512).astype(bf16)
        for g in range(GROUPS):
            start = g * GW + (c - 1) * 128
            products[g] = products[g] + mm(
                rows64[:, g * 128 : g * 128 + 128], columns_of[:, start : start + 128], 1, 1
            )
    factors = last[:, :, 512:640].astype(f32).reshape(64, 128)
    factors = factors + pltpu.roll(factors, 128 - GROUPS, 1)
    partial = factors[:, 0:1] * products[0]
    for g in range(1, GROUPS):
        partial = partial + factors[:, g : g + 1] * products[g]
    first_lanes = iota((32, 128), 1) < 64
    for d in (3, 2, 1, 0):
        both = partial[:, 128 * (d // 2) : 128 * (d // 2) + 128]
        turned = pltpu.roll(both, 64, 1)
        low, high = (both, turned) if d % 2 == 0 else (turned, both)
        fs[d] = jnp.where(first_lanes, low[:32], high[32:]).astype(bf16)
        zz, there = served(d), fr.at[pair * NT + t]
        if d == 0:
            fr[pair * NT + t] = fs[0]
        else:
            pltpu.make_async_remote_copy(
                fs.at[d], there, ssem.at[12], rsem.at[12], **at(zz, x, t)
            ).start()
        pltpu.make_async_remote_copy(
            fs.at[d], there, ssem.at[12], rsem.at[12], **at(zz, x, 1 - t)
        ).start()
    arrived(fr, 7, rsem.at[12])

    @pl.when(t == 1)
    def _():
        arrived(tt, 11, ssem.at[4])

    @pl.when(t == 1)
    def _():
        arrived(tt, 11, ssem.at[14])

    @pl.when(jnp.logical_not(steps_mine))
    def _():
        pltpu.make_async_copy(squares_out, squares_out, ssem.at[15]).wait()

    for c in range(4):
        arrived(wr.at[c], 7, ssem.at[c])
        arrived(send.at[c], PEERS - 1, ssem.at[5 + c])

    @pl.when(steps_mine)
    def _():
        arrived(steps_out, PEERS - 1, ssem.at[9])

    arrived(quarters, 3, ssem.at[10])
    arrived(three_quarters, 3, ssem.at[13])
    for c in range(2):
        arrived(nrm.at[c], 7, ssem.at[16 + c])
    arrived(last, 7, ssem.at[18])
    arrived(fr, 7, ssem.at[12])


def finish(fr, *refs):
    ins, outs, mixed, sems = refs[:6], refs[6:13], refs[13], refs[14]
    copies = [
        pltpu.make_async_copy(a, b, sems.at[n]) for n, (a, b) in enumerate(zip(ins, outs[1:]))
    ]
    for copy in copies:
        copy.start()
    done = fr[...].astype(f32).reshape(4, NT, 32, 128)
    done = done[:, 0] + done[:, 1]
    done = jnp.stack([done[:, :, :64], done[:, :, 64:]], axis=1)
    mixed[...] = done.reshape(64, PROPS, 64).astype(bf16)
    copies.append(pltpu.make_async_copy(mixed, outs[0], sems.at[6]))
    copies[-1].start()
    for copy in copies:
        copy.wait()


def local(
    tokens, input_norm_gain, head_input_weight, output_gate_weight, state_maps_weight,
    step_size_weight, step_size_bias, head_decay_speed, proposal_decay_total, head_input_kernel,
    state_maps_kernel, head_direct_gain, grouped_norm_gain, output_weight, prior_state_value,
    previous_head_input, previous_input_maps, previous_log_decays, prior_heads_window,
    prior_maps_window, accepted,
):
    anywhere = pl.BlockSpec(memory_space=pl.ANY)
    vmem = pl.BlockSpec(memory_space=pltpu.VMEM)
    V, DMA = pltpu.VMEM, pltpu.SemaphoreType.DMA
    outs = (
        jax.ShapeDtypeStruct((NX * NT, 32, 128), bf16),
        jax.ShapeDtypeStruct((SEQS, HEADS, HEAD_DIM, STATE), f32),
        jax.ShapeDtypeStruct((SEQS, PROPS, WIDTH), bf16),
        jax.ShapeDtypeStruct((SEQS, PROPS, BC), bf16),
        jax.ShapeDtypeStruct((SEQS, PROPS, HEADS), f32),
        jax.ShapeDtypeStruct((7, SEQS, WIDTH), bf16),
        jax.ShapeDtypeStruct((SEQS, 7, 2, BC), bf16),
    )
    def in_hbm(v):
        return pltpu.with_memory_space_constraint(v, pltpu.HBM)

    results = pl.pallas_call(
        kernel,
        out_shape=outs,
        in_specs=[anywhere] * 21,
        out_specs=[vmem] * 7,
        scratch_shapes=[
            V((64, PROPS, 64), bf16), V((D,), bf16), V((2, 64, WIDTH), bf16),
            V((64, 2, BC), bf16), V((48,), f32), V((48,), f32), V((SEQS, PROPS, HEADS), f32),
            V((4, WIDTH), bf16), V((4, 2, BC), bf16), V((48,), f32), V((2 * WIDTH,), bf16),
            V((64, WIDTH), bf16), V((SEQS, HEADS, HEAD_DIM, STATE), f32),
            V((SEQS, PROPS, WIDTH), bf16), V((SEQS, PROPS, BC), bf16),
            V((SEQS, PROPS, HEADS), f32), V((7, SEQS, WIDTH), bf16), V((SEQS, 7, 2, BC), bf16),
            V((128, 512), bf16), V((8, 64, 128), bf16), V((12, 64, 256), bf16), V((16, 256), bf16), V((8, 16, 256), bf16),
            V((256, 768), bf16), V((4, 8, 64, 128), bf16), V((4, PEERS, ROWS, 128), bf16),
            V((4, PEERS, ROWS, 128), bf16), V((PEERS, ROWS, 128), bf16), V((4, ROWS, 128), bf16),
            V((NX, 64, WIDTH), bf16), V((SEQS, GROUPS, GW, STATE), bf16),
            V((2, 8, ROWS, 512), bf16), V((8, ROWS, 640), bf16), V((NX, 32, 128), bf16),
            pltpu.SMEM((SEQS,), i32), DMA((21,)), DMA((19,)), DMA((19,)),
            pltpu.SemaphoreType.REGULAR((3, 2)),
        ],
        compiler_params=pltpu.CompilerParams(
            collective_id=0, has_side_effects=True, vmem_limit_bytes=40 * 1024 * 1024
        ),
    )(*(in_hbm(v) for v in (
        tokens, input_norm_gain, head_input_weight, output_gate_weight, state_maps_weight,
        step_size_weight.T, step_size_bias, head_decay_speed, proposal_decay_total,
        head_input_kernel, state_maps_kernel, head_direct_gain, grouped_norm_gain,
        output_weight.T, prior_state_value, previous_head_input, previous_input_maps,
        previous_log_decays, jnp.transpose(prior_heads_window, (1, 0, 2)), prior_maps_window,
        accepted,
    )))
    finals = (jax.ShapeDtypeStruct((64, PROPS, 64), bf16), *outs[1:])
    mixed, state, chi, cim, cld, chw, cmw = pl.pallas_call(
        finish,
        out_shape=finals,
        in_specs=[vmem] * 7,
        out_specs=[anywhere] * 7,
        scratch_shapes=[V((64, PROPS, 64), bf16), DMA((7,))],
        compiler_params=pltpu.CompilerParams(vmem_limit_bytes=8 * 1024 * 1024),
    )(*results)
    return mixed, state, chi, cim, cld, jnp.transpose(chw, (1, 0, 2)), cmw


def solution(mesh):
    seq = ("dp", "kv")
    return jax.shard_map(
        local,
        mesh=mesh,
        in_specs=(
            P("dp", None, "kv"), P(), P("kv", "tp"), P("kv", "tp"), P("kv", None, "tp"), P(), P(),
            P(), P(seq, None, "tp"), P(), P(), P(), P(), P("tp", "kv"), P(seq, "tp", None, None),
            P(seq, None, "tp"), P(seq, None, "tp"), P(seq, None, "tp"), P(seq, None, "tp"),
            P(seq, None, None, "tp"), P(seq),
        ),
        out_specs=(
            P("dp", None, "kv"), P(seq, "tp", None, None), P(seq, None, "tp"), P(seq, None, "tp"),
            P(seq, None, "tp"), P(seq, None, "tp"), P(seq, None, None, "tp"),
        ),
        check_vma=False,
    )
```

```python
import functools

import jax
import jax.numpy as jnp
from jax import lax
from jax.experimental import pallas as pl
from jax.experimental.pallas import tpu as pltpu
from jax.sharding import PartitionSpec as P

MESH = pl.DeviceIdType.MESH
HI = lax.Precision.HIGHEST
f32, bf16, i32 = jnp.float32, jnp.bfloat16, jnp.int32

NX, NY, NZ, NT = 4, 4, 8, 2
PEERS = NX * NZ
D, STATE, HEAD_DIM = 2048, 128, 64
SEQS, PROPS, ROWS = 2, 4, 8
HEADS, GROUPS, PER = 24, 4, 6
WIDTH, GW = 1536, 384
BC = 512
eps = 1e-06


def iota(shape, dim):
    return lax.broadcasted_iota(i32, shape, dim)


def mm(a, b, ca=1, cb=0, precision=None):
    return lax.dot_general(
        a, b, (((ca,), (cb,)), ((), ())), precision=precision, preferred_element_type=f32
    )


def heads_selection(acc):
    shape = (48, 24)
    i, j = iota(shape, 0), iota(shape, 1)
    out = i >= 32
    b = jnp.where(out, i & 1, (i >> 2) & 1)
    pos = jnp.where(out, (i - 32) >> 1, (i & 3) + (i >> 3))
    acc_b = jnp.where(b == 0, acc[0], acc[1])
    old = (j < 14) & ((j & 1) == b) & ((j >> 1) == acc_b + pos)
    raw = (j >= 16) & (((j - 16) >> 2) == b) & (((j - 16) & 3) == pos - 3)
    pick = jnp.where(pos < 3, jnp.where(old, 1.0, 0.0), jnp.where(raw, 1.0, 0.0))
    return pick.astype(bf16)


def maps_selection(acc):
    shape = (96, 48)
    i, j = iota(shape, 0), iota(shape, 1)
    out = i >= 64
    o = i - 64
    ob = jnp.where(o >= 14, 1, 0)
    orem = o - 14 * ob
    b = jnp.where(out, ob, (i >> 2) & 1)
    pos = jnp.where(out, orem >> 1, (i & 3) + (i >> 4))
    kind = jnp.where(out, orem & 1, (i >> 3) & 1)
    acc_b = jnp.where(b == 0, acc[0], acc[1])
    jb = jnp.where(j >= 14, 1, 0)
    jrem = j - 14 * jb
    old = (j < 28) & (jb == b) & ((jrem & 1) == kind) & ((jrem >> 1) == acc_b + pos)
    jr = j - 32
    raw = (j >= 32) & ((jr >> 3) == kind) & (((jr >> 2) & 1) == b) & ((jr & 3) == pos - 3)
    pick = jnp.where(pos < 3, jnp.where(old, 1.0, 0.0), jnp.where(raw, 1.0, 0.0))
    return pick.astype(bf16)


def kernel(
    tok_h, gain_h, wx_h, wg_h, smw_h, sw_h, ssb_h, hds_h, pdt_h, hik_h, smk_h, hdg_h, gng_h, wo_h,
    psv_h, phi_h, pim_h, pld_h, phw_h, pmw_h, acc_h,
    fr, state, chi, cim, cld, chw, cmw,
    tok, gain, wxg, smw, ssb, hds, pdt, hik, smk, hdg, gng, wo, psv, phi, pim, pld, phw, pmw,
    sw, bcs, tt, squares_out, squares_in, lhs, wr, send, got, steps_out, steps_in, wor, sb, nrm, last, fs,
    acc_s, lsem, ssem, rsem, level_sem,
):
    y, kv, t = lax.axis_index("dp"), lax.axis_index("kv"), lax.axis_index("tp")
    z, x = kv // NX, kv % NX
    pair, half = z // 2, z % 2

    def at(zz, xx, tt_):
        return dict(device_id=(y, zz * NX + xx, tt_), device_id_type=MESH)

    def over(d):
        return dict(device_id=(lax.rem(y + d, NY), kv, t), device_id_type=MESH)

    def served(e):
        return lax.rem(z + (2 * half - 1) * e + NZ, NZ)

    def server(e):
        return lax.rem(z + (1 - 2 * ((half + e) % 2)) * e + NZ, NZ)

    loads = {}
    plan = (
        (tok_h, tok), (gain_h, gain), (smw_h, smw), (wx_h, wxg.at[0]), (wg_h, wxg.at[1]),
        (sw_h.at[:, pl.ds(pl.multiple_of(pair * 512, 512), 512)], sw.at[pl.ds(0, 48)]),
        (ssb_h, ssb), (hds_h, hds), (pdt_h, pdt),
        (hik_h.at[:, pl.ds(pl.multiple_of(t * WIDTH, 128), WIDTH)], hik),
        (smk_h.at[:, :, pl.ds(pl.multiple_of(t * BC, 128), BC)], smk),
        (hdg_h, hdg), (gng_h, gng), (wo_h, wo), (phi_h, phi), (pim_h, pim), (pld_h, pld),
        (phw_h, phw), (pmw_h, pmw), (psv_h, psv), (acc_h, acc_s),
    )
    for n, (src, dst) in enumerate(plan):
        loads[n] = pltpu.make_async_copy(src, dst, lsem.at[n])
    for n in (0, 1, 2):
        loads[n].start()

    barrier = pltpu.get_barrier_semaphore()

    row_peers = [(0, 2), (0, 1), (0, 3)]
    up_peers = [(1, 2), (1, 1), (1, 3), (1, 0)]
    down_peers = [(NZ - 1, dx) for _, dx in up_peers]

    def near(dz, dx):
        return lax.rem(x + dx, NX), at(lax.rem(z + dz, NZ), lax.rem(x + dx, NX), t)

    for dz, dx in row_peers + up_peers + down_peers:
        pl.semaphore_signal(barrier, inc=1, **near(dz, dx)[1])
    for d in range(NX):
        pl.semaphore_signal(barrier, inc=1, **at(z, lax.rem(x + d, NX), 1 - t))
    for d in range(1, NY):
        pl.semaphore_signal(barrier, inc=1, **over(d))
    for e in (2, 3):
        pl.semaphore_signal(barrier, inc=1, **at(served(e), x, t))
    for n in range(3, len(plan)):
        loads[n].start()

    for n in (0, 1, 2):
        loads[n].wait()
    tok32 = tok[...].astype(f32).reshape(256, 64)
    gains = gain[...].astype(f32).reshape(16, 128)
    gain_row = jnp.sum(
        jnp.where(iota((16, 128), 0) == kv // 2, gains, 0.0), axis=0, keepdims=True
    )
    gain_row = jnp.where(kv % 2 == 0, gain_row[:, :64], gain_row[:, 64:])
    tt[x, 0:64] = (tok32 * gain_row).astype(bf16).T
    sumsq = jnp.sum(jnp.square(tok32.T), axis=0, keepdims=True)
    high = sumsq.astype(bf16).astype(f32)
    line = iota((16, 256), 0)
    squares_out[...] = jnp.where(
        line == 0, high, jnp.where(line == 1, sumsq - high, 0.0)
    ).astype(bf16)
    for n in range(2):
        part = smw[:, n, :]
        for g in range(GROUPS):
            bcs[n * GROUPS + g] = part[:, g * STATE : g * STATE + STATE]
    sw[48:128] = jnp.zeros((80, 512), bf16)

    def columns(c, h, xx):
        if c == 0:
            return bcs.at[h * NX + xx]
        return wxg.at[
            h if c == 1 else 1 - h, :, pl.ds(pl.multiple_of(xx * GW + (c - 1) * 128, 128), 128)
        ]

    loads[3].wait()
    loads[4].wait()
    for c in range(4):
        wr[c, x] = columns(c, half, x)[...]

    pl.semaphore_wait(barrier, 11 + NX + NY - 1 + 2)

    def pass_on(level):
        for n, dz in enumerate((1, NZ - 1)):
            pl.semaphore_signal(level_sem.at[level, n], inc=1, **near(dz, 0)[1])

    def hear(level):
        for n in range(2):
            pl.semaphore_wait(level_sem.at[level, n], 1)

    pass_on(0)

    @pl.when(t == 1)
    def _():
        turns = [p for two in zip(up_peers, down_peers) for p in zip(two, (8, 4))]
        for (dz, dx), base in turns + [(p, 0) for p in row_peers]:
            pltpu.make_async_remote_copy(
                tt.at[x], tt.at[base + x], ssem.at[4], rsem.at[4], **near(dz, dx)[1]
            ).start()

    def send_weights(c):
        for peers, h, base in (
            (down_peers if c < 2 else up_peers, 1 - half, 4),
            (row_peers, half, 0),
        ):
            for dz, dx in peers:
                xx, to = near(dz, dx)
                pltpu.make_async_remote_copy(
                    columns(c, h, xx), wr.at[c, base + x], ssem.at[c], rsem.at[c], **to
                ).start()

    loads[13].wait()
    wor[0] = wo[...]
    mine = pl.ds(pl.multiple_of(y * 16, 16), 16)

    def send_output_weights():
        for e in (3, 2, 1):
            pltpu.make_async_remote_copy(
                wo.at[mine], wor.at[e, mine], ssem.at[10], rsem.at[10], **at(server(e), x, t)
            ).start()

    @pl.when(t == 0)
    def _():
        send_output_weights()

    steps_mine = (half == 0) & (x == pair)

    @pl.when(jnp.logical_not(steps_mine))
    def _():
        pltpu.make_async_remote_copy(
            squares_out, squares_in.at[half * NX + x], ssem.at[15], rsem.at[15],
            **at(2 * pair, pair, t),
        ).start()

    def arrived(buffer, count, sem):
        block = buffer.at[pl.ds(0, count)]
        pltpu.make_async_copy(block, block, sem).wait()

    loads[20].wait()
    acc = (acc_s[0], acc_s[1])
    row = iota((ROWS, 1), 0)
    acc_row = jnp.where(row < PROPS, acc[0], acc[1])
    keep = jnp.where((row & 3) < acc_row, 1.0, 0.0)
    r8, c8 = iota((ROWS, ROWS), 0), iota((ROWS, ROWS), 1)
    same = (r8 >> 2) == (c8 >> 2)
    expand = jnp.where(iota((HEADS, WIDTH), 1) // HEAD_DIM == iota((HEADS, WIDTH), 0), 1.0, 0.0)
    for n in (14, 15, 16):
        loads[n].wait()
    kept = pld[...].reshape(ROWS, HEADS) * keep
    later = mm(jnp.where(same & (c8 > r8), 1.0, 0.0), kept, precision=HI)
    coef = mm(keep * jnp.exp(later), expand, precision=HI)
    scaled = coef * phi[...].astype(f32).reshape(ROWS, WIDTH)
    s_hi = scaled.astype(bf16)
    s_lo = (scaled - s_hi.astype(f32)).astype(bf16)
    updates = jnp.concatenate([s_hi.astype(f32), s_lo.astype(f32)], axis=0).astype(bf16)
    keys = pim[...].astype(f32).reshape(ROWS, BC)
    loads[19].wait()
    for b in range(SEQS):
        of_b = (row >> 2) == b
        logs = mm(jnp.where(of_b, kept, 0.0), jnp.ones((ROWS, STATE), f32), 0, 0, precision=HI)
        factor = jnp.exp(logs)
        keys_b = jnp.where(of_b, keys, 0.0)
        keys_b = jnp.concatenate([keys_b, keys_b], axis=0).astype(bf16)
        for g in range(GROUPS):
            upd = mm(
                updates[:, g * GW : g * GW + GW], keys_b[:, g * STATE : g * STATE + STATE], 0, 0
            )
            new = (
                psv[b, g * PER : g * PER + PER] * factor[g * PER : g * PER + PER][:, None, :]
                + upd.reshape(PER, HEAD_DIM, STATE)
            )
            state[b, g * PER : g * PER + PER] = new
            sb[b, g] = new.reshape(GW, STATE).astype(bf16)

    for c in range(4):
        send_weights(c)
    @pl.when(t == 1)
    def _():
        send_output_weights()

    quarters = wor.at[:, pl.ds(0, 16)]
    three_quarters = wor.at[:, pl.ds(0, 48)]

    from_me = (x * 2 + half) * 4 + pair

    def spread(src, dst, index, n):
        def one(d, _):
            other = lax.rem(kv + d, PEERS)
            pltpu.make_async_remote_copy(
                src.at[other],
                dst.at[index],
                ssem.at[n],
                rsem.at[n],
                device_id=(y, other, t),
                device_id_type=MESH,
            ).start()
            return 0

        lax.fori_loop(1, PEERS, one, 0)
        dst[index] = src[kv]

    for level in range(3):
        hear(level)
        if level < 2:
            pass_on(level + 1)


    @pl.when(t == 1)
    def _():
        arrived(tt, 11, rsem.at[4])
        blocks = [tt.at[pl.ds(4, 8)]]
        blocks += [tt.at[lax.rem(x + d, NX)] for d in range(1, NX)]
        for block in blocks:
            pltpu.make_async_remote_copy(
                block, block, ssem.at[14], rsem.at[14], **at(z, x, 1 - t)
            ).start()

    @pl.when(t == 0)
    def _():
        arrived(tt, 11, rsem.at[14])

    lhs[...] = tt[...].reshape(768, 256).T
    loads[5].wait()

    @pl.when(steps_mine)
    def _():
        steps = mm(lhs[:, 0:512], sw[...], 1, 1)
        arrived(squares_in, 7, rsem.at[15])
        squares_in[half * NX + x] = squares_out[...]
        squares = jnp.sum(squares_in[...].astype(f32), axis=0)
        pick = jnp.where(
            (iota((16, 128), 1) == 64) & (iota((16, 128), 0) < 2), 1.0, 0.0
        )
        squares = mm(squares, pick, 0, 0, precision=HI)
        total = squares[:, 64:65]
        high = total.astype(bf16).astype(f32)
        lane = iota((256, 128), 1)
        steps = jnp.where(lane == 64, high, jnp.where(lane == 65, total - high, steps))
        steps_out[...] = steps.reshape(PEERS, ROWS, 128).astype(bf16)
        spread(steps_out, steps_in, pair, 9)

    for c in range(4):
        arrived(wr.at[c], 7, rsem.at[c])
        if c < 2:
            part = mm(lhs[:, 0:512], wr[c].reshape(512, 128))
        else:
            part = mm(lhs[:, 0:256], wr[c, 0:4].reshape(256, 128))
            part = part + mm(lhs[:, 512:768], wr[c, 4:8].reshape(256, 128))
        send[c] = part.reshape(PEERS, ROWS, 128).astype(bf16)
        spread(send.at[c], got.at[c], from_me, 5 + c)
    arrived(quarters, 3, rsem.at[10])
    for d in (2, 1, 3):
        for e in (2, 1, 3):
            block = wor.at[d, mine]
            pltpu.make_async_remote_copy(
                block, block, ssem.at[13], rsem.at[13], **over(e)
            ).start()

    pick_x, pick_bc = heads_selection(acc), maps_selection(acc)
    for n in (6, 7, 8, 9, 10, 11, 12, 17, 18):
        loads[n].wait()
    old_x = phw[...].astype(f32).reshape(14, WIDTH)
    old_x = jnp.concatenate([old_x, jnp.zeros((2, WIDTH), f32)], axis=0)
    old_bc = pmw[...].astype(f32).reshape(28, BC)
    old_bc = jnp.concatenate([old_bc, jnp.zeros((4, BC), f32)], axis=0)
    taps_x = hik[...].astype(f32)
    taps_bc = smk[...].astype(f32).reshape(8, BC)

    def own_heads(ref):
        v = ref[...].reshape(1, 2 * HEADS)
        return jnp.where(t == 0, v[:, :HEADS], v[:, HEADS:])

    speed, direct, bias = own_heads(hds), own_heads(hdg), own_heads(ssb)
    gngv = gng[...].astype(f32).reshape(1, 2 * WIDTH)
    out_gain = jnp.where(t == 0, gngv[:, :WIDTH], gngv[:, WIDTH:])

    def total(c):
        return jnp.sum(got[c].astype(f32).reshape(NX, 2, 4, ROWS, 128), axis=2)

    arrived(got.at[0], PEERS - 1, rsem.at[5])

    @pl.when(steps_mine)
    def _():
        arrived(steps_in, 3, rsem.at[9])

    @pl.when(jnp.logical_not(steps_mine))
    def _():
        arrived(steps_in, 4, rsem.at[9])

    tail = jnp.sum(steps_in[...].astype(f32), axis=0)
    lane8 = iota((ROWS, 128), 1)
    squares = jnp.sum(jnp.where((lane8 == 64) | (lane8 == 65), tail, 0.0), axis=1, keepdims=True)
    inv = lax.rsqrt(squares / D + eps)
    sum0 = total(0)
    raw_b = jnp.concatenate([sum0[g, 0] for g in range(GROUPS)], axis=1) * inv
    raw_c = jnp.concatenate([sum0[g, 1] for g in range(GROUPS)], axis=1) * inv
    win_bc = mm(pick_bc, jnp.concatenate([old_bc, raw_b, raw_c], axis=0).astype(bf16))
    cmw[...] = win_bc[64:92].reshape(SEQS, 7, 2, BC).astype(bf16)
    b_conv = taps_bc[0:1] * win_bc[0:8]
    c_conv = taps_bc[1:2] * win_bc[8:16]
    for k in range(1, 4):
        b_conv = b_conv + taps_bc[2 * k : 2 * k + 1] * win_bc[16 * k : 16 * k + 8]
        c_conv = c_conv + taps_bc[2 * k + 1 : 2 * k + 2] * win_bc[16 * k + 8 : 16 * k + 16]
    b_conv = b_conv * lax.logistic(b_conv)
    c_conv = c_conv * lax.logistic(c_conv)
    step_pre = tail * inv
    step_pre = jnp.where(t == 0, step_pre[:, :HEADS], step_pre[:, HEADS : 2 * HEADS]) + bias
    step = jnp.maximum(step_pre, 0.0) + jnp.log1p(jnp.exp(-jnp.abs(step_pre)))
    decays = pdt[...].reshape(ROWS, HEADS) - speed * step
    cum = mm(jnp.where(same & (c8 <= r8), 1.0, 0.0), decays, precision=HI)
    wide = mm(
        jnp.concatenate([cum, step, jnp.broadcast_to(direct, (ROWS, HEADS))], axis=0),
        expand,
        precision=HI,
    )
    cim[...] = b_conv.reshape(SEQS, PROPS, BC).astype(bf16)
    cld[...] = decays.reshape(SEQS, PROPS, HEADS)
    from_state, pairs = [], []
    for g in range(GROUPS):
        lanes = slice(g * STATE, g * STATE + STATE)
        c_g = c_conv[:, lanes]
        y0 = mm(c_g.astype(bf16), sb[0, g], 1, 1)
        y1 = mm(c_g.astype(bf16), sb[1, g], 1, 1)
        from_state.append(jnp.where(row < PROPS, y0, y1))
        pairs.append(mm(c_g, b_conv[:, lanes], 1, 1, precision=HI))
    from_state = jnp.exp(wide[0:8]) * jnp.concatenate(from_state, axis=1)
    scores = []
    for d in range(PROPS):
        score = [
            jnp.broadcast_to(
                jnp.sum(jnp.where(c8 == r8 - d, p, 0.0), axis=1, keepdims=True), (ROWS, 128)
            )
            for p in pairs
        ]
        scores.append(jnp.concatenate(score, axis=1))

    def third(v, c):
        starts = [g * GW + (c - 1) * 128 for g in range(GROUPS)]
        return jnp.concatenate([v[:, n : n + 128] for n in starts], axis=1)

    def whole(thirds):
        return jnp.concatenate(
            [v[:, g * 128 : g * 128 + 128] for g in range(GROUPS) for v in thirds], axis=1
        )

    slot = half * NX + x

    def to_pair(block, n):
        for dx, dp in ((2, 1), (2, 0), (1, 1), (3, 1), (1, 0), (3, 0), (0, 1)):
            pltpu.make_async_remote_copy(
                block, block, ssem.at[n], rsem.at[n],
                **at(2 * pair + lax.rem(half + dp, 2), lax.rem(x + dx, NX), t),
            ).start()

    windows, inputs = [], []
    energy = [0.0] * GROUPS
    for c in range(1, 4):
        wide_c, taps_c, old_c = third(wide, c), third(taps_x, c), third(old_x, c)
        cum_w, step_w, direct_w = wide_c[0:8], wide_c[8:16], wide_c[16:24]
        decay_w = [None]
        for d in range(1, PROPS):
            gap = jnp.where((row & 3) >= d, cum_w - pltpu.roll(cum_w, d, 0), 0.0)
            decay_w.append(jnp.exp(gap) * scores[d])
        arrived(got.at[c], PEERS - 1, rsem.at[5 + c])
        sum_c = total(c)
        heads_at = 0 if c == 1 else 1
        raw_x = jnp.concatenate([sum_c[g, heads_at] for g in range(GROUPS)], axis=1) * inv
        gate = jnp.concatenate([sum_c[g, 1 - heads_at] for g in range(GROUPS)], axis=1) * inv
        win_x = mm(pick_x, jnp.concatenate([old_c, raw_x], axis=0).astype(bf16))
        windows.append(win_x[32:46])
        x_conv = taps_c[0:1] * win_x[0:8]
        for k in range(1, 4):
            x_conv = x_conv + taps_c[k : k + 1] * win_x[8 * k : 8 * k + 8]
        x_conv = x_conv * lax.logistic(x_conv)
        weighted = step_w * x_conv
        inputs.append(weighted)
        heads = third(from_state, c) + direct_w * x_conv + scores[0] * weighted
        for d in range(1, PROPS):
            term = decay_w[d] * pltpu.roll(weighted, d, 0)
            heads = heads + jnp.where((row & 3) >= d, term, 0.0)
        gated = heads * (gate * lax.logistic(gate))
        for g in range(GROUPS):
            part_g = gated[:, g * 128 : g * 128 + 128]
            energy[g] = energy[g] + jnp.sum(part_g * part_g, axis=1, keepdims=True)
        gated = gated * third(out_gain, c)
        if c < 3:
            nrm[c - 1, slot] = gated.astype(bf16)
            to_pair(nrm.at[c - 1, slot], 15 + c)
            continue
        factors = jnp.zeros((ROWS, 128), f32)
        for g in range(GROUPS):
            factor = lax.rsqrt(energy[g] / GW + eps)
            high = factor.astype(bf16).astype(f32)
            factors = jnp.where(lane8 == g, high, factors)
            factors = jnp.where(lane8 == GROUPS + g, factor - high, factors)
        last[slot] = jnp.concatenate([gated, factors], axis=1).astype(bf16)
        to_pair(last.at[slot], 18)
    chw[...] = whole(windows).reshape(7, SEQS, WIDTH).astype(bf16)
    chi[...] = whole(inputs).reshape(SEQS, PROPS, WIDTH).astype(bf16)

    arrived(three_quarters, 3, rsem.at[13])
    columns_of = wor[...].reshape(256, WIDTH)
    products = [jnp.zeros((64, 256), f32)] * GROUPS
    for c in range(1, 4):
        if c < 3:
            arrived(nrm.at[c - 1], 7, rsem.at[15 + c])
            rows64 = nrm[c - 1].astype(f32).reshape(64, 512).astype(bf16)
        else:
            arrived(last, 7, rsem.at[18])
            rows64 = last[:, :, 0:512].astype(f32).reshape(64, 512).astype(bf16)
        for g in range(GROUPS):
            start = g * GW + (c - 1) * 128
            products[g] = products[g] + mm(
                rows64[:, g * 128 : g * 128 + 128], columns_of[:, start : start + 128], 1, 1
            )
    factors = last[:, :, 512:640].astype(f32).reshape(64, 128)
    factors = factors + pltpu.roll(factors, 128 - GROUPS, 1)
    partial = factors[:, 0:1] * products[0]
    for g in range(1, GROUPS):
        partial = partial + factors[:, g : g + 1] * products[g]
    first_lanes = iota((32, 128), 1) < 64
    for d in (3, 2, 1, 0):
        both = partial[:, 128 * (d // 2) : 128 * (d // 2) + 128]
        turned = pltpu.roll(both, 64, 1)
        low, high = (both, turned) if d % 2 == 0 else (turned, both)
        fs[d] = jnp.where(first_lanes, low[:32], high[32:]).astype(bf16)
        zz, there = served(d), fr.at[pair * NT + t]
        if d == 0:
            fr[pair * NT + t] = fs[0]
        else:
            pltpu.make_async_remote_copy(
                fs.at[d], there, ssem.at[12], rsem.at[12], **at(zz, x, t)
            ).start()
        pltpu.make_async_remote_copy(
            fs.at[d], there, ssem.at[12], rsem.at[12], **at(zz, x, 1 - t)
        ).start()
    arrived(fr, 7, rsem.at[12])

    @pl.when(t == 1)
    def _():
        arrived(tt, 11, ssem.at[4])

    @pl.when(t == 1)
    def _():
        arrived(tt, 11, ssem.at[14])

    @pl.when(jnp.logical_not(steps_mine))
    def _():
        pltpu.make_async_copy(squares_out, squares_out, ssem.at[15]).wait()

    for c in range(4):
        arrived(wr.at[c], 7, ssem.at[c])
        arrived(send.at[c], PEERS - 1, ssem.at[5 + c])

    @pl.when(steps_mine)
    def _():
        arrived(steps_out, PEERS - 1, ssem.at[9])

    arrived(quarters, 3, ssem.at[10])
    arrived(three_quarters, 3, ssem.at[13])
    for c in range(2):
        arrived(nrm.at[c], 7, ssem.at[16 + c])
    arrived(last, 7, ssem.at[18])
    arrived(fr, 7, ssem.at[12])


def finish(fr, *refs):
    ins, outs, mixed, sems = refs[:6], refs[6:13], refs[13], refs[14]
    copies = [
        pltpu.make_async_copy(a, b, sems.at[n]) for n, (a, b) in enumerate(zip(ins, outs[1:]))
    ]
    for copy in copies:
        copy.start()
    done = fr[...].astype(f32).reshape(4, NT, 32, 128)
    done = done[:, 0] + done[:, 1]
    done = jnp.stack([done[:, :, :64], done[:, :, 64:]], axis=1)
    mixed[...] = done.reshape(64, PROPS, 64).astype(bf16)
    copies.append(pltpu.make_async_copy(mixed, outs[0], sems.at[6]))
    copies[-1].start()
    for copy in copies:
        copy.wait()


def local(
    tokens, input_norm_gain, head_input_weight, output_gate_weight, state_maps_weight,
    step_size_weight, step_size_bias, head_decay_speed, proposal_decay_total, head_input_kernel,
    state_maps_kernel, head_direct_gain, grouped_norm_gain, output_weight, prior_state_value,
    previous_head_input, previous_input_maps, previous_log_decays, prior_heads_window,
    prior_maps_window, accepted,
):
    anywhere = pl.BlockSpec(memory_space=pl.ANY)
    vmem = pl.BlockSpec(memory_space=pltpu.VMEM)
    V, DMA = pltpu.VMEM, pltpu.SemaphoreType.DMA
    outs = (
        jax.ShapeDtypeStruct((NX * NT, 32, 128), bf16),
        jax.ShapeDtypeStruct((SEQS, HEADS, HEAD_DIM, STATE), f32),
        jax.ShapeDtypeStruct((SEQS, PROPS, WIDTH), bf16),
        jax.ShapeDtypeStruct((SEQS, PROPS, BC), bf16),
        jax.ShapeDtypeStruct((SEQS, PROPS, HEADS), f32),
        jax.ShapeDtypeStruct((7, SEQS, WIDTH), bf16),
        jax.ShapeDtypeStruct((SEQS, 7, 2, BC), bf16),
    )
    def in_hbm(v):
        return pltpu.with_memory_space_constraint(v, pltpu.HBM)

    results = pl.pallas_call(
        kernel,
        out_shape=outs,
        in_specs=[anywhere] * 21,
        out_specs=[vmem] * 7,
        scratch_shapes=[
            V((64, PROPS, 64), bf16), V((D,), bf16), V((2, 64, WIDTH), bf16),
            V((64, 2, BC), bf16), V((48,), f32), V((48,), f32), V((SEQS, PROPS, HEADS), f32),
            V((4, WIDTH), bf16), V((4, 2, BC), bf16), V((48,), f32), V((2 * WIDTH,), bf16),
            V((64, WIDTH), bf16), V((SEQS, HEADS, HEAD_DIM, STATE), f32),
            V((SEQS, PROPS, WIDTH), bf16), V((SEQS, PROPS, BC), bf16),
            V((SEQS, PROPS, HEADS), f32), V((7, SEQS, WIDTH), bf16), V((SEQS, 7, 2, BC), bf16),
            V((128, 512), bf16), V((8, 64, 128), bf16), V((12, 64, 256), bf16), V((16, 256), bf16), V((8, 16, 256), bf16),
            V((256, 768), bf16), V((4, 8, 64, 128), bf16), V((4, PEERS, ROWS, 128), bf16),
            V((4, PEERS, ROWS, 128), bf16), V((PEERS, ROWS, 128), bf16), V((4, ROWS, 128), bf16),
            V((NX, 64, WIDTH), bf16), V((SEQS, GROUPS, GW, STATE), bf16),
            V((2, 8, ROWS, 512), bf16), V((8, ROWS, 640), bf16), V((NX, 32, 128), bf16),
            pltpu.SMEM((SEQS,), i32), DMA((21,)), DMA((19,)), DMA((19,)),
            pltpu.SemaphoreType.REGULAR((3, 2)),
        ],
        compiler_params=pltpu.CompilerParams(
            collective_id=0, has_side_effects=True, vmem_limit_bytes=40 * 1024 * 1024
        ),
    )(*(in_hbm(v) for v in (
        tokens, input_norm_gain, head_input_weight, output_gate_weight, state_maps_weight,
        step_size_weight.T, step_size_bias, head_decay_speed, proposal_decay_total,
        head_input_kernel, state_maps_kernel, head_direct_gain, grouped_norm_gain,
        output_weight.T, prior_state_value, previous_head_input, previous_input_maps,
        previous_log_decays, jnp.transpose(prior_heads_window, (1, 0, 2)), prior_maps_window,
        accepted,
    )))
    finals = (jax.ShapeDtypeStruct((64, PROPS, 64), bf16), *outs[1:])
    mixed, state, chi, cim, cld, chw, cmw = pl.pallas_call(
        finish,
        out_shape=finals,
        in_specs=[vmem] * 7,
        out_specs=[anywhere] * 7,
        scratch_shapes=[V((64, PROPS, 64), bf16), DMA((7,))],
        compiler_params=pltpu.CompilerParams(vmem_limit_bytes=8 * 1024 * 1024),
    )(*results)
    return mixed, state, chi, cim, cld, jnp.transpose(chw, (1, 0, 2)), cmw


def solution(mesh):
    seq = ("dp", "kv")
    return jax.shard_map(
        local,
        mesh=mesh,
        in_specs=(
            P("dp", None, "kv"), P(), P("kv", "tp"), P("kv", "tp"), P("kv", None, "tp"), P(), P(),
            P(), P(seq, None, "tp"), P(), P(), P(), P(), P("tp", "kv"), P(seq, "tp", None, None),
            P(seq, None, "tp"), P(seq, None, "tp"), P(seq, None, "tp"), P(seq, None, "tp"),
            P(seq, None, None, "tp"), P(seq),
        ),
        out_specs=(
            P("dp", None, "kv"), P(seq, "tp", None, None), P(seq, None, "tp"), P(seq, None, "tp"),
            P(seq, None, "tp"), P(seq, None, "tp"), P(seq, None, None, "tp"),
        ),
        check_vma=False,
    )
```

```python
import functools

import jax
import jax.numpy as jnp
from jax import lax
from jax.experimental import pallas as pl
from jax.experimental.pallas import tpu as pltpu
from jax.sharding import PartitionSpec as P

MESH = pl.DeviceIdType.MESH
HI = lax.Precision.HIGHEST
f32, bf16, i32 = jnp.float32, jnp.bfloat16, jnp.int32

NX, NY, NZ, NT = 4, 4, 8, 2
PEERS = NX * NZ
D, STATE, HEAD_DIM = 2048, 128, 64
SEQS, PROPS, ROWS = 2, 4, 8
HEADS, GROUPS, PER = 24, 4, 6
WIDTH, GW = 1536, 384
BC = 512
eps = 1e-06


def iota(shape, dim):
    return lax.broadcasted_iota(i32, shape, dim)


def mm(a, b, ca=1, cb=0, precision=None):
    return lax.dot_general(
        a, b, (((ca,), (cb,)), ((), ())), precision=precision, preferred_element_type=f32
    )


def heads_selection(acc):
    shape = (48, 24)
    i, j = iota(shape, 0), iota(shape, 1)
    out = i >= 32
    b = jnp.where(out, i & 1, (i >> 2) & 1)
    pos = jnp.where(out, (i - 32) >> 1, (i & 3) + (i >> 3))
    acc_b = jnp.where(b == 0, acc[0], acc[1])
    old = (j < 14) & ((j & 1) == b) & ((j >> 1) == acc_b + pos)
    raw = (j >= 16) & (((j - 16) >> 2) == b) & (((j - 16) & 3) == pos - 3)
    pick = jnp.where(pos < 3, jnp.where(old, 1.0, 0.0), jnp.where(raw, 1.0, 0.0))
    return pick.astype(bf16)


def maps_selection(acc):
    shape = (96, 48)
    i, j = iota(shape, 0), iota(shape, 1)
    out = i >= 64
    o = i - 64
    ob = jnp.where(o >= 14, 1, 0)
    orem = o - 14 * ob
    b = jnp.where(out, ob, (i >> 2) & 1)
    pos = jnp.where(out, orem >> 1, (i & 3) + (i >> 4))
    kind = jnp.where(out, orem & 1, (i >> 3) & 1)
    acc_b = jnp.where(b == 0, acc[0], acc[1])
    jb = jnp.where(j >= 14, 1, 0)
    jrem = j - 14 * jb
    old = (j < 28) & (jb == b) & ((jrem & 1) == kind) & ((jrem >> 1) == acc_b + pos)
    jr = j - 32
    raw = (j >= 32) & ((jr >> 3) == kind) & (((jr >> 2) & 1) == b) & ((jr & 3) == pos - 3)
    pick = jnp.where(pos < 3, jnp.where(old, 1.0, 0.0), jnp.where(raw, 1.0, 0.0))
    return pick.astype(bf16)


def kernel(
    tok_h, gain_h, wx_h, wg_h, smw_h, sw_h, ssb_h, hds_h, pdt_h, hik_h, smk_h, hdg_h, gng_h, wo_h,
    psv_h, phi_h, pim_h, pld_h, phw_h, pmw_h, acc_h,
    fr, state, chi, cim, cld, chw, cmw,
    tok, gain, wxg, smw, ssb, hds, pdt, hik, smk, hdg, gng, wo, psv, phi, pim, pld, phw, pmw,
    sw, bcs, tt, squares_out, squares_in, lhs, wr, send, got, steps_out, steps_in, wor, sb, nrm, last, fs,
    acc_s, lsem, ssem, rsem, level_sem,
):
    y, kv, t = lax.axis_index("dp"), lax.axis_index("kv"), lax.axis_index("tp")
    z, x = kv // NX, kv % NX
    pair, half = z // 2, z % 2

    def at(zz, xx, tt_):
        return dict(device_id=(y, zz * NX + xx, tt_), device_id_type=MESH)

    def over(d):
        return dict(device_id=(lax.rem(y + d, NY), kv, t), device_id_type=MESH)

    def served(e):
        return lax.rem(z + (2 * half - 1) * e + NZ, NZ)

    def server(e):
        return lax.rem(z + (1 - 2 * ((half + e) % 2)) * e + NZ, NZ)

    loads = {}
    plan = (
        (tok_h, tok), (gain_h, gain), (smw_h, smw), (wx_h, wxg.at[0]), (wg_h, wxg.at[1]),
        (sw_h.at[:, pl.ds(pl.multiple_of(pair * 512, 512), 512)], sw.at[pl.ds(0, 48)]),
        (ssb_h, ssb), (hds_h, hds), (pdt_h, pdt),
        (hik_h.at[:, pl.ds(pl.multiple_of(t * WIDTH, 128), WIDTH)], hik),
        (smk_h.at[:, :, pl.ds(pl.multiple_of(t * BC, 128), BC)], smk),
        (hdg_h, hdg), (gng_h, gng), (wo_h, wo), (phi_h, phi), (pim_h, pim), (pld_h, pld),
        (phw_h, phw), (pmw_h, pmw), (psv_h, psv), (acc_h, acc_s),
    )
    for n, (src, dst) in enumerate(plan):
        loads[n] = pltpu.make_async_copy(src, dst, lsem.at[n])
    for n in (0, 1, 2):
        loads[n].start()

    barrier = pltpu.get_barrier_semaphore()

    row_peers = [(0, 2), (0, 1), (0, 3)]
    up_peers = [(1, 2), (1, 1), (1, 3), (1, 0)]
    down_peers = [(NZ - 1, dx) for _, dx in up_peers]

    def near(dz, dx):
        return lax.rem(x + dx, NX), at(lax.rem(z + dz, NZ), lax.rem(x + dx, NX), t)

    for dz, dx in row_peers + up_peers + down_peers:
        pl.semaphore_signal(barrier, inc=1, **near(dz, dx)[1])
    for d in range(NX):
        pl.semaphore_signal(barrier, inc=1, **at(z, lax.rem(x + d, NX), 1 - t))
    for d in range(1, NY):
        pl.semaphore_signal(barrier, inc=1, **over(d))
    for e in (2, 3):
        pl.semaphore_signal(barrier, inc=1, **at(served(e), x, t))
    for n in range(3, len(plan)):
        loads[n].start()

    for n in (0, 1, 2):
        loads[n].wait()
    tok32 = tok[...].astype(f32).reshape(256, 64)
    gains = gain[...].astype(f32).reshape(16, 128)
    gain_row = jnp.sum(
        jnp.where(iota((16, 128), 0) == kv // 2, gains, 0.0), axis=0, keepdims=True
    )
    gain_row = jnp.where(kv % 2 == 0, gain_row[:, :64], gain_row[:, 64:])
    tt[x, 0:64] = (tok32 * gain_row).astype(bf16).T
    sumsq = jnp.sum(jnp.square(tok32.T), axis=0, keepdims=True)
    high = sumsq.astype(bf16).astype(f32)
    line = iota((16, 256), 0)
    squares_out[...] = jnp.where(
        line == 0, high, jnp.where(line == 1, sumsq - high, 0.0)
    ).astype(bf16)
    for n in range(2):
        part = smw[:, n, :]
        for g in range(GROUPS):
            bcs[n * GROUPS + g] = part[:, g * STATE : g * STATE + STATE]
    sw[48:128] = jnp.zeros((80, 512), bf16)

    def columns(c, h, xx):
        if c == 0:
            return bcs.at[h * NX + xx]
        return wxg.at[
            h if c == 1 else 1 - h, :, pl.ds(pl.multiple_of(xx * GW + (c - 1) * 128, 128), 128)
        ]

    loads[3].wait()
    loads[4].wait()
    for c in range(4):
        wr[c, x] = columns(c, half, x)[...]

    pl.semaphore_wait(barrier, 11 + NX + NY - 1 + 2)

    def pass_on(level):
        for n, dz in enumerate((1, NZ - 1)):
            pl.semaphore_signal(level_sem.at[level, n], inc=1, **near(dz, 0)[1])

    def hear(level):
        for n in range(2):
            pl.semaphore_wait(level_sem.at[level, n], 1)

    pass_on(0)

    @pl.when(t == 1)
    def _():
        turns = [p for two in zip(up_peers, down_peers) for p in zip(two, (8, 4))]
        for (dz, dx), base in turns + [(p, 0) for p in row_peers]:
            pltpu.make_async_remote_copy(
                tt.at[x],
                tt.at[base + x],
                ssem.at[4],
                rsem.at[{0: 11, 4: 4, 8: 19}[base]],
                **near(dz, dx)[1],
            ).start()

    def send_weights(c):
        for peers, h, base in (
            (down_peers if c < 2 else up_peers, 1 - half, 4),
            (row_peers, half, 0),
        ):
            for dz, dx in peers:
                xx, to = near(dz, dx)
                pltpu.make_async_remote_copy(
                    columns(c, h, xx), wr.at[c, base + x], ssem.at[c], rsem.at[c], **to
                ).start()

    loads[13].wait()
    wor[0] = wo[...]
    mine = pl.ds(pl.multiple_of(y * 16, 16), 16)

    def send_output_weights():
        for e in (3, 2, 1):
            pltpu.make_async_remote_copy(
                wo.at[mine], wor.at[e, mine], ssem.at[10], rsem.at[10], **at(server(e), x, t)
            ).start()

    @pl.when(t == 0)
    def _():
        send_output_weights()

    steps_mine = (half == 0) & (x == pair)

    @pl.when(jnp.logical_not(steps_mine))
    def _():
        pltpu.make_async_remote_copy(
            squares_out, squares_in.at[half * NX + x], ssem.at[15], rsem.at[15],
            **at(2 * pair, pair, t),
        ).start()

    def arrived(buffer, count, sem):
        block = buffer.at[pl.ds(0, count)]
        pltpu.make_async_copy(block, block, sem).wait()

    loads[20].wait()
    acc = (acc_s[0], acc_s[1])
    row = iota((ROWS, 1), 0)
    acc_row = jnp.where(row < PROPS, acc[0], acc[1])
    keep = jnp.where((row & 3) < acc_row, 1.0, 0.0)
    r8, c8 = iota((ROWS, ROWS), 0), iota((ROWS, ROWS), 1)
    same = (r8 >> 2) == (c8 >> 2)
    expand = jnp.where(iota((HEADS, WIDTH), 1) // HEAD_DIM == iota((HEADS, WIDTH), 0), 1.0, 0.0)
    for n in (14, 15, 16):
        loads[n].wait()
    kept = pld[...].reshape(ROWS, HEADS) * keep
    later = mm(jnp.where(same & (c8 > r8), 1.0, 0.0), kept, precision=HI)
    coef = mm(keep * jnp.exp(later), expand, precision=HI)
    scaled = coef * phi[...].astype(f32).reshape(ROWS, WIDTH)
    s_hi = scaled.astype(bf16)
    s_lo = (scaled - s_hi.astype(f32)).astype(bf16)
    updates = jnp.concatenate([s_hi.astype(f32), s_lo.astype(f32)], axis=0).astype(bf16)
    keys = pim[...].astype(f32).reshape(ROWS, BC)
    loads[19].wait()
    for b in range(SEQS):
        of_b = (row >> 2) == b
        logs = mm(jnp.where(of_b, kept, 0.0), jnp.ones((ROWS, STATE), f32), 0, 0, precision=HI)
        factor = jnp.exp(logs)
        keys_b = jnp.where(of_b, keys, 0.0)
        keys_b = jnp.concatenate([keys_b, keys_b], axis=0).astype(bf16)
        for g in range(GROUPS):
            upd = mm(
                updates[:, g * GW : g * GW + GW], keys_b[:, g * STATE : g * STATE + STATE], 0, 0
            )
            new = (
                psv[b, g * PER : g * PER + PER] * factor[g * PER : g * PER + PER][:, None, :]
                + upd.reshape(PER, HEAD_DIM, STATE)
            )
            state[b, g * PER : g * PER + PER] = new
            sb[b, g] = new.reshape(GW, STATE).astype(bf16)

    for c in range(4):
        send_weights(c)
    @pl.when(t == 1)
    def _():
        send_output_weights()

    quarters = wor.at[:, pl.ds(0, 16)]
    three_quarters = wor.at[:, pl.ds(0, 48)]

    from_me = (x * 2 + half) * 4 + pair

    def spread(src, dst, index, n):
        def one(d, _):
            other = lax.rem(kv + d, PEERS)
            pltpu.make_async_remote_copy(
                src.at[other],
                dst.at[index],
                ssem.at[n],
                rsem.at[n],
                device_id=(y, other, t),
                device_id_type=MESH,
            ).start()
            return 0

        lax.fori_loop(1, PEERS, one, 0)
        dst[index] = src[kv]

    for level in range(3):
        hear(level)
        if level < 2:
            pass_on(level + 1)


    @pl.when(t == 1)
    def _():
        row_blocks = [tt.at[lax.rem(x + d, NX)] for d in range(1, NX)]
        for count, n, blocks in (
            (3, 11, row_blocks),
            (4, 4, [tt.at[pl.ds(4, 4)]]),
            (4, 19, [tt.at[pl.ds(8, 4)]]),
        ):
            arrived(tt, count, rsem.at[n])
            for block in blocks:
                pltpu.make_async_remote_copy(
                    block, block, ssem.at[14], rsem.at[14], **at(z, x, 1 - t)
                ).start()

    @pl.when(t == 0)
    def _():
        arrived(tt, 11, rsem.at[14])

    lhs[...] = tt[...].reshape(768, 256).T
    loads[5].wait()

    @pl.when(steps_mine)
    def _():
        steps = mm(lhs[:, 0:512], sw[...], 1, 1)
        arrived(squares_in, 7, rsem.at[15])
        squares_in[half * NX + x] = squares_out[...]
        squares = jnp.sum(squares_in[...].astype(f32), axis=0)
        pick = jnp.where(
            (iota((16, 128), 1) == 64) & (iota((16, 128), 0) < 2), 1.0, 0.0
        )
        squares = mm(squares, pick, 0, 0, precision=HI)
        total = squares[:, 64:65]
        high = total.astype(bf16).astype(f32)
        lane = iota((256, 128), 1)
        steps = jnp.where(lane == 64, high, jnp.where(lane == 65, total - high, steps))
        steps_out[...] = steps.reshape(PEERS, ROWS, 128).astype(bf16)
        spread(steps_out, steps_in, pair, 9)

    for c in range(4):
        arrived(wr.at[c], 7, rsem.at[c])
        if c < 2:
            part = mm(lhs[:, 0:512], wr[c].reshape(512, 128))
        else:
            part = mm(lhs[:, 0:256], wr[c, 0:4].reshape(256, 128))
            part = part + mm(lhs[:, 512:768], wr[c, 4:8].reshape(256, 128))
        send[c] = part.reshape(PEERS, ROWS, 128).astype(bf16)
        spread(send.at[c], got.at[c], from_me, 5 + c)
    arrived(quarters, 3, rsem.at[10])
    for d in (2, 1, 3):
        for e in (2, 1, 3):
            block = wor.at[d, mine]
            pltpu.make_async_remote_copy(
                block, block, ssem.at[13], rsem.at[13], **over(e)
            ).start()

    pick_x, pick_bc = heads_selection(acc), maps_selection(acc)
    for n in (6, 7, 8, 9, 10, 11, 12, 17, 18):
        loads[n].wait()
    old_x = phw[...].astype(f32).reshape(14, WIDTH)
    old_x = jnp.concatenate([old_x, jnp.zeros((2, WIDTH), f32)], axis=0)
    old_bc = pmw[...].astype(f32).reshape(28, BC)
    old_bc = jnp.concatenate([old_bc, jnp.zeros((4, BC), f32)], axis=0)
    taps_x = hik[...].astype(f32)
    taps_bc = smk[...].astype(f32).reshape(8, BC)

    def own_heads(ref):
        v = ref[...].reshape(1, 2 * HEADS)
        return jnp.where(t == 0, v[:, :HEADS], v[:, HEADS:])

    speed, direct, bias = own_heads(hds), own_heads(hdg), own_heads(ssb)
    gngv = gng[...].astype(f32).reshape(1, 2 * WIDTH)
    out_gain = jnp.where(t == 0, gngv[:, :WIDTH], gngv[:, WIDTH:])

    def total(c):
        return jnp.sum(got[c].astype(f32).reshape(NX, 2, 4, ROWS, 128), axis=2)

    arrived(got.at[0], PEERS - 1, rsem.at[5])

    @pl.when(steps_mine)
    def _():
        arrived(steps_in, 3, rsem.at[9])

    @pl.when(jnp.logical_not(steps_mine))
    def _():
        arrived(steps_in, 4, rsem.at[9])

    tail = jnp.sum(steps_in[...].astype(f32), axis=0)
    lane8 = iota((ROWS, 128), 1)
    squares = jnp.sum(jnp.where((lane8 == 64) | (lane8 == 65), tail, 0.0), axis=1, keepdims=True)
    inv = lax.rsqrt(squares / D + eps)
    sum0 = total(0)
    raw_b = jnp.concatenate([sum0[g, 0] for g in range(GROUPS)], axis=1) * inv
    raw_c = jnp.concatenate([sum0[g, 1] for g in range(GROUPS)], axis=1) * inv
    win_bc = mm(pick_bc, jnp.concatenate([old_bc, raw_b, raw_c], axis=0).astype(bf16))
    cmw[...] = win_bc[64:92].reshape(SEQS, 7, 2, BC).astype(bf16)
    b_conv = taps_bc[0:1] * win_bc[0:8]
    c_conv = taps_bc[1:2] * win_bc[8:16]
    for k in range(1, 4):
        b_conv = b_conv + taps_bc[2 * k : 2 * k + 1] * win_bc[16 * k : 16 * k + 8]
        c_conv = c_conv + taps_bc[2 * k + 1 : 2 * k + 2] * win_bc[16 * k + 8 : 16 * k + 16]
    b_conv = b_conv * lax.logistic(b_conv)
    c_conv = c_conv * lax.logistic(c_conv)
    step_pre = tail * inv
    step_pre = jnp.where(t == 0, step_pre[:, :HEADS], step_pre[:, HEADS : 2 * HEADS]) + bias
    step = jnp.maximum(step_pre, 0.0) + jnp.log1p(jnp.exp(-jnp.abs(step_pre)))
    decays = pdt[...].reshape(ROWS, HEADS) - speed * step
    cum = mm(jnp.where(same & (c8 <= r8), 1.0, 0.0), decays, precision=HI)
    wide = mm(
        jnp.concatenate([cum, step, jnp.broadcast_to(direct, (ROWS, HEADS))], axis=0),
        expand,
        precision=HI,
    )
    cim[...] = b_conv.reshape(SEQS, PROPS, BC).astype(bf16)
    cld[...] = decays.reshape(SEQS, PROPS, HEADS)
    from_state, pairs = [], []
    for g in range(GROUPS):
        lanes = slice(g * STATE, g * STATE + STATE)
        c_g = c_conv[:, lanes]
        y0 = mm(c_g.astype(bf16), sb[0, g], 1, 1)
        y1 = mm(c_g.astype(bf16), sb[1, g], 1, 1)
        from_state.append(jnp.where(row < PROPS, y0, y1))
        pairs.append(mm(c_g, b_conv[:, lanes], 1, 1, precision=HI))
    from_state = jnp.exp(wide[0:8]) * jnp.concatenate(from_state, axis=1)
    scores = []
    for d in range(PROPS):
        score = [
            jnp.broadcast_to(
                jnp.sum(jnp.where(c8 == r8 - d, p, 0.0), axis=1, keepdims=True), (ROWS, 128)
            )
            for p in pairs
        ]
        scores.append(jnp.concatenate(score, axis=1))

    def third(v, c):
        starts = [g * GW + (c - 1) * 128 for g in range(GROUPS)]
        return jnp.concatenate([v[:, n : n + 128] for n in starts], axis=1)

    def whole(thirds):
        return jnp.concatenate(
            [v[:, g * 128 : g * 128 + 128] for g in range(GROUPS) for v in thirds], axis=1
        )

    slot = half * NX + x

    def to_pair(block, n):
        for dx, dp in ((2, 1), (2, 0), (1, 1), (3, 1), (1, 0), (3, 0), (0, 1)):
            pltpu.make_async_remote_copy(
                block, block, ssem.at[n], rsem.at[n],
                **at(2 * pair + lax.rem(half + dp, 2), lax.rem(x + dx, NX), t),
            ).start()

    windows, inputs = [], []
    energy = [0.0] * GROUPS
    for c in range(1, 4):
        wide_c, taps_c, old_c = third(wide, c), third(taps_x, c), third(old_x, c)
        cum_w, step_w, direct_w = wide_c[0:8], wide_c[8:16], wide_c[16:24]
        decay_w = [None]
        for d in range(1, PROPS):
            gap = jnp.where((row & 3) >= d, cum_w - pltpu.roll(cum_w, d, 0), 0.0)
            decay_w.append(jnp.exp(gap) * scores[d])
        arrived(got.at[c], PEERS - 1, rsem.at[5 + c])
        sum_c = total(c)
        heads_at = 0 if c == 1 else 1
        raw_x = jnp.concatenate([sum_c[g, heads_at] for g in range(GROUPS)], axis=1) * inv
        gate = jnp.concatenate([sum_c[g, 1 - heads_at] for g in range(GROUPS)], axis=1) * inv
        win_x = mm(pick_x, jnp.concatenate([old_c, raw_x], axis=0).astype(bf16))
        windows.append(win_x[32:46])
        x_conv = taps_c[0:1] * win_x[0:8]
        for k in range(1, 4):
            x_conv = x_conv + taps_c[k : k + 1] * win_x[8 * k : 8 * k + 8]
        x_conv = x_conv * lax.logistic(x_conv)
        weighted = step_w * x_conv
        inputs.append(weighted)
        heads = third(from_state, c) + direct_w * x_conv + scores[0] * weighted
        for d in range(1, PROPS):
            term = decay_w[d] * pltpu.roll(weighted, d, 0)
            heads = heads + jnp.where((row & 3) >= d, term, 0.0)
        gated = heads * (gate * lax.logistic(gate))
        for g in range(GROUPS):
            part_g = gated[:, g * 128 : g * 128 + 128]
            energy[g] = energy[g] + jnp.sum(part_g * part_g, axis=1, keepdims=True)
        gated = gated * third(out_gain, c)
        if c < 3:
            nrm[c - 1, slot] = gated.astype(bf16)
            to_pair(nrm.at[c - 1, slot], 15 + c)
            continue
        factors = jnp.zeros((ROWS, 128), f32)
        for g in range(GROUPS):
            factor = lax.rsqrt(energy[g] / GW + eps)
            high = factor.astype(bf16).astype(f32)
            factors = jnp.where(lane8 == g, high, factors)
            factors = jnp.where(lane8 == GROUPS + g, factor - high, factors)
        last[slot] = jnp.concatenate([gated, factors], axis=1).astype(bf16)
        to_pair(last.at[slot], 18)
    chw[...] = whole(windows).reshape(7, SEQS, WIDTH).astype(bf16)
    chi[...] = whole(inputs).reshape(SEQS, PROPS, WIDTH).astype(bf16)

    arrived(three_quarters, 3, rsem.at[13])
    columns_of = wor[...].reshape(256, WIDTH)
    products = [jnp.zeros((64, 256), f32)] * GROUPS
    for c in range(1, 4):
        if c < 3:
            arrived(nrm.at[c - 1], 7, rsem.at[15 + c])
            rows64 = nrm[c - 1].astype(f32).reshape(64, 512).astype(bf16)
        else:
            arrived(last, 7, rsem.at[18])
            rows64 = last[:, :, 0:512].astype(f32).reshape(64, 512).astype(bf16)
        for g in range(GROUPS):
            start = g * GW + (c - 1) * 128
            products[g] = products[g] + mm(
                rows64[:, g * 128 : g * 128 + 128], columns_of[:, start : start + 128], 1, 1
            )
    factors = last[:, :, 512:640].astype(f32).reshape(64, 128)
    factors = factors + pltpu.roll(factors, 128 - GROUPS, 1)
    partial = factors[:, 0:1] * products[0]
    for g in range(1, GROUPS):
        partial = partial + factors[:, g : g + 1] * products[g]
    first_lanes = iota((32, 128), 1) < 64
    for d in (3, 2, 1, 0):
        both = partial[:, 128 * (d // 2) : 128 * (d // 2) + 128]
        turned = pltpu.roll(both, 64, 1)
        low, high = (both, turned) if d % 2 == 0 else (turned, both)
        fs[d] = jnp.where(first_lanes, low[:32], high[32:]).astype(bf16)
        zz, there = served(d), fr.at[pair * NT + t]
        if d == 0:
            fr[pair * NT + t] = fs[0]
        else:
            pltpu.make_async_remote_copy(
                fs.at[d], there, ssem.at[12], rsem.at[12], **at(zz, x, t)
            ).start()
        pltpu.make_async_remote_copy(
            fs.at[d], there, ssem.at[12], rsem.at[12], **at(zz, x, 1 - t)
        ).start()
    arrived(fr, 7, rsem.at[12])

    @pl.when(t == 1)
    def _():
        arrived(tt, 11, ssem.at[4])

    @pl.when(t == 1)
    def _():
        arrived(tt, 11, ssem.at[14])

    @pl.when(jnp.logical_not(steps_mine))
    def _():
        pltpu.make_async_copy(squares_out, squares_out, ssem.at[15]).wait()

    for c in range(4):
        arrived(wr.at[c], 7, ssem.at[c])
        arrived(send.at[c], PEERS - 1, ssem.at[5 + c])

    @pl.when(steps_mine)
    def _():
        arrived(steps_out, PEERS - 1, ssem.at[9])

    arrived(quarters, 3, ssem.at[10])
    arrived(three_quarters, 3, ssem.at[13])
    for c in range(2):
        arrived(nrm.at[c], 7, ssem.at[16 + c])
    arrived(last, 7, ssem.at[18])
    arrived(fr, 7, ssem.at[12])


def finish(fr, *refs):
    ins, outs, mixed, sems = refs[:6], refs[6:13], refs[13], refs[14]
    copies = [
        pltpu.make_async_copy(a, b, sems.at[n]) for n, (a, b) in enumerate(zip(ins, outs[1:]))
    ]
    for copy in copies:
        copy.start()
    done = fr[...].astype(f32).reshape(4, NT, 32, 128)
    done = done[:, 0] + done[:, 1]
    done = jnp.stack([done[:, :, :64], done[:, :, 64:]], axis=1)
    mixed[...] = done.reshape(64, PROPS, 64).astype(bf16)
    copies.append(pltpu.make_async_copy(mixed, outs[0], sems.at[6]))
    copies[-1].start()
    for copy in copies:
        copy.wait()


def local(
    tokens, input_norm_gain, head_input_weight, output_gate_weight, state_maps_weight,
    step_size_weight, step_size_bias, head_decay_speed, proposal_decay_total, head_input_kernel,
    state_maps_kernel, head_direct_gain, grouped_norm_gain, output_weight, prior_state_value,
    previous_head_input, previous_input_maps, previous_log_decays, prior_heads_window,
    prior_maps_window, accepted,
):
    anywhere = pl.BlockSpec(memory_space=pl.ANY)
    vmem = pl.BlockSpec(memory_space=pltpu.VMEM)
    V, DMA = pltpu.VMEM, pltpu.SemaphoreType.DMA
    outs = (
        jax.ShapeDtypeStruct((NX * NT, 32, 128), bf16),
        jax.ShapeDtypeStruct((SEQS, HEADS, HEAD_DIM, STATE), f32),
        jax.ShapeDtypeStruct((SEQS, PROPS, WIDTH), bf16),
        jax.ShapeDtypeStruct((SEQS, PROPS, BC), bf16),
        jax.ShapeDtypeStruct((SEQS, PROPS, HEADS), f32),
        jax.ShapeDtypeStruct((7, SEQS, WIDTH), bf16),
        jax.ShapeDtypeStruct((SEQS, 7, 2, BC), bf16),
    )
    def in_hbm(v):
        return pltpu.with_memory_space_constraint(v, pltpu.HBM)

    results = pl.pallas_call(
        kernel,
        out_shape=outs,
        in_specs=[anywhere] * 21,
        out_specs=[vmem] * 7,
        scratch_shapes=[
            V((64, PROPS, 64), bf16), V((D,), bf16), V((2, 64, WIDTH), bf16),
            V((64, 2, BC), bf16), V((48,), f32), V((48,), f32), V((SEQS, PROPS, HEADS), f32),
            V((4, WIDTH), bf16), V((4, 2, BC), bf16), V((48,), f32), V((2 * WIDTH,), bf16),
            V((64, WIDTH), bf16), V((SEQS, HEADS, HEAD_DIM, STATE), f32),
            V((SEQS, PROPS, WIDTH), bf16), V((SEQS, PROPS, BC), bf16),
            V((SEQS, PROPS, HEADS), f32), V((7, SEQS, WIDTH), bf16), V((SEQS, 7, 2, BC), bf16),
            V((128, 512), bf16), V((8, 64, 128), bf16), V((12, 64, 256), bf16), V((16, 256), bf16), V((8, 16, 256), bf16),
            V((256, 768), bf16), V((4, 8, 64, 128), bf16), V((4, PEERS, ROWS, 128), bf16),
            V((4, PEERS, ROWS, 128), bf16), V((PEERS, ROWS, 128), bf16), V((4, ROWS, 128), bf16),
            V((NX, 64, WIDTH), bf16), V((SEQS, GROUPS, GW, STATE), bf16),
            V((2, 8, ROWS, 512), bf16), V((8, ROWS, 640), bf16), V((NX, 32, 128), bf16),
            pltpu.SMEM((SEQS,), i32), DMA((21,)), DMA((19,)), DMA((20,)),
            pltpu.SemaphoreType.REGULAR((3, 2)),
        ],
        compiler_params=pltpu.CompilerParams(
            collective_id=0, has_side_effects=True, vmem_limit_bytes=40 * 1024 * 1024
        ),
    )(*(in_hbm(v) for v in (
        tokens, input_norm_gain, head_input_weight, output_gate_weight, state_maps_weight,
        step_size_weight.T, step_size_bias, head_decay_speed, proposal_decay_total,
        head_input_kernel, state_maps_kernel, head_direct_gain, grouped_norm_gain,
        output_weight.T, prior_state_value, previous_head_input, previous_input_maps,
        previous_log_decays, jnp.transpose(prior_heads_window, (1, 0, 2)), prior_maps_window,
        accepted,
    )))
    finals = (jax.ShapeDtypeStruct((64, PROPS, 64), bf16), *outs[1:])
    mixed, state, chi, cim, cld, chw, cmw = pl.pallas_call(
        finish,
        out_shape=finals,
        in_specs=[vmem] * 7,
        out_specs=[anywhere] * 7,
        scratch_shapes=[V((64, PROPS, 64), bf16), DMA((7,))],
        compiler_params=pltpu.CompilerParams(vmem_limit_bytes=8 * 1024 * 1024),
    )(*results)
    return mixed, state, chi, cim, cld, jnp.transpose(chw, (1, 0, 2)), cmw


def solution(mesh):
    seq = ("dp", "kv")
    return jax.shard_map(
        local,
        mesh=mesh,
        in_specs=(
            P("dp", None, "kv"), P(), P("kv", "tp"), P("kv", "tp"), P("kv", None, "tp"), P(), P(),
            P(), P(seq, None, "tp"), P(), P(), P(), P(), P("tp", "kv"), P(seq, "tp", None, None),
            P(seq, None, "tp"), P(seq, None, "tp"), P(seq, None, "tp"), P(seq, None, "tp"),
            P(seq, None, None, "tp"), P(seq),
        ),
        out_specs=(
            P("dp", None, "kv"), P(seq, "tp", None, None), P(seq, None, "tp"), P(seq, None, "tp"),
            P(seq, None, "tp"), P(seq, None, "tp"), P(seq, None, None, "tp"),
        ),
        check_vma=False,
    )
```
